512 devices in a mesh: sp: 32 (over z, x), tp: 16 (over y, core).
Axes of the slice: x: 4, y: 8, z: 8, core: 2. Of those that a mesh axis runs over, the one named last changes fastest.
Arguments:
- query_one: bfloat16 [8192, 1024], P('sp', 'tp'), may hold values from -6 to 6
- key_one: bfloat16 [8192, 1024], P('sp', 'tp'), may hold values from -6 to 6
- value_one: bfloat16 [8192, 2048], P('sp', 'tp'), may hold values from -6 to 6
- gate_one: bfloat16 [8192, 2048], P('sp', 'tp'), may hold values from -6 to 6
- decay_one: float32 [2, 8192, 1024], P(None, 'sp', 'tp')
- query_two: bfloat16 [8192, 2048], P('sp', 'tp'), may hold values from -6 to 6
- key_two: bfloat16 [8192, 2048], P('sp', 'tp'), may hold values from -6 to 6
- value_two: bfloat16 [8192, 2048], P('sp', 'tp'), may hold values from -6 to 6
- gate_two: bfloat16 [8192, 2048], P('sp', 'tp'), may hold values from -6 to 6
- decay_two: float32 [2, 8192, 2048], P(None, 'sp', 'tp')
- head_gain: float32 [128], replicated, may hold values from 0.1 to 1.9
- proj_one: bfloat16 [2048, 2048], P('tp'), may hold values from -0.09375 to 0.09375
- proj_two: bfloat16 [2048, 2048], P('tp'), may hold values from -0.09375 to 0.09375
- stream: bfloat16 [8192, 2048], P('sp'), may hold values from -6 to 6
- gain_mix: float32 [2048], replicated, may hold values from 0.1 to 1.9
- gain_moe: float32 [2048], replicated, may hold values from 0.1 to 1.9
- routes: int32 [8192, 2], P('sp'), may hold values from 0 to 31, all different within a row; in each aligned block of 256 rows (0 to 255, 256 to 511, ...) at most 24 rows name the same one
- affinity: float32 [8192, 2], P('sp'), may hold values from 0.1 to 1
- expert_gate: bfloat16 [32, 2048, 2048], P('sp', None, 'tp'), may hold values from -0.125 to 0.125
- expert_up: bfloat16 [32, 2048, 2048], P('sp', None, 'tp'), may hold values from -0.125 to 0.125
- expert_down: bfloat16 [32, 2048, 2048], P('sp', 'tp'), may hold values from -0.125 to 0.125
Outputs:
- output: bfloat16 [8192, 2048], P(('sp', 'tp'))
The draws below stay inside these ranges and needn't reach their ends.
Inputs may be any that keep to these rules, and one draw needn't show every extreme that they name: `routes`: in the 256 rows of one index of sp no expert is named more than 24 times, a bound that some block reaches there in every draw; a row names 2 different experts.
All inputs are finite; a program needn't handle non-finite values.
Results may differ from the reference program's by a relative error of at most 0.017.
Values may be sent and summed in bfloat16 or wider, within the bound.
A program may use at most 64 MiB of HBM per device.

```python
import math
import jax
import jax.numpy as jnp
import numpy as np
from jax import lax

D = 2048
HEADS_A = 16
HEADS_B = 16
DK_A = 64
DK_B = 128
DV = 128
BLK = 64
FF_E = 2048
TOPK = 2
TOK_DEV = 256
STRING_LENGTH = 8192
EXPERTS = 32
CAP = 24
N_SP = 32
N_TP = 16


def decay_field(key, channels):
    keys = jax.random.split(key, 7)
    share = 0.5
    rapid_toggle = jax.random.bernoulli(keys[0], share, (2, 1, channels))
    quick = jax.random.uniform(keys[1], (2, 1, channels), jnp.float32, -0.5, 1.5)
    steady = math.log(STRING_LENGTH / 16.0) + jax.random.uniform(keys[2], (2, 1, channels), jnp.float32, 0.5, 1.5)
    floor_amount = jnp.where(rapid_toggle, quick, steady)
    spans = STRING_LENGTH // TOK_DEV
    additive_displacement = jnp.repeat(jax.random.uniform(keys[3], (2, spans, 1), jnp.float32, -0.7, 0.7), TOK_DEV, axis=1)
    jitter_magnitude = 0.7 * jax.random.truncated_normal(keys[4], -3.0, 3.0, (2, STRING_LENGTH, channels), jnp.float32)
    slot_numbers = jax.random.randint(keys[5], (2, 6), 0, STRING_LENGTH)
    sudden_jump = jnp.any(jnp.arange(STRING_LENGTH)[None, :, None] == slot_numbers[:, None, :], axis=2)[:, :, None]
    intensity_multiplier = jax.random.uniform(keys[6], (2, STRING_LENGTH, 1), jnp.float32, -11.0, -4.0)
    return jnp.where(sudden_jump & jnp.logical_not(rapid_toggle), intensity_multiplier, floor_amount + additive_displacement + jitter_magnitude).astype(jnp.float32)


def draw_decay_one(key, part):
    return decay_field(jax.random.fold_in(key, 11), HEADS_A * DK_A)


def draw_decay_two(key, part):
    return decay_field(jax.random.fold_in(key, 23), HEADS_B * DK_B)


def shard_levels(rng, shape, shards, smallest, high):
    level = 1.0
    for axis_at, shards_of in shards:
        heights = jax.random.uniform(jax.random.fold_in(jax.random.fold_in(rng, 6), axis_at), (shards_of,), jnp.float32, smallest / len(shards), high / len(shards))
        level = level * jnp.repeat(jnp.exp(heights), shape[axis_at] // shards_of).reshape((-1,) + (1,) * (len(shape) - 1 - axis_at))
    return level


def routed_block(stream_key, own, number, rows, count, top, bound, slope):
    ranking = jax.random.permutation(stream_key, count)
    packed, common = shares(count, rows * top, bound, slope, True), shares(count, rows * top, bound, slope, False)
    places = jnp.arange(count)

    def named(tallies, turn):
        used = int((tallies > 0).sum())
        fixed = max(1, used // 4)
        moved = fixed + (places - fixed + turn * (used - fixed)) % max(1, count - fixed)
        return jnp.zeros((count,), jnp.int32).at[ranking[jnp.where(places < fixed, places, moved)]].set(jnp.asarray(tallies, jnp.int32))

    tallies = jnp.where(number % 4 == 0, named(packed, number // 4), named(common, number - number // 4 - 1))
    mixed = jax.random.permutation(jax.random.fold_in(own, 3), count)
    donor, receiver = mixed[0:count // 2 * 2:2], mixed[1:count // 2 * 2:2]
    margin = jnp.minimum(tallies[donor] - 1, bound - tallies[receiver]) // 2
    margin = jnp.where((donor == ranking[0]) | (receiver == ranking[0]) | (tallies[receiver] == 0), 0, jnp.maximum(margin, 0))
    moved = jax.random.randint(jax.random.fold_in(own, 4), (count // 2,), 0, 1 << 20) % (margin + 1)
    tallies = tallies.at[donor].add(-moved).at[receiver].add(moved)
    labels = jnp.searchsorted(jnp.cumsum(tallies), jnp.arange(rows * top), side="right").astype(jnp.int32)
    listing = labels.reshape(top, rows).T
    listing = listing[jax.random.permutation(jax.random.fold_in(own, 1), rows)]
    turn = jax.random.randint(jax.random.fold_in(own, 2), (rows, 1), 0, top)
    return jnp.take_along_axis(listing, (jnp.arange(top)[None, :] + turn) % top, axis=1)


def shares(amount, total, bound, slope, full):
    loads = [(1 << 20) // math.isqrt(rank ** slope) + 1 for rank in range(1, amount + 1)]
    largest = bound if full else min(bound, max(-(-total // amount), total * loads[0] // sum(loads)))
    least = 1 if total - largest >= amount - 1 else 0
    given, rest = [largest] + [least] * (amount - 1), total - largest - least * (amount - 1)
    while rest > 0:
        movable = [i for i in range(1, amount) if given[i] < largest] or [i for i in range(1, amount) if given[i] < bound]
        pool, left = sum([loads[i] for i in movable]), rest
        for i in movable:
            addition = min(bound - given[i], max(1, left * loads[i] // pool), rest)
            given[i] = given[i] + addition
            rest = rest - addition
    return np.array(given)


def centred(own_key, extent, scale, limit, pieces=(), kind=jnp.bfloat16):
    values = jax.random.normal(own_key, extent, jnp.float32) * scale
    if len(pieces) > 0:
        values = shard_levels(own_key, extent, pieces, -0.22, 0.18) * values
    return jnp.clip(values, min=-limit, max=limit).astype(kind)


def setup_inputs(seed: int = 0) -> dict:
    seeds = jax.random.split(jax.random.key(seed), 22)
    query_one = centred(seeds[0], (STRING_LENGTH, HEADS_A * DK_A), 1.0, 6.0, ((0, 32), (1, 16)))
    key_one = centred(seeds[1], (STRING_LENGTH, HEADS_A * DK_A), 1.0, 6.0, ((0, 32), (1, 16)))
    value_one = centred(seeds[2], (STRING_LENGTH, HEADS_A * DV), 1.0, 6.0, ((0, 32), (1, 16)))
    gate_one = centred(seeds[3], (STRING_LENGTH, HEADS_A * DV), 1.0, 6.0, ((0, 32), (1, 16)))
    decay_one = draw_decay_one(jax.random.fold_in(seeds[21], 71), 0)
    query_two = centred(seeds[5], (STRING_LENGTH, HEADS_B * DK_B), 1.0, 6.0, ((0, 32), (1, 16)))
    key_two = centred(seeds[6], (STRING_LENGTH, HEADS_B * DK_B), 1.0, 6.0, ((0, 32), (1, 16)))
    value_two = centred(seeds[7], (STRING_LENGTH, HEADS_B * DV), 1.0, 6.0, ((0, 32), (1, 16)))
    gate_two = centred(seeds[8], (STRING_LENGTH, HEADS_B * DV), 1.0, 6.0, ((0, 32), (1, 16)))
    decay_two = draw_decay_two(jax.random.fold_in(seeds[21], 71), 0)
    head_gain = jnp.clip(1.0 + 0.18 * jax.random.normal(seeds[10], (DV,), jnp.float32), 0.1, 1.9)
    proj_one = centred(seeds[11], (HEADS_A * DV, D), ((HEADS_A + HEADS_B) * DV) ** -0.5, 0.09375, ((0, 16),))
    proj_two = centred(seeds[12], (HEADS_B * DV, D), ((HEADS_A + HEADS_B) * DV) ** -0.5, 0.09375, ((0, 16),))
    stream = centred(seeds[13], (STRING_LENGTH, D), 1.0, 6.0, ((0, 32),))
    gain_mix = jnp.clip(1.0 + 0.18 * jax.random.normal(seeds[14], (D,), jnp.float32), 0.1, 1.9)
    gain_moe = jnp.clip(1.0 + 0.18 * jax.random.normal(seeds[15], (D,), jnp.float32), 0.1, 1.9)
    routes_keys = jax.random.split(jax.random.fold_in(seeds[16], 1), STRING_LENGTH // TOK_DEV)
    routes_turns = jax.random.permutation(jax.random.fold_in(seeds[16], 3), STRING_LENGTH // TOK_DEV)
    routes = jax.vmap(lambda own, number: routed_block(jax.random.fold_in(seeds[16], 2), own, number, TOK_DEV, EXPERTS, TOPK, CAP, 2))(routes_keys, routes_turns).reshape((STRING_LENGTH, TOPK))
    affinity = jnp.clip(0.1 + 0.9 * jax.random.uniform(seeds[17], (STRING_LENGTH, TOPK), jnp.float32) ** shard_levels(seeds[17], (STRING_LENGTH, TOPK), ((0, 32),), -0.2, 0.2), 0.1, 1.0)
    expert_gate = centred(seeds[18], (EXPERTS, D, FF_E), D ** -0.5, 0.125, ((0, 32), (2, 16)))
    expert_up = centred(seeds[19], (EXPERTS, D, FF_E), D ** -0.5, 0.125, ((0, 32), (2, 16)))
    expert_down = centred(seeds[20], (EXPERTS, FF_E, D), FF_E ** -0.5, 0.125, ((0, 32), (1, 16)))
    return {"query_one": query_one, "key_one": key_one, "value_one": value_one, "gate_one": gate_one, "decay_one": decay_one, "query_two": query_two, "key_two": key_two, "value_two": value_two, "gate_two": gate_two, "decay_two": decay_two, "head_gain": head_gain, "proj_one": proj_one, "proj_two": proj_two, "stream": stream, "gain_mix": gain_mix, "gain_moe": gain_moe, "routes": routes, "affinity": affinity, "expert_gate": expert_gate, "expert_up": expert_up, "expert_down": expert_down}


normalizer_sharpness = 16.0
highest = lax.Precision.HIGHEST

def heads_first(values, heads):
    return values.reshape(values.shape[0], heads, -1).transpose(1, 0, 2)

def block_scan(query, key, value, logarithm_fading):
    heads, length, key_size = query.shape
    value_size = value.shape[-1]
    count = length // BLK

    def blocks(tensor):
        return tensor.reshape(heads, count, BLK, tensor.shape[-1])
    qb, kb, vb, gb = (blocks(query), blocks(key), blocks(value), blocks(logarithm_fading))
    cum = jnp.cumsum(gb, axis=2)
    last = cum[:, :, -1:, :]
    q_in = qb * jnp.exp(cum)
    k_in = kb * jnp.exp(-cum)
    k_st = kb * jnp.exp(last - cum)
    lower = jnp.tril(jnp.ones((BLK, BLK), dtype=bool))
    scores = jnp.where(lower, jnp.einsum('hnid,hnjd->hnij', q_in, k_in, precision=highest), 0.0)
    inner = jnp.einsum('hnij,hnjv->hniv', scores, vb, precision=highest)
    growth = jnp.einsum('hnjd,hnjv->hndv', k_st, vb, precision=highest)
    fading_speed = jnp.exp(last[:, :, 0, :])

    def step(state, inputs):
        factor, added = inputs
        return (factor[..., None] * state + added, state)
    final, starts = lax.scan(step, jnp.zeros((heads, key_size, value_size), jnp.float32), (fading_speed.transpose(1, 0, 2), growth.transpose(1, 0, 2, 3)))
    carried = jnp.einsum('hnid,hndv->hniv', q_in, starts.transpose(1, 0, 2, 3), precision=highest)
    return ((inner + carried).reshape(heads, length, value_size), final)

def group_mixed(query, key, value, fading_speed, key_size):
    heads = query.shape[1] // key_size
    qh = heads_first(query.astype(jnp.float32), heads) * key_size ** (-0.5)
    kh = heads_first(key.astype(jnp.float32), heads)
    vh = heads_first(value.astype(jnp.float32), heads)
    logarithm_fading = jax.nn.log_sigmoid(fading_speed) / normalizer_sharpness
    ahead = heads_first(logarithm_fading[0], heads)
    behind = heads_first(logarithm_fading[1], heads)
    forward, _ = block_scan(qh, kh, vh, ahead)
    backward, _ = block_scan(qh[:, ::-1], kh[:, ::-1], vh[:, ::-1], behind[:, ::-1])
    return forward + backward[:, ::-1]

def finish(mixed, gate, head_gain):
    normed = mixed * lax.rsqrt(lax.optimization_barrier(jnp.mean(mixed * mixed, axis=-1, keepdims=True)) + 1e-06) * head_gain
    flat = normed.transpose(1, 0, 2).reshape(mixed.shape[1], -1)
    return (flat * jax.nn.silu(gate.astype(jnp.float32))).astype(jnp.bfloat16)

def layer_norm(values, gain):
    mean = lax.optimization_barrier(jnp.mean(values, axis=-1, keepdims=True))
    spread = lax.optimization_barrier(jnp.mean(jnp.square(values - mean), axis=-1, keepdims=True))
    return (values - mean) * lax.rsqrt(spread + 1e-05) * gain

def reference(query_one, key_one, value_one, gate_one, decay_one, query_two, key_two, value_two, gate_two, decay_two, head_gain, proj_one, proj_two, stream, gain_mix, gain_moe, routes, affinity, expert_gate, expert_up, expert_down):
    heads_one = finish(group_mixed(query_one, key_one, value_one, decay_one, DK_A), gate_one, head_gain)
    heads_two = finish(group_mixed(query_two, key_two, value_two, decay_two, DK_B), gate_two, head_gain)
    width_one = HEADS_A // N_TP * DV
    width_two = HEADS_B // N_TP * DV
    total = jnp.zeros((STRING_LENGTH, D), jnp.float32)
    for block in range(N_TP):
        part = jnp.dot(heads_one[:, block * width_one:(block + 1) * width_one], proj_one[block * width_one:(block + 1) * width_one], preferred_element_type=jnp.float32)
        part = part + jnp.dot(heads_two[:, block * width_two:(block + 1) * width_two], proj_two[block * width_two:(block + 1) * width_two], preferred_element_type=jnp.float32)
        total = total + lax.optimization_barrier(part.astype(jnp.bfloat16)).astype(jnp.float32)
    attn = total.astype(jnp.bfloat16)
    settled = layer_norm(stream.astype(jnp.float32) + attn.astype(jnp.float32), gain_mix)
    moe_in = settled.astype(jnp.bfloat16)
    weights = (affinity / lax.optimization_barrier(jnp.sum(affinity, axis=-1, keepdims=True))).reshape(-1)
    assigned = STRING_LENGTH * TOPK
    flat_expert = routes.reshape(-1).astype(jnp.int32)
    order = jnp.argsort(flat_expert, stable=True).astype(jnp.int32)
    sorted_expert = flat_expert[order]
    counts = lax.optimization_barrier(jnp.sum((flat_expert[:, None] == jnp.arange(EXPERTS, dtype=jnp.int32)[None, :]).astype(jnp.int32), axis=0)).astype(jnp.int32)
    starts = (jnp.cumsum(counts).astype(jnp.int32) - counts).astype(jnp.int32)
    most_rows = N_SP * CAP
    slot = (jnp.arange(assigned, dtype=jnp.int32) - starts[sorted_expert]).astype(jnp.int32)
    table = jnp.full((EXPERTS * most_rows,), -1, jnp.int32).at[sorted_expert * most_rows + slot].set(order)
    table = table.reshape(EXPERTS, most_rows)
    unit_block = FF_E // N_TP

    def per_expert(acc, expert):
        entries = table[expert]
        valid = entries >= 0
        safe = jnp.where(valid, entries, 0).astype(jnp.int32)
        token = (safe // TOPK).astype(jnp.int32)
        rows = moe_in[token]
        gate = jnp.dot(rows, expert_gate[expert], preferred_element_type=jnp.float32)
        upward = jnp.dot(rows, expert_up[expert], preferred_element_type=jnp.float32)
        act = (jax.nn.silu(gate) * upward).astype(jnp.bfloat16)
        act_blocks = act.astype(jnp.float32).reshape(most_rows, N_TP, unit_block)
        down_blocks = expert_down[expert].astype(jnp.float32).reshape(N_TP, unit_block, D)
        partial_value = jnp.einsum('rbf,bfd->rbd', act_blocks, down_blocks, precision=highest)
        rounded = lax.optimization_barrier(partial_value.astype(jnp.bfloat16)).astype(jnp.float32)
        piece = lax.optimization_barrier(lax.optimization_barrier(jnp.sum(rounded, axis=1)).astype(jnp.bfloat16)).astype(jnp.float32)
        scale = jnp.where(valid, weights[safe], 0.0)
        return (acc.at[token].add(scale[:, None] * piece), None)
    mixture, _ = lax.scan(per_expert, jnp.zeros((STRING_LENGTH, D), jnp.float32), jnp.arange(EXPERTS, dtype=jnp.int32))
    return layer_norm(settled + mixture, gain_moe).astype(jnp.bfloat16)
```

```python
import functools

import jax
import jax.numpy as jnp
from jax import lax
from jax.experimental import pallas as pl
from jax.experimental.pallas import tpu as pltpu
from jax.sharding import PartitionSpec as P

DK_A = 64
DK_B = 128
BLK = 64
SHARPNESS = 16.0
ZN, XN, YN = 8, 4, 8
F32 = jnp.float32
BF16 = jnp.bfloat16
MESH = pl.DeviceIdType.MESH
VMEM = pl.BlockSpec(memory_space=pltpu.VMEM)
DMA = pltpu.SemaphoreType.DMA


def params(collective_id=None):
    if collective_id is None:
        return pltpu.CompilerParams(vmem_limit_bytes=48 * 2**20)
    return pltpu.CompilerParams(
        vmem_limit_bytes=48 * 2**20, collective_id=collective_id, has_side_effects=True
    )


def mm(a, b):
    return jnp.dot(a, b, preferred_element_type=F32)


def mm_nt(a, b):
    return lax.dot_general(a, b, (((1,), (1,)), ((), ())), preferred_element_type=F32)


def mm_tn(a, b):
    return lax.dot_general(a, b, (((0,), (0,)), ((), ())), preferred_element_type=F32)


def log_sigmoid(x):
    return jnp.minimum(x, 0.0) - jnp.log1p(jnp.exp(-jnp.abs(x)))


def silu(x):
    return x / (1.0 + jnp.exp(-x))


def layer_norm(values, gain):
    mean = jnp.mean(values, axis=-1, keepdims=True)
    spread = jnp.mean(jnp.square(values - mean), axis=-1, keepdims=True)
    return (values - mean) * lax.rsqrt(spread + 1e-05) * gain


def greet(peers):
    barrier = pltpu.get_barrier_semaphore()
    for peer in peers:
        pl.semaphore_signal(barrier, inc=1, device_id=peer, device_id_type=MESH)
    pl.semaphore_wait(barrier, len(peers))


def remote(src, dst, send, recv, peer):
    return pltpu.make_async_remote_copy(
        src_ref=src, dst_ref=dst, send_sem=send, recv_sem=recv, device_id=peer, device_id_type=MESH
    )


def across(me, k, n):
    place, bit = 0, 1
    while bit < n:
        digit = lax.rem(me // bit, 2)
        place = place + (1 - digit if k & bit else digit) * bit
        bit *= 2
    return place


def state_kernel(ka, va, da, kb, vb, db, stack, cum):
    rows = ka.shape[0]
    count = rows // BLK
    ii = lax.broadcasted_iota(jnp.int32, (rows, rows), 0)
    jj = lax.broadcasted_iota(jnp.int32, (rows, rows), 1)
    same = (ii // BLK) == (jj // BLK)
    lower = jnp.where(same & (ii >= jj), 1.0, 0.0).astype(BF16)
    upper = jnp.where(same & (ii <= jj), 1.0, 0.0).astype(BF16)
    base = 0
    for k, v, d, dk in ((ka, va, da, DK_A), (kb, vb, db, DK_B)):
        wide = k.shape[1]
        heads = wide // dk
        dv = v.shape[1] // heads
        keys = k[...].astype(F32)
        for way in range(2):
            fade = log_sigmoid(d[way]) / SHARPNESS
            high = fade.astype(BF16)
            low = (fade - high.astype(F32)).astype(BF16)
            tri = lower if way == 0 else upper
            total = mm(tri, high) + mm(tri, low)
            cum[way, :, base : base + wide] = total
            tail = jnp.zeros((1, wide), F32)
            weighted = [None] * count
            for b in reversed(range(count)) if way == 0 else range(count):
                part = total[b * BLK : (b + 1) * BLK]
                last = part[BLK - 1 : BLK] if way == 0 else part[0:1]
                weighted[b] = (keys[b * BLK : (b + 1) * BLK] * jnp.exp(last - part + tail)).astype(BF16)
                tail = tail + last
            weighted = jnp.concatenate(weighted, axis=0)
            states = [
                mm_tn(v[:, h * dv : (h + 1) * dv], weighted[:, h * dk : (h + 1) * dk]).astype(BF16)
                for h in range(heads)
            ]
            states = states[0] if heads == 1 else jnp.concatenate(states, axis=1)
            thigh = tail.astype(BF16).astype(F32)
            row = lax.broadcasted_iota(jnp.int32, (16, wide), 0)
            fades = jnp.where(row == 0, thigh, jnp.where(row == 1, tail - thigh, 0.0)).astype(BF16)
            half = dv // 2
            for i in range(2):
                stack[i, way, 0:half, base : base + wide] = states[i * half : (i + 1) * half]
                stack[i, way, half : half + 16, base : base + wide] = fades
        base += wide


def spread(total, wide):
    row = lax.broadcasted_iota(jnp.int32, (16, wide), 0)
    high = total.astype(BF16).astype(F32)
    return jnp.where(row == 0, high, jnp.where(row == 1, total - high, 0.0)).astype(BF16)


def states_exchange_kernel(n, stack, out, xbox, agg, zbox, outbox, xs, xr, zs, zr, bs, br):
    me = lax.axis_index("sp")
    side = lax.rem(me, 2)
    pair = me // 2
    pairs = n // 2
    partner = me + 1 - 2 * side
    half = out.shape[2]
    lanes = out.shape[3]
    chunk = 256 if lanes % 256 == 0 else lanes
    count = lanes // chunk

    def pair_at(j):
        return lax.rem(pair + j, pairs)

    greet([{"sp": partner}] + [{"sp": pair_at(j) * 2 + side} for j in range(1, pairs)])

    def at(c):
        return pl.ds(c * chunk, chunk)

    def swap(c):
        return remote(
            stack.at[1 - side, :, :, at(c)], xbox.at[:, :, at(c)], xs.at[c], xr.at[c], {"sp": partner}
        )

    def along(c, j):
        way = jnp.where(pair_at(j) < pair, 1, 0)
        return remote(
            agg.at[way, :, at(c)], zbox.at[pair, :, at(c)], zs.at[c, j], zr.at[c, j],
            {"sp": pair_at(j) * 2 + side},
        )

    def back(c):
        return remote(
            outbox.at[:, :, at(c)], out.at[:, side, :, at(c)], bs.at[c], br.at[c], {"sp": partner}
        )

    for c in range(count):
        swap(c).start()
    zbox[pair] = jnp.zeros_like(zbox[pair])

    def load(ref, index, c):
        block = ref[index + (slice(None), at(c))].astype(F32)
        return block[0:half], block[half : half + 1] + block[half + 1 : half + 2]

    def both(c, way):
        own, own_fade = load(stack, (side, way), c)
        other, other_fade = load(xbox, (way,), c)
        low = side == 0
        return (
            jnp.where(low, own, other), jnp.where(low, own_fade, other_fade),
            jnp.where(low, other, own), jnp.where(low, other_fade, own_fade),
        )

    for c in range(count):
        swap(c).wait_recv()
        s0, t0, s1, t1 = both(c, 0)
        agg[0, 0:half, at(c)] = (jnp.exp(t1) * s0 + s1).astype(BF16)
        agg[0, half : half + 16, at(c)] = spread(t0 + t1, chunk)
        s0, t0, s1, t1 = both(c, 1)
        agg[1, 0:half, at(c)] = (jnp.exp(t0) * s1 + s0).astype(BF16)
        agg[1, half : half + 16, at(c)] = spread(t0 + t1, chunk)
        for j in range(1, pairs):
            along(c, j).start()
    for c in range(count):
        for j in range(1, pairs):
            along(c, j).wait_recv()
        ahead = jnp.zeros((half, chunk), F32)
        behind = jnp.zeros((half, chunk), F32)
        for s in range(pairs):
            state, fade = load(zbox, (s,), c)
            ahead = jnp.where(s < pair, jnp.exp(fade) * ahead + state, ahead)
        for s in reversed(range(pairs)):
            state, fade = load(zbox, (s,), c)
            behind = jnp.where(s > pair, jnp.exp(fade) * behind + state, behind)
        low = side == 0
        s0, t0, _, _ = both(c, 0)
        next_ahead = jnp.exp(t0) * ahead + s0
        _, _, s1, t1 = both(c, 1)
        next_behind = jnp.exp(t1) * behind + s1
        outbox[0, :, at(c)] = jnp.where(low, next_ahead, ahead).astype(BF16)
        outbox[1, :, at(c)] = jnp.where(low, behind, next_behind).astype(BF16)
        back(c).start()
        out[0, side, :, at(c)] = jnp.where(low, ahead, next_ahead).astype(BF16)
        out[1, side, :, at(c)] = jnp.where(low, next_behind, behind).astype(BF16)
    for c in range(count):
        swap(c).wait_send()
        for j in range(1, pairs):
            along(c, j).wait_send()
        back(c).wait_send()
        remote(
            outbox.at[:, :, at(c)], out.at[:, 1 - side, :, at(c)], bs.at[c], br.at[c], {"sp": partner}
        ).wait_recv()


def mix_kernel(states, cum, qa, ka, va, ga, qb, kb, vb, gb, gain, pa, pb, out, heads_ref):
    rows = qa.shape[0]
    count = rows // BLK
    dv = gain.shape[1]
    ii = lax.broadcasted_iota(jnp.int32, (BLK, BLK), 0)
    jj = lax.broadcasted_iota(jnp.int32, (BLK, BLK), 1)
    base = 0
    column = 0
    for q, k, v, g, dk in ((qa, ka, va, ga, DK_A), (qb, kb, vb, gb, DK_B)):
        heads = q.shape[1] // dk
        for h in range(heads):
            lanes = slice(base + h * dk, base + (h + 1) * dk)
            own = slice(h * dk, (h + 1) * dk)
            vown = slice(h * dv, (h + 1) * dv)
            forward = jnp.concatenate([states[0, i, :, lanes] for i in range(2)], axis=0).astype(F32)
            backward = jnp.concatenate([states[1, i, :, lanes] for i in range(2)], axis=0).astype(F32)
            mixed = [None] * count
            readers = [None] * count
            growth = [None] * count
            for b in range(count):
                at = slice(b * BLK, (b + 1) * BLK)
                query = q[at, own].astype(F32) * dk ** (-0.5)
                key = k[at, own].astype(F32)
                value = v[at, vown]
                cf = cum[0, at, lanes]
                cb = cum[1, at, lanes]
                qf = (query * jnp.exp(cf)).astype(BF16)
                kf = (key * jnp.exp(-cf)).astype(BF16)
                qr = (query * jnp.exp(cb)).astype(BF16)
                kr = (key * jnp.exp(-cb)).astype(BF16)
                scores = jnp.where(ii >= jj, mm_nt(qf, kf), 0.0) + jnp.where(ii <= jj, mm_nt(qr, kr), 0.0)
                inner = mm(scores.astype(BF16), value)
                lastf = cf[BLK - 1 : BLK]
                inner = inner + mm_nt(qf, forward.astype(BF16))
                if b < count - 1:
                    kfs = (key * jnp.exp(lastf - cf)).astype(BF16)
                    forward = jnp.exp(lastf) * forward + mm_tn(value, kfs)
                mixed[b] = inner
                readers[b] = qr
                lastb = cb[0:1]
                if b > 0:
                    kbs = (key * jnp.exp(lastb - cb)).astype(BF16)
                    growth[b] = (jnp.exp(lastb), mm_tn(value, kbs))
            for b in reversed(range(count)):
                at = slice(b * BLK, (b + 1) * BLK)
                whole = mixed[b] + mm_nt(readers[b], backward.astype(BF16))
                if b > 0:
                    backward = growth[b][0] * backward + growth[b][1]
                scale = lax.rsqrt(jnp.mean(whole * whole, axis=-1, keepdims=True) + 1e-06)
                heads_ref[at, column + h * dv : column + (h + 1) * dv] = (
                    whole * scale * gain[...] * silu(g[at, vown].astype(F32))
                ).astype(BF16)
        base += heads * dk
        column += heads * dv
    split = pa.shape[0]
    width = out.shape[1]
    tile = min(512, width)
    for j in range(width // tile):
        cols = slice(j * tile, (j + 1) * tile)
        out[:, cols] = (
            mm(heads_ref[:, :split], pa[:, cols]) + mm(heads_ref[:, split:], pb[:, cols])
        ).astype(BF16)


def settle_kernel(
    n, part, stream, gain, settled, columns, inbox, mid, midbox, outbox, cs, cr, ys, yr, send2, recv2
):
    me = lax.axis_index("tp")
    own = part.shape[0] // n
    wide = part.shape[1] // n
    core = lax.rem(me, 2)
    line = me // 2
    lines = n // 2
    greet([{"tp": lax.rem(me + k, n)} for k in range(1, n)])

    def rows_of(i):
        return pl.ds(pl.multiple_of(i * own, own), own)

    def cols_of(i):
        return pl.ds(pl.multiple_of(i * wide, wide), wide)

    def line_at(j):
        return lax.rem(line + j, lines)

    def to_core(j):
        i = line_at(j) * 2 + 1 - core
        return remote(
            part.at[rows_of(i), :], inbox.at[j], cs.at[j], cr.at[j], {"tp": me + 1 - 2 * core}
        )

    def to_line(j):
        return remote(mid.at[j], midbox.at[j], ys.at[j], yr.at[j], {"tp": line_at(j) * 2 + core})

    for j in reversed(range(lines)):
        to_core(j).start()
    for j in reversed(range(lines)):
        to_core(j).wait_recv()
        mine = part[rows_of(line_at(j) * 2 + core), :].astype(F32) + inbox[j].astype(F32)
        if j > 0:
            mid[j] = mine.astype(BF16)
            to_line(j).start()
        else:
            total = mine
    for j in range(1, lines):
        to_line(j).wait_recv()
        total = total + midbox[j].astype(F32)
    total = total.astype(BF16).astype(F32)
    value = layer_norm(stream[rows_of(me), :].astype(F32) + total, gain[...])
    settled[...] = value
    outbox[...] = value.astype(BF16)
    second = []
    for k in range(1, n):
        peer = lax.rem(me + k, n)
        copy = remote(
            outbox.at[:, cols_of(peer)], columns.at[rows_of(me), :], send2.at[k], recv2.at[k], {"tp": peer}
        )
        copy.start()
        second.append(copy)
    columns[rows_of(me), :] = outbox[:, cols_of(me)]
    for k in range(1, n):
        source = lax.rem(me + n - k, n)
        second[k - 1].wait_send()
        remote(
            outbox.at[:, cols_of(source)], columns.at[rows_of(source), :], send2.at[k], recv2.at[k], {"tp": source}
        ).wait_recv()
    for j in range(lines):
        to_core(j).wait_send()
        if j > 0:
            to_line(j).wait_send()


def ring_sites():
    sp = lax.axis_index("sp")
    tp = lax.axis_index("tp")
    return sp, sp // XN, lax.rem(sp, XN), tp, tp // 2, lax.rem(tp, 2)


def sp_at(z, x, dz, dx):
    return lax.rem(z + dz, ZN) * XN + lax.rem(x + dx, XN)


def near(d, n):
    return min(d, n - d)


def carried(way, d, k):
    return d < YN // 2 or k == way


def moe_kernel(
    routes, affinity, columns, settled, gain, wg_hbm, wu_hbm, wd_hbm, out,
    wg, wu, wd, mixhi, mixlo, picked, x, acc, act, p, s, r, q, pieces, term, mixture,
    wls, wrs, wrr, as_, ar, gs, gr, rs, rr, bs, br, fs, fr,
):
    sp, z, xx, tp, y, c = ring_sites()
    n = ZN * XN
    m = YN * 2
    half = YN // 2
    per = XN // 2
    slots = picked.shape[1]
    count = ZN * per
    group = count * slots
    lanes = picked.shape[2]
    rows = columns.shape[0]
    own = rows // m
    partner = {"tp": tp + 1 - 2 * c}

    barrier = pltpu.get_barrier_semaphore()

    def greet_one(peer):
        pl.semaphore_signal(barrier, inc=1, device_id=peer, device_id_type=MESH)

    for k in range(1, m):
        greet_one({"tp": lax.rem(tp + k, m)})
    for dz in range(ZN):
        for dx in range(XN):
            if dz or dx:
                greet_one({"sp": sp_at(z, xx, dz, dx), "tp": y * 2 + dx % 2})
    for j in range(count):
        peer = {"sp": sp_at(z, xx, j // per, 2 * (j % per) + c), "tp": y * 2 + 1 - c}
        if j == 0:
            pl.when(c == 1)(functools.partial(greet_one, peer))
        else:
            greet_one(peer)

    loads = [
        pltpu.make_async_copy(src.at[0], dst.at[0], wls.at[i])
        for i, (src, dst) in enumerate(((wg_hbm, wg), (wu_hbm, wu), (wd_hbm, wd)))
    ]
    for load in loads:
        load.start()

    lane = lax.broadcasted_iota(jnp.int32, (n, rows), 0)
    hots = [routes[i : i + 1, :] == lane for i in range(2)]
    named = sum(jnp.where(h, 1.0, 0.0) for h in hots)
    ii = lax.broadcasted_iota(jnp.int32, (rows, rows), 0)
    jj = lax.broadcasted_iota(jnp.int32, (rows, rows), 1)
    before = mm(named.astype(BF16), jnp.where(ii < jj, 1.0, 0.0).astype(BF16))
    place = [
        routes[i : i + 1, :] * slots
        + jnp.sum(jnp.where(hots[i], before, 0.0), axis=0, keepdims=True).astype(jnp.int32)
        for i in range(2)
    ]
    seat = lax.broadcasted_iota(jnp.int32, (n * slots, rows), 0)
    hot = jnp.where((seat == place[0]) | (seat == place[1]), 1.0, 0.0).astype(BF16)
    picked[...] = mm(hot, columns[...]).astype(BF16).reshape(picked.shape)

    pl.semaphore_wait(barrier, (m - 1) + (n - 1) + (count - 1) + c)

    def dispatch(dz, dx):
        e = sp_at(z, xx, dz, dx)
        rz, rx = (-dz) % ZN, (-dx) % XN
        j = rz * per + rx // 2
        return remote(
            picked.at[e], x.at[y, c, j], as_.at[dz * XN + dx], ar.at[c, j], {"sp": e, "tp": y * 2 + dx % 2}
        )

    home = pltpu.make_async_copy(picked.at[sp], x.at[y, 0, 0], ar.at[0, 0])
    offsets = sorted(
        [(dz, dx) for dz in range(ZN) for dx in range(XN)],
        key=lambda o: -(near(o[0], ZN) + near(o[1], XN)),
    )
    for dz, dx in offsets:
        if dz or dx:
            dispatch(dz, dx).start()
    pl.when(c == 0)(lambda: home.start())
    pl.when(c == 1)(lambda: dispatch(0, 0).start())

    swaps = [
        remote(src.at[0], dst.at[1], wrs.at[i], wrr.at[i], partner)
        for i, (src, dst) in enumerate(((wg_hbm, wg), (wu_hbm, wu), (wd_hbm, wd)))
    ]
    for swap in swaps:
        swap.start()

    weights = [affinity[i : i + 1, :] / (affinity[0:1, :] + affinity[1:2, :]) for i in range(2)]
    mix = jnp.where(seat == place[0], weights[0], jnp.where(seat == place[1], weights[1], 0.0)).T
    high = mix.astype(BF16)
    mixhi[...] = high
    mixlo[...] = (mix - high.astype(F32)).astype(BF16)

    def arrive(k, j):
        remote(picked.at[0], x.at[y, k, j], as_.at[0], ar.at[k, j], partner).wait_recv()

    def hop(way, h, k):
        step = 1 if way == 0 else YN - 1
        b = lax.rem(y + (h - 1) * (YN - step), YN)
        return remote(
            x.at[b, k], x.at[b, k], gs.at[way, h - 1, k], gr.at[way, h - 1, k],
            {"tp": lax.rem(y + step, YN) * 2 + c},
        )

    def landed(way, h, k):
        step = 1 if way == 0 else YN - 1
        b = lax.rem(y + h * (YN - step), YN)
        remote(
            x.at[b, k], x.at[b, k], gs.at[way, h - 1, k], gr.at[way, h - 1, k],
            {"tp": lax.rem(y + step, YN) * 2 + c},
        ).wait_recv()

    def widen(b, first=False):
        at = pl.ds(pl.multiple_of(b * 2 * lanes, 2 * lanes), 2 * lanes)
        block = jnp.concatenate([x[b, k].reshape(group, lanes) for k in range(2)], axis=1)
        w = jnp.concatenate([ref[i, at, :] for ref in (wg, wu) for i in range(2)], axis=1)
        value = mm(block, w)
        acc[...] = value if first else acc[...] + value

    for k in range(2):
        for j in range(count):
            if k == 0 and j == 0:
                pl.when(c == 0)(lambda: home.wait())
                pl.when(c == 1)(lambda: arrive(0, 0))
            else:
                arrive(k, j)
        for way in range(2):
            if carried(way, 1, k):
                hop(way, 1, k).start()
    for load in loads:
        load.wait()
    for swap in swaps:
        swap.wait_recv()
    widen(y, first=True)
    for h in range(1, half + 1):
        for k in range(2):
            for way in range(2):
                if carried(way, h, k):
                    landed(way, h, k)
                    if h < half and carried(way, h + 1, k):
                        hop(way, h + 1, k).start()
        widen(lax.rem(y + YN - h, YN))
        if h < half:
            widen(lax.rem(y + h, YN))

    hidden = 2 * lanes
    act[...] = (silu(acc[:, :hidden]) * acc[:, hidden:]).astype(BF16)

    def narrow(o):
        b = lax.rem(y + o, YN)
        at = pl.ds(pl.multiple_of(b * hidden, hidden), hidden)
        p[o] = mm(act[...], jnp.concatenate([wd[i, :, at] for i in range(2)], axis=0))

    def offset(way, d):
        return d if way == 0 else YN - d

    def part(o, k):
        return p[o, :, k * lanes : (k + 1) * lanes]

    def pass_sum(way, d, k):
        step = 1 if way == 0 else YN - 1
        return remote(
            s.at[way, d - 1, k], r.at[way, d - 1, k], rs.at[way, d - 1, k], rr.at[way, d - 1, k],
            {"tp": lax.rem(y + step, YN) * 2 + c},
        )

    narrow(half)
    for way in range(2):
        s[way, half - 1, way] = part(half, way).astype(BF16)
        pass_sum(way, half, way).start()
    for d in range(half - 1, 0, -1):
        narrow(d)
        narrow(YN - d)
        for turn in range(2):
            for way in range(2):
                k = 1 - turn if way == 0 else turn
                total = part(offset(way, d), k)
                if carried(way, d + 1, k):
                    pass_sum(way, d + 1, k).wait_recv()
                    total = total + r[way, d, k].astype(F32)
                s[way, d - 1, k] = total.astype(BF16)
                pass_sum(way, d, k).start()
    narrow(0)

    def give(k, j):
        rz = j // per
        rx = 2 * (j % per) + c
        o = ((-rz) % ZN) * XN + lax.rem(XN - rx, XN)
        return remote(
            q.at[k, j], pieces.at[sp], bs.at[k, j], br.at[o], {"sp": sp_at(z, xx, rz, rx), "tp": y * 2 + k}
        )

    back = pltpu.make_async_copy(q.at[0, 0], pieces.at[sp], br.at[0])
    for k in range(2):
        total = part(0, k)
        for way in range(2):
            if carried(way, 1, k):
                pass_sum(way, 1, k).wait_recv()
                total = total + r[way, 0, k].astype(F32)
        q[k] = total.astype(BF16).reshape(count, slots, lanes)
        order = sorted(range(count), key=lambda j: -near(j // per, ZN))
        for j in order:
            if k == 0 and j == 0:
                pl.when(c == 0)(lambda: back.start())
                pl.when(c == 1)(lambda: give(0, 0).start())
            else:
                give(k, j).start()

    for dz in range(ZN):
        for dx in range(XN):
            o = dz * XN + dx
            e = sp_at(z, xx, dz, dx)
            coming = remote(q.at[0, 0], pieces.at[e], bs.at[0, 0], br.at[o], partner)
            if o == 0:
                pl.when(c == 0)(lambda: back.wait())
                pl.when(c == 1)(lambda: coming.wait_recv())
            else:
                coming.wait_recv()

    flat = pieces[...].reshape(n * slots, lanes)
    term[...] = (mm(mixhi[...], flat) + mm(mixlo[...], flat)).astype(BF16)

    def rows_of(i):
        return pl.ds(pl.multiple_of(i * own, own), own)

    def cols_of(i):
        return pl.ds(pl.multiple_of(i * lanes, lanes), lanes)

    def spread_rows(k):
        peer = lax.rem(tp + k, m)
        return remote(term.at[rows_of(peer), :], mixture.at[:, cols_of(tp)], fs.at[k], fr.at[k], {"tp": peer})

    for k in sorted(range(1, m), key=lambda k: -near(k // 2, YN)):
        spread_rows(k).start()
    mixture[:, cols_of(tp)] = term[rows_of(tp), :]
    for k in range(1, m):
        source = lax.rem(tp + m - k, m)
        remote(
            term.at[rows_of(source), :], mixture.at[:, cols_of(source)], fs.at[k], fr.at[k], {"tp": source}
        ).wait_recv()
    out[...] = layer_norm(settled[...] + mixture[...].astype(F32), gain[...]).astype(BF16)

    for dz, dx in offsets:
        if dz or dx:
            dispatch(dz, dx).wait_send()
    pl.when(c == 1)(lambda: dispatch(0, 0).wait_send())
    for swap in swaps:
        swap.wait_send()
    for way in range(2):
        for d in range(1, half + 1):
            for k in range(2):
                if carried(way, d, k):
                    hop(way, d, k).wait_send()
                    pass_sum(way, d, k).wait_send()
    for k in range(2):
        for j in range(count):
            if k == 0 and j == 0:
                pl.when(c == 1)(lambda: give(0, 0).wait_send())
            else:
                give(k, j).wait_send()
    for k in range(1, m):
        spread_rows(k).wait_send()


ANY = pl.BlockSpec(memory_space=pl.ANY)


def moe_call(routes, affinity, columns, settled, gain, wg, wu, wd):
    n = ZN * XN
    m = YN * 2
    half = YN // 2
    rows, lanes = columns.shape
    slots = 3 * rows * 2 // (2 * n)
    count = n // 2
    group = count * slots
    width = settled.shape[1]
    own = rows // m
    scratch = [
        pltpu.VMEM((2, width, lanes), BF16),
        pltpu.VMEM((2, width, lanes), BF16),
        pltpu.VMEM((2, lanes, width), BF16),
        pltpu.VMEM((rows, n * slots), BF16),
        pltpu.VMEM((rows, n * slots), BF16),
        pltpu.VMEM((n, slots, lanes), BF16),
        pltpu.VMEM((YN, 2, count, slots, lanes), BF16),
        pltpu.VMEM((group, 4 * lanes), F32),
        pltpu.VMEM((group, 2 * lanes), BF16),
        pltpu.VMEM((YN, group, 2 * lanes), F32),
        pltpu.VMEM((2, half, 2, group, lanes), BF16),
        pltpu.VMEM((2, half, 2, group, lanes), BF16),
        pltpu.VMEM((2, count, slots, lanes), BF16),
        pltpu.VMEM((n, slots, lanes), BF16),
        pltpu.VMEM((rows, lanes), BF16),
        pltpu.VMEM((own, width), BF16),
        DMA((3,)), DMA((3,)), DMA((3,)),
        DMA((n,)), DMA((2, count)),
        DMA((2, half, 2)), DMA((2, half, 2)),
        DMA((2, half, 2)), DMA((2, half, 2)),
        DMA((2, count)), DMA((n,)),
        DMA((m,)), DMA((m,)),
    ]
    return pl.pallas_call(
        moe_kernel,
        out_shape=jax.ShapeDtypeStruct((own, width), BF16),
        in_specs=[VMEM] * 5 + [ANY] * 3,
        out_specs=VMEM,
        scratch_shapes=scratch,
        compiler_params=params(3),
    )(routes, affinity, columns, settled, gain, wg, wu, wd)


def call(kernel, outs, scratch, count, collective_id=None):
    single = not isinstance(outs, list)
    return pl.pallas_call(
        kernel,
        out_shape=outs,
        in_specs=[VMEM] * count,
        out_specs=VMEM if single else [VMEM] * len(outs),
        scratch_shapes=scratch,
        compiler_params=params(collective_id),
    )


def body(
    query_one,
    key_one,
    value_one,
    gate_one,
    decay_one,
    query_two,
    key_two,
    value_two,
    gate_two,
    decay_two,
    head_gain,
    proj_one,
    proj_two,
    stream,
    gain_mix,
    gain_moe,
    routes,
    affinity,
    expert_gate,
    expert_up,
    expert_down,
):
    shape = jax.ShapeDtypeStruct
    rows = query_one.shape[0]
    n = lax.axis_size("sp")
    m = lax.axis_size("tp")
    width = stream.shape[1]
    own = rows // m
    wide = width // m
    dv = head_gain.shape[0]
    lanes = query_one.shape[1] + query_two.shape[1]
    values = value_one.shape[1] + value_two.shape[1]
    half = dv // 2
    stack, cum = call(
        state_kernel, [shape((2, 2, half + 16, lanes), BF16), shape((2, rows, lanes), F32)], [], 6
    )(key_one, value_one, decay_one, key_two, value_two, decay_two)
    chunks = max(1, lanes // 256)
    states = call(
        functools.partial(states_exchange_kernel, n),
        shape((2, 2, half, lanes), BF16),
        [
            pltpu.VMEM((2, half + 16, lanes), BF16),
            pltpu.VMEM((2, half + 16, lanes), BF16),
            pltpu.VMEM((n // 2, half + 16, lanes), BF16),
            pltpu.VMEM((2, half, lanes), BF16),
            DMA((chunks,)), DMA((chunks,)), DMA((chunks, n // 2)), DMA((chunks, n // 2)),
            DMA((chunks,)), DMA((chunks,)),
        ],
        1,
        1,
    )(stack)
    part = call(mix_kernel, shape((rows, width), BF16), [pltpu.VMEM((rows, values), BF16)], 13)(
        states, cum, query_one, key_one, value_one, gate_one, query_two, key_two, value_two, gate_two,
        head_gain.reshape(1, -1), proj_one, proj_two,
    )
    settled, columns = call(
        functools.partial(settle_kernel, m),
        [shape((own, width), F32), shape((rows, wide), BF16)],
        [pltpu.VMEM((m // 2, own, width), BF16)] * 3
        + [pltpu.VMEM((own, width), BF16)]
        + [DMA((m // 2,))] * 4
        + [DMA((m,))] * 2,
        3,
        2,
    )(part, stream, gain_mix.reshape(1, -1))
    return moe_call(
        routes.T, affinity.T, columns, settled, gain_moe.reshape(1, -1), expert_gate, expert_up, expert_down
    )


def solution(mesh):
    return jax.shard_map(
        body,
        mesh=mesh,
        in_specs=(
            P("sp", "tp"),
            P("sp", "tp"),
            P("sp", "tp"),
            P("sp", "tp"),
            P(None, "sp", "tp"),
            P("sp", "tp"),
            P("sp", "tp"),
            P("sp", "tp"),
            P("sp", "tp"),
            P(None, "sp", "tp"),
            P(),
            P("tp", None),
            P("tp", None),
            P("sp", None),
            P(),
            P(),
            P("sp", None),
            P("sp", None),
            P("sp", None, "tp"),
            P("sp", None, "tp"),
            P("sp", "tp", None),
        ),
        out_specs=P(("sp", "tp"), None),
        check_vma=False,
    )
```

```python
import functools

import jax
import jax.numpy as jnp
from jax import lax
from jax.experimental import pallas as pl
from jax.experimental.pallas import tpu as pltpu
from jax.sharding import PartitionSpec as P

DK_A = 64
DK_B = 128
BLK = 64
SHARPNESS = 16.0
ZN, XN, YN = 8, 4, 8
CUTS = 4
FADES = 8
F32 = jnp.float32
BF16 = jnp.bfloat16
MESH = pl.DeviceIdType.MESH
VMEM = pl.BlockSpec(memory_space=pltpu.VMEM)
ANY = pl.BlockSpec(memory_space=pl.ANY)
DMA = pltpu.SemaphoreType.DMA


def mm(a, b):
    return jnp.dot(a, b, preferred_element_type=F32)


def mm_nt(a, b):
    return lax.dot_general(a, b, (((1,), (1,)), ((), ())), preferred_element_type=F32)


def mm_tn(a, b):
    return lax.dot_general(a, b, (((0,), (0,)), ((), ())), preferred_element_type=F32)


def log_sigmoid(x):
    return jnp.minimum(x, 0.0) - jnp.log1p(jnp.exp(-jnp.abs(x)))


def silu(x):
    return x / (1.0 + jnp.exp(-x))


def layer_norm(values, gain):
    mean = jnp.mean(values, axis=-1, keepdims=True)
    spread = jnp.mean(jnp.square(values - mean), axis=-1, keepdims=True)
    return (values - mean) * lax.rsqrt(spread + 1e-05) * gain


def remote(src, dst, send, recv, peer):
    return pltpu.make_async_remote_copy(
        src_ref=src, dst_ref=dst, send_sem=send, recv_sem=recv, device_id=peer, device_id_type=MESH
    )


def sp_at(z, x, dz, dx):
    return lax.rem(z + dz, ZN) * XN + lax.rem(x + dx, XN)


def near(d, n):
    return min(d, n - d)


def carried(way, d, k, cuts):
    return d < YN // 2 or k // (cuts // 2) == way


def step_of(way):
    return 1 if way == 0 else YN - 1


def fade_rows(total):
    wide = total.shape[1]
    row = lax.broadcasted_iota(jnp.int32, (FADES, wide), 0)
    high = total.astype(BF16).astype(F32)
    return jnp.where(row == 0, high, jnp.where(row == 1, total - high, 0.0)).astype(BF16)


def local_states(keys, values, decays, base, stack, cum):
    rows, wide = keys.shape
    count = rows // BLK
    dv = values.shape[1]
    piece = dv // XN
    ii = lax.broadcasted_iota(jnp.int32, (rows, rows), 0)
    jj = lax.broadcasted_iota(jnp.int32, (rows, rows), 1)
    same = (ii // BLK) == (jj // BLK)
    for way in range(2):
        tri = jnp.where(same & ((ii >= jj) if way == 0 else (ii <= jj)), 1.0, 0.0).astype(BF16)
        fade = log_sigmoid(decays[way]) / SHARPNESS
        high = fade.astype(BF16)
        low = (fade - high.astype(F32)).astype(BF16)
        total = mm(tri, high) + mm(tri, low)
        cum[way, :, base : base + wide] = total
        tail = jnp.zeros((1, wide), F32)
        weighted = [None] * count
        for b in reversed(range(count)) if way == 0 else range(count):
            part = total[b * BLK : (b + 1) * BLK]
            last = part[BLK - 1 : BLK] if way == 0 else part[0:1]
            weighted[b] = (keys[b * BLK : (b + 1) * BLK] * jnp.exp(last - part + tail)).astype(BF16)
            tail = tail + last
        state = mm_tn(values, jnp.concatenate(weighted, axis=0)).astype(BF16)
        fades = fade_rows(tail)
        for i in range(XN):
            stack[i, way, 0:piece, base : base + wide] = state[i * piece : (i + 1) * piece]
            stack[i, way, piece : piece + FADES, base : base + wide] = fades


def local_mix(query, keys, values, base, cum, reach, column, mixed):
    rows, dk = keys.shape
    count = rows // BLK
    dv = values.shape[1]
    ii = lax.broadcasted_iota(jnp.int32, (BLK, BLK), 0)
    jj = lax.broadcasted_iota(jnp.int32, (BLK, BLK), 1)
    lanes = slice(base, base + dk)
    query = query * dk ** (-0.5)
    inner = [None] * count
    readers = [None] * count
    state = None
    passed = jnp.zeros((1, dk), F32)
    for b in range(count):
        at = slice(b * BLK, (b + 1) * BLK)
        value = values[at]
        cf = cum[0, at, lanes]
        cb = cum[1, at, lanes]
        qf = (query[at] * jnp.exp(cf)).astype(BF16)
        kf = (keys[at] * jnp.exp(-cf)).astype(BF16)
        qr = (query[at] * jnp.exp(cb)).astype(BF16)
        kr = (keys[at] * jnp.exp(-cb)).astype(BF16)
        scores = jnp.where(ii >= jj, mm_nt(qf, kf), 0.0) + jnp.where(ii <= jj, mm_nt(qr, kr), 0.0)
        inner[b] = mm(scores.astype(BF16), value)
        if b > 0:
            inner[b] = inner[b] + mm_nt(qf, state.astype(BF16))
        reach[0, at, lanes] = (query[at] * jnp.exp(cf + passed)).astype(BF16)
        last = cf[BLK - 1 : BLK]
        if b < count - 1:
            gain = mm_tn(value, (keys[at] * jnp.exp(last - cf)).astype(BF16))
            state = gain if b == 0 else jnp.exp(last) * state + gain
        passed = passed + last
        readers[b] = qr
    state = None
    passed = jnp.zeros((1, dk), F32)
    for b in reversed(range(count)):
        at = slice(b * BLK, (b + 1) * BLK)
        cb = cum[1, at, lanes]
        if b < count - 1:
            inner[b] = inner[b] + mm_nt(readers[b], state.astype(BF16))
        reach[1, at, lanes] = (query[at] * jnp.exp(cb + passed)).astype(BF16)
        last = cb[0:1]
        if b > 0:
            gain = mm_tn(values[at], (keys[at] * jnp.exp(last - cb)).astype(BF16))
            state = gain if b == count - 1 else jnp.exp(last) * state + gain
        passed = passed + last
        mixed[at, column : column + dv] = inner[b]


def ring_sum(y, c, cuts, part, prepare, s, r, ss, sr, finish):
    half = YN // 2

    def pass_sum(way, d, k):
        return remote(
            s.at[way, d - 1, k], r.at[way, d - 1, k], ss.at[way, d - 1, k], sr.at[way, d - 1, k],
            {"tp": lax.rem(y + step_of(way), YN) * 2 + c},
        )

    def order(way):
        mine = [k for k in range(cuts) if k // (cuts // 2) == way]
        return mine, [k for k in range(cuts) if k not in mine]

    def send(way, d, k):
        total = part(d if way == 0 else YN - d, k)
        if d < half and carried(way, d + 1, k, cuts):
            pass_sum(way, d + 1, k).wait_recv()
            total = total + r[way, d, k].astype(F32)
        s[way, d - 1, k] = total.astype(BF16)
        pass_sum(way, d, k).start()

    prepare(half)
    for turn in range(cuts // 2):
        for way in range(2):
            send(way, half, order(way)[0][turn])
    for d in range(half - 1, 0, -1):
        prepare(d)
        prepare(YN - d)
        for turn in range(cuts):
            for way in range(2):
                near_first, late = order(way)
                ks = late + near_first if d == half - 1 else near_first + late
                if d < half - 1 and half > 2:
                    ks = late + near_first
                send(way, d, ks[turn])
    prepare(0)
    for turn in range(cuts):
        k = (cuts // 2 * (turn % 2) + turn // 2) % cuts
        total = part(0, k)
        for way in range(2):
            if carried(way, 1, k, cuts):
                pass_sum(way, 1, k).wait_recv()
                total = total + r[way, 0, k].astype(F32)
        finish(k, total)

    def settle_sends():
        for way in range(2):
            for d in range(1, half + 1):
                for k in range(cuts):
                    if carried(way, d, k, cuts):
                        pass_sum(way, d, k).wait_send()

    return settle_sends


INPUTS = (
    "qa", "ka", "va", "ga", "da", "qb", "kb", "vb", "gb", "db", "head_gain", "pa", "pb", "stream",
    "gain_mix", "gain_moe", "routes", "affinity", "wg", "wu", "wd",
)


def shapes_of(rows, dv, width):
    n = ZN * XN
    m = YN * 2
    half = YN // 2
    own = rows // m
    lanes = width // m
    slots = 3 * rows * 2 // (2 * n)
    count = n // 2
    group = count * slots
    keys = DK_A + DK_B
    piece = dv // XN
    big = piece + FADES
    mine = rows // 2
    cut = width // CUTS
    v = pltpu.VMEM
    return dict(
        qa=v((DK_A, rows), BF16), ka=v((DK_A, rows), BF16), va=v((rows, dv), BF16), ga=v((rows, dv), BF16),
        da=v((2, DK_A, rows), F32), qb=v((rows, DK_B), BF16), kb=v((rows, DK_B), BF16), vb=v((rows, dv), BF16),
        gb=v((rows, dv), BF16), db=v((2, rows, DK_B), F32), head_gain=v((1, dv), F32),
        stream=v((own, width), BF16), gain_mix=v((1, width), F32), gain_moe=v((1, width), F32),
        routes=v((2, rows), jnp.int32), affinity=v((2, rows), F32),
        pj=v((2, 2, dv, width), BF16), wg=v((2, width, lanes), BF16), wu=v((2, width, lanes), BF16),
        wd=v((2, lanes, width), BF16), early=DMA((19,)), loads=DMA((3,)), swap_s=DMA((5,)), swap_r=DMA((5,)),
        cum=v((2, rows, keys), F32), stack=v((XN, 2, big, keys), BF16), xbox=v((XN, 2, big, keys), BF16),
        agg=v((2, big, keys), BF16), zbox=v((ZN, big, keys), BF16), outx=v((XN, 2, piece, keys), BF16),
        states=v((XN, 2, piece, keys), BF16), xs=DMA((XN,)), xr=DMA((XN,)), zs=DMA((ZN,)), zr=DMA((ZN,)),
        es=DMA((XN,)), er=DMA((XN,)),
        mixed=v((rows, 2 * dv), F32), reach=v((2, rows, keys), BF16), heads=v((2, mine, 2 * dv), BF16),
        hbox=v((mine, 2 * dv), BF16), hs=DMA((2,)), pp=v((YN, own, width), F32),
        s1=v((2, half, CUTS, own, cut), BF16), r1=v((2, half, CUTS, own, cut), BF16),
        s1s=DMA((2, half, CUTS)), s1r=DMA((2, half, CUTS)), settled=v((own, width), F32),
        moe_in=v((own, width), BF16), columns=v((rows, lanes), BF16), cs=DMA((m,)), cr=DMA((m,)),
        hot=v((n * slots, rows), BF16),
        mixhi=v((rows, n * slots), BF16), mixlo=v((rows, n * slots), BF16), picked=v((n, slots, lanes), BF16),
        x=v((YN, 2, count, slots, lanes), BF16), acc=v((group, 4 * lanes), F32), act=v((group, 2 * lanes), BF16),
        p=v((YN, group, 2 * lanes), F32), s2=v((2, half, 2, group, lanes), BF16),
        r2=v((2, half, 2, group, lanes), BF16), s2s=DMA((2, half, 2)), s2r=DMA((2, half, 2)),
        q=v((2, count, slots, lanes), BF16), pieces=v((n, slots, lanes), BF16), term=v((rows, lanes), BF16),
        mixture=v((own, width), BF16), ds=DMA((n,)), dr=DMA((2, count)), gs=DMA((2, half, 2)), gr=DMA((2, half, 2)),
        bs=DMA((2, count)), br=DMA((n,)), fs=DMA((m,)), fr=DMA((m,)),
    )


def layer_kernel(scratch_names, *refs):
    hbm = dict(zip(INPUTS, refs))
    out = refs[len(INPUTS)]
    v = dict(zip(scratch_names, refs[len(INPUTS) + 1 :]))
    sp = lax.axis_index("sp")
    tp = lax.axis_index("tp")
    z, xx, y, c = sp // XN, lax.rem(sp, XN), tp // 2, lax.rem(tp, 2)
    n = ZN * XN
    m = YN * 2
    half = YN // 2
    per = XN // 2
    picked, x, acc, act, p, q, pieces = (v[i] for i in ("picked", "x", "acc", "act", "p", "q", "pieces"))
    slots = picked.shape[1]
    count = ZN * per
    group = count * slots
    lanes = picked.shape[2]
    rows = v["columns"].shape[0]
    own = rows // m
    partner = {"tp": tp + 1 - 2 * c}

    def rows_of(i):
        return pl.ds(pl.multiple_of(i * own, own), own)

    def cols_of(i):
        return pl.ds(pl.multiple_of(i * lanes, lanes), lanes)

    barrier = pltpu.get_barrier_semaphore()
    greeted = 0
    for k in range(1, m):
        pl.semaphore_signal(barrier, inc=1, device_id={"tp": lax.rem(tp + k, m)}, device_id_type=MESH)
        greeted += 1
    for dz in range(ZN):
        for dx in range(XN):
            for core in range(2):
                if dz or dx:
                    peer = {"sp": sp_at(z, xx, dz, dx), "tp": y * 2 + core}
                    pl.semaphore_signal(barrier, inc=1, device_id=peer, device_id_type=MESH)
                    greeted += 1

    fetch = {}
    order = (
        "ka", "kb", "da", "db", "va", "vb", "qa", "qb", "ga", "gb", "head_gain", "routes", "affinity", "stream",
        "gain_mix", "gain_moe",
    )
    for i, name in enumerate(order):
        src = hbm[name].at[rows_of(tp), :] if name == "stream" else hbm[name]
        fetch[name] = pltpu.make_async_copy(src, v[name], v["early"].at[i])
        fetch[name].start()
    for i, name in enumerate(("pa", "pb")):
        fetch[name] = pltpu.make_async_copy(hbm[name], v["pj"].at[0, i], v["early"].at[len(order) + i])
        fetch[name].start()
    pairs = [(hbm[name].at[0], v[name]) for name in ("wg", "wu", "wd")]
    loads = [pltpu.make_async_copy(src, dst.at[0], v["loads"].at[i]) for i, (src, dst) in enumerate(pairs)]
    for load in loads:
        load.start()
    swaps = [
        remote(src, dst, v["swap_s"].at[i], v["swap_r"].at[i], partner)
        for i, (src, dst) in enumerate(
            [(hbm["pa"], v["pj"].at[1, 0]), (hbm["pb"], v["pj"].at[1, 1])] + [(s, d.at[1]) for s, d in pairs]
        )
    ]

    for name in ("ka", "kb", "da", "db", "va", "vb"):
        fetch[name].wait()
    cum, stack = v["cum"], v["stack"]
    keys_a = v["ka"][...].astype(F32).T
    keys_b = v["kb"][...].astype(F32)
    local_states(keys_a, v["va"][...], [v["da"][i].T for i in range(2)], 0, stack, cum)
    local_states(keys_b, v["vb"][...], [v["db"][i] for i in range(2)], DK_A, stack, cum)

    pl.semaphore_wait(barrier, greeted)

    xbox, agg, zbox, outx, states = (v[i] for i in ("xbox", "agg", "zbox", "outx", "states"))
    piece = outx.shape[2]

    def along_x(j):
        peer = lax.rem(xx + j, XN)
        return remote(stack.at[peer], xbox.at[xx], v["xs"].at[j], v["xr"].at[j], {"sp": z * XN + peer})

    def along_z(j):
        peer = lax.rem(z + j, ZN)
        way = jnp.where(peer > z, 0, 1)
        return remote(agg.at[way], zbox.at[z], v["zs"].at[j], v["zr"].at[j], {"sp": peer * XN + xx})

    def back_x(j):
        peer = lax.rem(xx + j, XN)
        return remote(outx.at[peer], states.at[xx], v["es"].at[j], v["er"].at[j], {"sp": z * XN + peer})

    far_x = sorted(range(1, XN), key=lambda j: -near(j, XN))
    far_z = sorted(range(1, ZN), key=lambda j: -near(j, ZN))
    for j in far_x:
        along_x(j).start()
    for swap in swaps:
        swap.start()
    xbox[xx] = stack[xx]
    zbox[z] = jnp.zeros_like(zbox[z])

    for name in ("qa", "qb"):
        fetch[name].wait()
    mixed, reach = v["mixed"], v["reach"]
    dv = v["va"].shape[1]
    local_mix(v["qa"][...].astype(F32).T, keys_a, v["va"][...], 0, cum, reach, 0, mixed)

    def load(block):
        block = block.astype(F32)
        return block[0:piece], block[piece : piece + 1] + block[piece + 1 : piece + 2]

    for j in range(1, XN):
        source = lax.rem(xx + XN - j, XN)
        remote(stack.at[source], xbox.at[source], v["xs"].at[j], v["xr"].at[j], {"sp": z * XN + source}).wait_recv()
    for way in range(2):
        state, fade = None, None
        for i in range(XN) if way == 0 else reversed(range(XN)):
            own_state, own_fade = load(xbox[i, way])
            state = own_state if state is None else jnp.exp(own_fade) * state + own_state
            fade = own_fade if fade is None else fade + own_fade
        agg[way, 0:piece] = state.astype(BF16)
        agg[way, piece : piece + FADES] = fade_rows(fade)
    for j in far_z:
        along_z(j).start()

    local_mix(v["qb"][...].astype(F32), keys_b, v["vb"][...], DK_A, cum, reach, dv, mixed)
    for name in ("routes", "affinity"):
        fetch[name].wait()
    routes, affinity = v["routes"][...], v["affinity"][...]
    lane = lax.broadcasted_iota(jnp.int32, (n, rows), 0)
    hots = [routes[i : i + 1] == lane for i in range(2)]
    named = sum(jnp.where(h, 1.0, 0.0) for h in hots)
    ii = lax.broadcasted_iota(jnp.int32, (rows, rows), 0)
    jj = lax.broadcasted_iota(jnp.int32, (rows, rows), 1)
    before = mm(named.astype(BF16), jnp.where(ii < jj, 1.0, 0.0).astype(BF16))
    place = [
        routes[i : i + 1] * slots
        + jnp.sum(jnp.where(hots[i], before, 0.0), axis=0, keepdims=True).astype(jnp.int32)
        for i in range(2)
    ]
    seat = lax.broadcasted_iota(jnp.int32, (n * slots, rows), 0)
    v["hot"][...] = jnp.where((seat == place[0]) | (seat == place[1]), 1.0, 0.0).astype(BF16)
    weights = [affinity[i : i + 1] / (affinity[0:1] + affinity[1:2]) for i in range(2)]
    mix = jnp.where(seat == place[0], weights[0], jnp.where(seat == place[1], weights[1], 0.0)).T
    high = mix.astype(BF16)
    v["mixhi"][...] = high
    v["mixlo"][...] = (mix - high.astype(F32)).astype(BF16)

    for j in range(1, ZN):
        source = lax.rem(z + ZN - j, ZN)
        remote(agg.at[0], zbox.at[source], v["zs"].at[j], v["zr"].at[j], {"sp": source * XN + xx}).wait_recv()
    keys = zbox.shape[2]
    ahead = jnp.zeros((piece, keys), F32)
    behind = jnp.zeros((piece, keys), F32)
    for i in range(ZN):
        state, fade = load(zbox[i])
        ahead = jnp.where(i < z, jnp.exp(fade) * ahead + state, ahead)
    for i in reversed(range(ZN)):
        state, fade = load(zbox[i])
        behind = jnp.where(i > z, jnp.exp(fade) * behind + state, behind)
    for i in range(XN):
        outx[i, 0] = ahead.astype(BF16)
        if i < XN - 1:
            state, fade = load(xbox[i, 0])
            ahead = jnp.exp(fade) * ahead + state
    for i in reversed(range(XN)):
        outx[i, 1] = behind.astype(BF16)
        if i > 0:
            state, fade = load(xbox[i, 1])
            behind = jnp.exp(fade) * behind + state
    for j in far_x:
        back_x(j).start()
    states[xx] = outx[xx]
    for name in ("ga", "gb", "head_gain", "pa", "pb", "stream", "gain_mix", "gain_moe"):
        fetch[name].wait()
    for j in range(1, XN):
        source = lax.rem(xx + XN - j, XN)
        remote(outx.at[source], states.at[source], v["es"].at[j], v["er"].at[j], {"sp": z * XN + source}).wait_recv()

    heads, hbox = v["heads"], v["hbox"]
    for i, (base, dk, gate) in enumerate(((0, DK_A, v["ga"]), (DK_A, DK_B, v["gb"]))):
        at = slice(base, base + dk)
        whole = mixed[:, i * dv : (i + 1) * dv]
        for way in range(2):
            start = states[:, way].reshape(dv, keys)
            whole = whole + mm_nt(reach[way, :, at], start[:, at])
        scale = lax.rsqrt(jnp.mean(whole * whole, axis=-1, keepdims=True) + 1e-06)
        value = (whole * scale * v["head_gain"][...] * silu(gate[...].astype(F32))).astype(BF16)
        value = value.reshape(YN, 2, own, dv)
        for core in range(2):
            heads[core, :, i * dv : (i + 1) * dv] = value[:, core].reshape(YN * own, dv)
    hand = remote(heads.at[1 - c], hbox, v["hs"].at[0], v["hs"].at[1], partner)
    hand.start()
    pj, pp = v["pj"], v["pp"]
    pp[...] = (mm(heads[c], pj[0].reshape(2 * dv, pj.shape[3]))).reshape(pp.shape)
    swaps[0].wait_recv()
    swaps[1].wait_recv()
    hand.wait_recv()
    pp[...] = pp[...] + (mm(hbox[...], pj[1].reshape(2 * dv, pj.shape[3]))).reshape(pp.shape)

    settled, moe_in, columns = v["settled"], v["moe_in"], v["columns"]
    cut = v["s1"].shape[4]

    def attn_part(o, k):
        return pp[lax.rem(y + o, YN), :, k * cut : (k + 1) * cut]

    def attn_done(k, total):
        settled[:, k * cut : (k + 1) * cut] = total

    sent_attn = ring_sum(
        y, c, CUTS, attn_part, lambda o: None, v["s1"], v["r1"], v["s1s"], v["s1r"], attn_done
    )
    value = layer_norm(v["stream"][...].astype(F32) + settled[...], v["gain_mix"][...])
    settled[...] = value
    moe_in[...] = value.astype(BF16)

    far_tp = sorted(range(1, m), key=lambda k: -near(k // 2, YN))

    def to_columns(k):
        peer = lax.rem(tp + k, m)
        return remote(moe_in.at[:, cols_of(peer)], columns.at[rows_of(tp), :], v["cs"].at[k], v["cr"].at[k], {"tp": peer})

    for k in far_tp:
        to_columns(k).start()
    columns[rows_of(tp), :] = moe_in[:, cols_of(tp)]
    for k in range(1, m):
        source = lax.rem(tp + m - k, m)
        remote(
            moe_in.at[:, cols_of(source)], columns.at[rows_of(source), :], v["cs"].at[k], v["cr"].at[k], {"tp": source}
        ).wait_recv()
    picked[...] = mm(v["hot"][...], columns[...]).astype(BF16).reshape(picked.shape)

    def dispatch(dz, dx):
        e = sp_at(z, xx, dz, dx)
        rz, rx = (-dz) % ZN, (-dx) % XN
        j = rz * per + rx // 2
        return remote(
            picked.at[e], x.at[y, c, j], v["ds"].at[dz * XN + dx], v["dr"].at[c, j], {"sp": e, "tp": y * 2 + dx % 2}
        )

    home = pltpu.make_async_copy(picked.at[sp], x.at[y, 0, 0], v["dr"].at[0, 0])
    offsets = sorted(
        [(dz, dx) for dz in range(ZN) for dx in range(XN)],
        key=lambda o: -(near(o[0], ZN) + near(o[1], XN)),
    )
    for dz, dx in offsets:
        if dz or dx:
            dispatch(dz, dx).start()
    pl.when(c == 0)(lambda: home.start())
    pl.when(c == 1)(lambda: dispatch(0, 0).start())

    def arrive(k, j):
        remote(picked.at[0], x.at[y, k, j], v["ds"].at[0], v["dr"].at[k, j], partner).wait_recv()

    def hop(way, h, k, behind=0):
        step = step_of(way)
        b = lax.rem(y + (h - 1 + behind) * (YN - step), YN)
        return remote(
            x.at[b, k], x.at[b, k], v["gs"].at[way, h - 1, k], v["gr"].at[way, h - 1, k],
            {"tp": lax.rem(y + step, YN) * 2 + c},
        )

    wg, wu, wd = v["wg"], v["wu"], v["wd"]

    def widen(b, first=False):
        at = pl.ds(pl.multiple_of(b * 2 * lanes, 2 * lanes), 2 * lanes)
        block = jnp.concatenate([x[b, k].reshape(group, lanes) for k in range(2)], axis=1)
        w = jnp.concatenate([ref[i, at, :] for ref in (wg, wu) for i in range(2)], axis=1)
        value = mm(block, w)
        acc[...] = value if first else acc[...] + value

    for k in range(2):
        for j in range(count):
            if k == 0 and j == 0:
                pl.when(c == 0)(lambda: home.wait())
                pl.when(c == 1)(lambda: arrive(0, 0))
            else:
                arrive(k, j)
        for way in range(2):
            if carried(way, 1, k, 2):
                hop(way, 1, k).start()
    for load_w in loads:
        load_w.wait()
    for swap in swaps[2:]:
        swap.wait_recv()
    widen(y, first=True)
    for h in range(1, half + 1):
        for k in range(2):
            for way in range(2):
                if carried(way, h, k, 2):
                    hop(way, h, k, 1).wait_recv()
                    if h < half and carried(way, h + 1, k, 2):
                        hop(way, h + 1, k).start()
        widen(lax.rem(y + YN - h, YN))
        if h < half:
            widen(lax.rem(y + h, YN))

    hidden = 2 * lanes
    act[...] = (silu(acc[:, :hidden]) * acc[:, hidden:]).astype(BF16)

    def narrow(o):
        b = lax.rem(y + o, YN)
        at = pl.ds(pl.multiple_of(b * hidden, hidden), hidden)
        p[o] = mm(act[...], jnp.concatenate([wd[i, :, at] for i in range(2)], axis=0))

    def give(k, j):
        rz = j // per
        rx = 2 * (j % per) + c
        o = ((-rz) % ZN) * XN + lax.rem(XN - rx, XN)
        return remote(
            q.at[k, j], pieces.at[sp], v["bs"].at[k, j], v["br"].at[o], {"sp": sp_at(z, xx, rz, rx), "tp": y * 2 + k}
        )

    back = pltpu.make_async_copy(q.at[0, 0], pieces.at[sp], v["br"].at[0])
    far_j = sorted(range(count), key=lambda j: -near(j // per, ZN))

    def moe_done(k, total):
        q[k] = total.astype(BF16).reshape(count, slots, lanes)
        for j in far_j:
            if k == 0 and j == 0:
                pl.when(c == 0)(lambda: back.start())
                pl.when(c == 1)(lambda: give(0, 0).start())
            else:
                give(k, j).start()

    sent_moe = ring_sum(
        y, c, 2, lambda o, k: p[o, :, k * lanes : (k + 1) * lanes], narrow, v["s2"], v["r2"], v["s2s"], v["s2r"],
        moe_done,
    )
    for dz in range(ZN):
        for dx in range(XN):
            o = dz * XN + dx
            e = sp_at(z, xx, dz, dx)
            coming = remote(q.at[0, 0], pieces.at[e], v["bs"].at[0, 0], v["br"].at[o], partner)
            if o == 0:
                pl.when(c == 0)(lambda: back.wait())
                pl.when(c == 1)(lambda: coming.wait_recv())
            else:
                coming.wait_recv()

    term, mixture = v["term"], v["mixture"]
    flat = pieces[...].reshape(n * slots, lanes)
    term[...] = (mm(v["mixhi"][...], flat) + mm(v["mixlo"][...], flat)).astype(BF16)

    def spread_rows(k):
        peer = lax.rem(tp + k, m)
        return remote(term.at[rows_of(peer), :], mixture.at[:, cols_of(tp)], v["fs"].at[k], v["fr"].at[k], {"tp": peer})

    for k in far_tp:
        spread_rows(k).start()
    mixture[:, cols_of(tp)] = term[rows_of(tp), :]
    for k in range(1, m):
        source = lax.rem(tp + m - k, m)
        remote(
            term.at[rows_of(source), :], mixture.at[:, cols_of(source)], v["fs"].at[k], v["fr"].at[k], {"tp": source}
        ).wait_recv()
    out[...] = layer_norm(settled[...] + mixture[...].astype(F32), v["gain_moe"][...]).astype(BF16)

    for j in range(1, XN):
        along_x(j).wait_send()
        back_x(j).wait_send()
    for j in range(1, ZN):
        along_z(j).wait_send()
    hand.wait_send()
    for swap in swaps:
        swap.wait_send()
    sent_attn()
    for k in range(1, m):
        to_columns(k).wait_send()
        spread_rows(k).wait_send()
    for dz, dx in offsets:
        if dz or dx:
            dispatch(dz, dx).wait_send()
    pl.when(c == 1)(lambda: dispatch(0, 0).wait_send())
    for way in range(2):
        for h in range(1, half + 1):
            for k in range(2):
                if carried(way, h, k, 2):
                    hop(way, h, k).wait_send()
    sent_moe()
    for k in range(2):
        for j in range(count):
            if k == 0 and j == 0:
                pl.when(c == 1)(lambda: give(0, 0).wait_send())
            else:
                give(k, j).wait_send()


def body(
    query_one, key_one, value_one, gate_one, decay_one, query_two, key_two, value_two, gate_two, decay_two,
    head_gain, proj_one, proj_two, stream, gain_mix, gain_moe, routes, affinity, expert_gate, expert_up,
    expert_down,
):
    rows, width = stream.shape
    dv = head_gain.shape[0]
    scratch = shapes_of(rows, dv, width)
    return pl.pallas_call(
        functools.partial(layer_kernel, tuple(scratch)),
        out_shape=jax.ShapeDtypeStruct((rows // (YN * 2), width), BF16),
        in_specs=[ANY] * len(INPUTS),
        out_specs=VMEM,
        scratch_shapes=list(scratch.values()),
        compiler_params=pltpu.CompilerParams(
            vmem_limit_bytes=56 * 2**20, collective_id=1, has_side_effects=True
        ),
    )(
        query_one.T, key_one.T, value_one, gate_one, jnp.swapaxes(decay_one, 1, 2), query_two, key_two, value_two,
        gate_two, decay_two, head_gain.reshape(1, -1), proj_one, proj_two, stream, gain_mix.reshape(1, -1),
        gain_moe.reshape(1, -1), routes.T, affinity.T, expert_gate, expert_up, expert_down,
    )


def solution(mesh):
    return jax.shard_map(
        body,
        mesh=mesh,
        in_specs=(
            P("sp", "tp"),
            P("sp", "tp"),
            P("sp", "tp"),
            P("sp", "tp"),
            P(None, "sp", "tp"),
            P("sp", "tp"),
            P("sp", "tp"),
            P("sp", "tp"),
            P("sp", "tp"),
            P(None, "sp", "tp"),
            P(),
            P("tp", None),
            P("tp", None),
            P("sp", None),
            P(),
            P(),
            P("sp", None),
            P("sp", None),
            P("sp", None, "tp"),
            P("sp", None, "tp"),
            P("sp", "tp", None),
        ),
        out_specs=P(("sp", "tp"), None),
        check_vma=False,
    )
```

```python
import functools

import jax
import jax.numpy as jnp
from jax import lax
from jax.experimental import pallas as pl
from jax.experimental.pallas import tpu as pltpu
from jax.sharding import PartitionSpec as P

DK_A = 64
DK_B = 128
BLK = 64
SHARPNESS = 16.0
ZN, XN, YN = 8, 4, 8
CUTS = 4
GROUPS = 4
FADES = 8
F32 = jnp.float32
BF16 = jnp.bfloat16
MESH = pl.DeviceIdType.MESH
VMEM = pl.BlockSpec(memory_space=pltpu.VMEM)
ANY = pl.BlockSpec(memory_space=pl.ANY)
DMA = pltpu.SemaphoreType.DMA


def mm(a, b):
    return jnp.dot(a, b, preferred_element_type=F32)


def mm_nt(a, b):
    return lax.dot_general(a, b, (((1,), (1,)), ((), ())), preferred_element_type=F32)


def mm_tn(a, b):
    return lax.dot_general(a, b, (((0,), (0,)), ((), ())), preferred_element_type=F32)


def log_sigmoid(x):
    return jnp.minimum(x, 0.0) - jnp.log1p(jnp.exp(-jnp.abs(x)))


def silu(x):
    return x / (1.0 + jnp.exp(-x))


def layer_norm(values, gain):
    mean = jnp.mean(values, axis=-1, keepdims=True)
    spread = jnp.mean(jnp.square(values - mean), axis=-1, keepdims=True)
    return (values - mean) * lax.rsqrt(spread + 1e-05) * gain


def remote(src, dst, send, recv, peer):
    return pltpu.make_async_remote_copy(
        src_ref=src, dst_ref=dst, send_sem=send, recv_sem=recv, device_id=peer, device_id_type=MESH
    )


def sp_at(z, x, dz, dx):
    return lax.rem(z + dz, ZN) * XN + lax.rem(x + dx, XN)


def near(d, n):
    return min(d, n - d)


def step_of(way):
    return 1 if way == 0 else YN - 1


def fade_rows(total):
    wide = total.shape[1]
    row = lax.broadcasted_iota(jnp.int32, (FADES, wide), 0)
    high = total.astype(BF16).astype(F32)
    return jnp.where(row == 0, high, jnp.where(row == 1, total - high, 0.0)).astype(BF16)


def local_states(keys, values, decays, base, stack, cum):
    rows, wide = keys.shape
    count = rows // BLK
    dv = values.shape[1]
    piece = dv // XN
    ii = lax.broadcasted_iota(jnp.int32, (rows, rows), 0)
    jj = lax.broadcasted_iota(jnp.int32, (rows, rows), 1)
    same = (ii // BLK) == (jj // BLK)
    for way in range(2):
        tri = jnp.where(same & ((ii >= jj) if way == 0 else (ii <= jj)), 1.0, 0.0).astype(BF16)
        fade = log_sigmoid(decays[way]) / SHARPNESS
        high = fade.astype(BF16)
        low = (fade - high.astype(F32)).astype(BF16)
        total = mm(tri, high) + mm(tri, low)
        cum[way, :, base : base + wide] = total
        tail = jnp.zeros((1, wide), F32)
        weighted = [None] * count
        for b in reversed(range(count)) if way == 0 else range(count):
            part = total[b * BLK : (b + 1) * BLK]
            last = part[BLK - 1 : BLK] if way == 0 else part[0:1]
            weighted[b] = (keys[b * BLK : (b + 1) * BLK] * jnp.exp(last - part + tail)).astype(BF16)
            tail = tail + last
        state = mm_tn(values, jnp.concatenate(weighted, axis=0)).astype(BF16)
        fades = fade_rows(tail)
        for i in range(XN):
            stack[i, way, 0:piece, base : base + wide] = state[i * piece : (i + 1) * piece]
            stack[i, way, piece : piece + FADES, base : base + wide] = fades


def local_mix(query, keys, values, base, cum, reach, column, mixed):
    rows, dk = keys.shape
    count = rows // BLK
    dv = values.shape[1]
    ii = lax.broadcasted_iota(jnp.int32, (BLK, BLK), 0)
    jj = lax.broadcasted_iota(jnp.int32, (BLK, BLK), 1)
    lanes = slice(base, base + dk)
    query = query * dk ** (-0.5)
    inner = [None] * count
    readers = [None] * count
    state = None
    passed = jnp.zeros((1, dk), F32)
    for b in range(count):
        at = slice(b * BLK, (b + 1) * BLK)
        value = values[at]
        cf = cum[0, at, lanes]
        cb = cum[1, at, lanes]
        qf = (query[at] * jnp.exp(cf)).astype(BF16)
        kf = (keys[at] * jnp.exp(-cf)).astype(BF16)
        qr = (query[at] * jnp.exp(cb)).astype(BF16)
        kr = (keys[at] * jnp.exp(-cb)).astype(BF16)
        scores = jnp.where(ii >= jj, mm_nt(qf, kf), 0.0) + jnp.where(ii <= jj, mm_nt(qr, kr), 0.0)
        inner[b] = mm(scores.astype(BF16), value)
        if b > 0:
            inner[b] = inner[b] + mm_nt(qf, state.astype(BF16))
        reach[0, at, lanes] = (query[at] * jnp.exp(cf + passed)).astype(BF16)
        last = cf[BLK - 1 : BLK]
        if b < count - 1:
            gain = mm_tn(value, (keys[at] * jnp.exp(last - cf)).astype(BF16))
            state = gain if b == 0 else jnp.exp(last) * state + gain
        passed = passed + last
        readers[b] = qr
    state = None
    passed = jnp.zeros((1, dk), F32)
    for b in reversed(range(count)):
        at = slice(b * BLK, (b + 1) * BLK)
        cb = cum[1, at, lanes]
        if b < count - 1:
            inner[b] = inner[b] + mm_nt(readers[b], state.astype(BF16))
        reach[1, at, lanes] = (query[at] * jnp.exp(cb + passed)).astype(BF16)
        last = cb[0:1]
        if b > 0:
            gain = mm_tn(values[at], (keys[at] * jnp.exp(last - cb)).astype(BF16))
            state = gain if b == count - 1 else jnp.exp(last) * state + gain
        passed = passed + last
        mixed[at, column : column + dv] = inner[b]


def ring_sum(y, c, order, jump, part, prepare, extra, s, r, ss, sr, finish):
    half = YN // 2
    started = []

    def mine(way, k):
        return k // (len(order) // 2) == way

    def pass_sum(way, d, k):
        step = jump if d == half else 1
        return remote(
            s.at[way, d - 1, k], r.at[way, d - 1, k], ss.at[way, d - 1, k], sr.at[way, d - 1, k],
            {"tp": lax.rem(y + (step if way == 0 else YN - step), YN) * 2 + c},
        )

    def collect(total, way, d, k):
        if d + 1 < half:
            pass_sum(way, d + 1, k).wait_recv()
            total = total + r[way, d, k].astype(F32)
        if jump and mine(way, k) and half - jump == d:
            pass_sum(way, half, k).wait_recv()
            total = total + r[way, half - 1, k].astype(F32)
        return total

    def send(way, d, k):
        s[way, d - 1, k] = collect(part(d if way == 0 else YN - d, k), way, d, k).astype(BF16)
        copy = pass_sum(way, d, k)
        copy.start()
        started.append(copy)

    if jump:
        prepare(half)
        for k in order:
            for way in range(2):
                if mine(way, k):
                    send(way, half, k)
    for d in range(half - 1, 0, -1):
        prepare(d)
        prepare(YN - d)
        for k in order:
            for way in range(2):
                send(way, d, k)
        if d == half - 1:
            extra()
    if half == 1:
        extra()
    prepare(0)
    for k in order:
        total = part(0, k)
        for way in range(2):
            total = collect(total, way, 0, k)
        finish(k, total)
    return started


INPUTS = (
    "qa", "ka", "va", "ga", "da", "qb", "kb", "vb", "gb", "db", "head_gain", "pa", "pb", "stream",
    "gain_mix", "gain_moe", "routes", "affinity", "wg", "wu", "wd",
)


def shapes_of(rows, dv, width):
    n = ZN * XN
    m = YN * 2
    half = YN // 2
    own = rows // m
    lanes = width // m
    slots = 3 * rows * 2 // (2 * n)
    count = n // 2
    group = count * slots
    keys = DK_A + DK_B
    piece = dv // XN
    big = piece + FADES
    mine = rows // 2
    groups = min(GROUPS, count)
    hops = max(1, half - 1)
    cut = width // CUTS
    v = pltpu.VMEM
    return dict(
        qa=v((DK_A, rows), BF16), ka=v((DK_A, rows), BF16), va=v((rows, dv), BF16), ga=v((rows, dv), BF16),
        da=v((2, DK_A, rows), F32), qb=v((rows, DK_B), BF16), kb=v((rows, DK_B), BF16), vb=v((rows, dv), BF16),
        gb=v((rows, dv), BF16), db=v((2, rows, DK_B), F32), head_gain=v((1, dv), F32),
        stream=v((own, width), BF16), gain_mix=v((1, width), F32), gain_moe=v((1, width), F32),
        routes=v((2, rows), jnp.int32), affinity=v((2, rows), F32),
        pj=v((2, 2, dv, width), BF16), wg=v((2, width, lanes), BF16), wu=v((2, width, lanes), BF16),
        wd=v((2, lanes, width), BF16), early=DMA((19,)), loads=DMA((3,)), swap_s=DMA((5,)), swap_r=DMA((5,)),
        cum=v((2, rows, keys), F32), stack=v((XN, 2, big, keys), BF16), xbox=v((XN, 2, big, keys), BF16),
        agg=v((2, big, keys), BF16), zbox=v((ZN, big, keys), BF16), outx=v((XN, 2, piece, keys), BF16),
        states=v((XN, 2, piece, keys), BF16), xs=DMA((XN,)), xr=DMA((XN,)), zs=DMA((ZN,)), zr=DMA((ZN,)),
        es=DMA((XN,)), er=DMA((XN,)),
        mixed=v((rows, 2 * dv), F32), reach=v((2, rows, keys), BF16), heads=v((2, mine, 2 * dv), BF16),
        hbox=v((mine, 2 * dv), BF16), hs=DMA((2,)), pp=v((YN, own, width), F32),
        s1=v((2, half, CUTS, own, cut), BF16), r1=v((2, half, CUTS, own, cut), BF16),
        s1s=DMA((2, half, CUTS)), s1r=DMA((2, half, CUTS)), settled=v((own, width), F32),
        moe_in=v((2, YN, own, lanes), BF16), columns=v((2, rows, lanes), BF16), cs=DMA((m,)), cr=DMA((m,)),
        hot=v((n * slots, rows), BF16),
        mixhi=v((rows, n * slots), BF16), mixlo=v((rows, n * slots), BF16), picked=v((2, n, slots, lanes), BF16),
        x=v((YN, groups, 2, count // groups, slots, lanes), BF16), acc=v((group, 4 * lanes), F32),
        act=v((group, 2 * lanes), BF16), p=v((YN, group, 2 * lanes), F32),
        s2=v((2, hops, groups, group // groups, 2 * lanes), BF16),
        r2=v((2, hops, groups, group // groups, 2 * lanes), BF16), s2s=DMA((2, hops, groups)),
        s2r=DMA((2, hops, groups)), q=v((2, 2, count, slots, lanes), BF16), pieces=v((2, n, slots, lanes), BF16),
        term=v((2, rows, lanes), BF16), mixbox=v((m, 2, own, lanes), BF16), ds=DMA((2, n)), dr=DMA((2, 2, count)),
        gs=DMA((2, hops, groups)), gr=DMA((2, hops, groups)), bs=DMA((2, 2, count)), br=DMA((2, n)),
        fs=DMA((m,)), fr=DMA((m,)),
    )


def layer_kernel(scratch_names, *refs):
    hbm = dict(zip(INPUTS, refs))
    out = refs[len(INPUTS)]
    v = dict(zip(scratch_names, refs[len(INPUTS) + 1 :]))
    sp = lax.axis_index("sp")
    tp = lax.axis_index("tp")
    z, xx, y, c = sp // XN, lax.rem(sp, XN), tp // 2, lax.rem(tp, 2)
    n = ZN * XN
    m = YN * 2
    half = YN // 2
    per = XN // 2
    picked, x, acc, act, p, q, pieces = (v[i] for i in ("picked", "x", "acc", "act", "p", "q", "pieces"))
    slots = picked.shape[2]
    count = ZN * per
    group = count * slots
    lanes = picked.shape[3]
    groups = x.shape[1]
    size = count // groups
    rows = v["columns"].shape[1]
    own = rows // m
    partner = {"tp": tp + 1 - 2 * c}

    def rows_of(i):
        return pl.ds(pl.multiple_of(i * own, own), own)

    barrier = pltpu.get_barrier_semaphore()
    greeted = 0
    for k in range(1, m):
        pl.semaphore_signal(barrier, inc=1, device_id={"tp": lax.rem(tp + k, m)}, device_id_type=MESH)
        greeted += 1
    for dz in range(ZN):
        for dx in range(XN):
            for core in range(2):
                if dz or dx:
                    peer = {"sp": sp_at(z, xx, dz, dx), "tp": y * 2 + core}
                    pl.semaphore_signal(barrier, inc=1, device_id=peer, device_id_type=MESH)
                    greeted += 1

    fetch = {}
    order = (
        "ka", "kb", "da", "db", "va", "vb", "qa", "qb", "ga", "gb", "head_gain", "routes", "affinity", "stream",
        "gain_mix", "gain_moe",
    )
    for i, name in enumerate(order):
        src = hbm[name].at[rows_of(tp), :] if name == "stream" else hbm[name]
        fetch[name] = pltpu.make_async_copy(src, v[name], v["early"].at[i])
        fetch[name].start()
    for i, name in enumerate(("pa", "pb")):
        fetch[name] = pltpu.make_async_copy(hbm[name], v["pj"].at[0, i], v["early"].at[len(order) + i])
        fetch[name].start()
    pairs = [(hbm[name].at[0], v[name]) for name in ("wg", "wu", "wd")]
    loads = [pltpu.make_async_copy(src, dst.at[0], v["loads"].at[i]) for i, (src, dst) in enumerate(pairs)]
    for load in loads:
        load.start()
    swaps = [
        remote(src, dst, v["swap_s"].at[i], v["swap_r"].at[i], partner)
        for i, (src, dst) in enumerate(
            [(hbm["pa"], v["pj"].at[1, 0]), (hbm["pb"], v["pj"].at[1, 1])] + [(s, d.at[1]) for s, d in pairs]
        )
    ]

    for name in ("ka", "kb", "da", "db", "va", "vb"):
        fetch[name].wait()
    cum, stack = v["cum"], v["stack"]
    keys_a = v["ka"][...].astype(F32).T
    keys_b = v["kb"][...].astype(F32)
    local_states(keys_a, v["va"][...], [v["da"][i].T for i in range(2)], 0, stack, cum)
    local_states(keys_b, v["vb"][...], [v["db"][i] for i in range(2)], DK_A, stack, cum)

    pl.semaphore_wait(barrier, greeted)

    xbox, agg, zbox, outx, states = (v[i] for i in ("xbox", "agg", "zbox", "outx", "states"))
    piece = outx.shape[2]

    def along_x(j):
        peer = lax.rem(xx + j, XN)
        return remote(stack.at[peer], xbox.at[xx], v["xs"].at[j], v["xr"].at[j], {"sp": z * XN + peer})

    def along_z(j):
        peer = lax.rem(z + j, ZN)
        way = jnp.where(peer > z, 0, 1)
        return remote(agg.at[way], zbox.at[z], v["zs"].at[j], v["zr"].at[j], {"sp": peer * XN + xx})

    def back_x(j):
        peer = lax.rem(xx + j, XN)
        return remote(outx.at[peer], states.at[xx], v["es"].at[j], v["er"].at[j], {"sp": z * XN + peer})

    far_x = sorted(range(1, XN), key=lambda j: -near(j, XN))
    far_z = sorted(range(1, ZN), key=lambda j: -near(j, ZN))
    for j in far_x:
        along_x(j).start()
    for swap in swaps:
        swap.start()
    xbox[xx] = stack[xx]
    zbox[z] = jnp.zeros_like(zbox[z])

    for name in ("qa", "qb"):
        fetch[name].wait()
    mixed, reach = v["mixed"], v["reach"]
    dv = v["va"].shape[1]
    local_mix(v["qa"][...].astype(F32).T, keys_a, v["va"][...], 0, cum, reach, 0, mixed)

    def load(block):
        block = block.astype(F32)
        return block[0:piece], block[piece : piece + 1] + block[piece + 1 : piece + 2]

    for j in range(1, XN):
        source = lax.rem(xx + XN - j, XN)
        remote(stack.at[source], xbox.at[source], v["xs"].at[j], v["xr"].at[j], {"sp": z * XN + source}).wait_recv()
    for way in range(2):
        state, fade = None, None
        for i in range(XN) if way == 0 else reversed(range(XN)):
            own_state, own_fade = load(xbox[i, way])
            state = own_state if state is None else jnp.exp(own_fade) * state + own_state
            fade = own_fade if fade is None else fade + own_fade
        agg[way, 0:piece] = state.astype(BF16)
        agg[way, piece : piece + FADES] = fade_rows(fade)
    for j in far_z:
        along_z(j).start()

    local_mix(v["qb"][...].astype(F32), keys_b, v["vb"][...], DK_A, cum, reach, dv, mixed)
    for name in ("routes", "affinity"):
        fetch[name].wait()
    routes, affinity = v["routes"][...], v["affinity"][...]
    lane = lax.broadcasted_iota(jnp.int32, (n, rows), 0)
    hots = [routes[i : i + 1] == lane for i in range(2)]
    named = sum(jnp.where(h, 1.0, 0.0) for h in hots)
    ii = lax.broadcasted_iota(jnp.int32, (rows, rows), 0)
    jj = lax.broadcasted_iota(jnp.int32, (rows, rows), 1)
    before = mm(named.astype(BF16), jnp.where(ii < jj, 1.0, 0.0).astype(BF16))
    place = [
        routes[i : i + 1] * slots
        + jnp.sum(jnp.where(hots[i], before, 0.0), axis=0, keepdims=True).astype(jnp.int32)
        for i in range(2)
    ]
    seat = lax.broadcasted_iota(jnp.int32, (n * slots, rows), 0)
    v["hot"][...] = jnp.where((seat == place[0]) | (seat == place[1]), 1.0, 0.0).astype(BF16)
    weights = [affinity[i : i + 1] / (affinity[0:1] + affinity[1:2]) for i in range(2)]
    mix = jnp.where(seat == place[0], weights[0], jnp.where(seat == place[1], weights[1], 0.0)).T
    high = mix.astype(BF16)
    v["mixhi"][...] = high
    v["mixlo"][...] = (mix - high.astype(F32)).astype(BF16)

    for j in range(1, ZN):
        source = lax.rem(z + ZN - j, ZN)
        remote(agg.at[0], zbox.at[source], v["zs"].at[j], v["zr"].at[j], {"sp": source * XN + xx}).wait_recv()
    keys = zbox.shape[2]
    ahead = jnp.zeros((piece, keys), F32)
    behind = jnp.zeros((piece, keys), F32)
    for i in range(ZN):
        state, fade = load(zbox[i])
        ahead = jnp.where(i < z, jnp.exp(fade) * ahead + state, ahead)
    for i in reversed(range(ZN)):
        state, fade = load(zbox[i])
        behind = jnp.where(i > z, jnp.exp(fade) * behind + state, behind)
    for i in range(XN):
        outx[i, 0] = ahead.astype(BF16)
        if i < XN - 1:
            state, fade = load(xbox[i, 0])
            ahead = jnp.exp(fade) * ahead + state
    for i in reversed(range(XN)):
        outx[i, 1] = behind.astype(BF16)
        if i > 0:
            state, fade = load(xbox[i, 1])
            behind = jnp.exp(fade) * behind + state
    for j in far_x:
        back_x(j).start()
    states[xx] = outx[xx]
    for name in ("ga", "gb", "head_gain", "pa", "pb", "stream", "gain_mix", "gain_moe"):
        fetch[name].wait()
    for j in range(1, XN):
        source = lax.rem(xx + XN - j, XN)
        remote(outx.at[source], states.at[source], v["es"].at[j], v["er"].at[j], {"sp": z * XN + source}).wait_recv()

    heads, hbox = v["heads"], v["hbox"]
    for i, (base, dk, gate) in enumerate(((0, DK_A, v["ga"]), (DK_A, DK_B, v["gb"]))):
        at = slice(base, base + dk)
        whole = mixed[:, i * dv : (i + 1) * dv]
        for way in range(2):
            start = states[:, way].reshape(dv, keys)
            whole = whole + mm_nt(reach[way, :, at], start[:, at])
        scale = lax.rsqrt(jnp.mean(whole * whole, axis=-1, keepdims=True) + 1e-06)
        value = (whole * scale * v["head_gain"][...] * silu(gate[...].astype(F32))).astype(BF16)
        value = value.reshape(YN, 2, own, dv)
        for core in range(2):
            heads[core, :, i * dv : (i + 1) * dv] = value[:, core].reshape(YN * own, dv)
    hand = remote(heads.at[1 - c], hbox, v["hs"].at[0], v["hs"].at[1], partner)
    hand.start()
    pj, pp = v["pj"], v["pp"]
    pp[...] = (mm(heads[c], pj[0].reshape(2 * dv, pj.shape[3]))).reshape(pp.shape)
    swaps[0].wait_recv()
    swaps[1].wait_recv()
    hand.wait_recv()
    pp[...] = pp[...] + (mm(hbox[...], pj[1].reshape(2 * dv, pj.shape[3]))).reshape(pp.shape)

    settled, moe_in, columns = v["settled"], v["moe_in"], v["columns"]
    cut = v["s1"].shape[4]

    def attn_part(o, k):
        return pp[lax.rem(y + o, YN), :, k * cut : (k + 1) * cut]

    def attn_done(k, total):
        settled[:, k * cut : (k + 1) * cut] = total

    sent = ring_sum(
        y, c, [k // 2 + CUTS // 2 * (k % 2) for k in range(CUTS)], min(2, half), attn_part, lambda o: None,
        lambda: None, v["s1"], v["r1"], v["s1s"], v["s1r"], attn_done,
    )
    value = layer_norm(v["stream"][...].astype(F32) + settled[...], v["gain_mix"][...])
    settled[...] = value
    value = value.astype(BF16)
    for i in range(m):
        moe_in[i // YN, i % YN] = value[:, i * lanes : (i + 1) * lanes]

    far_tp = sorted(range(1, m), key=lambda k: -near(k // 2, YN))

    def to_columns(k):
        peer = lax.rem(tp + k, m)
        return remote(
            moe_in.at[:, lax.rem(peer, YN)], columns.at[:, rows_of(tp), :], v["cs"].at[k], v["cr"].at[k], {"tp": peer}
        )

    for k in far_tp:
        to_columns(k).start()
    columns[:, rows_of(tp), :] = moe_in[:, lax.rem(tp, YN)]
    for k in range(1, m):
        source = lax.rem(tp + m - k, m)
        remote(
            moe_in.at[:, 0], columns.at[:, rows_of(source), :], v["cs"].at[k], v["cr"].at[k], {"tp": source}
        ).wait_recv()
    wide = mm(v["hot"][...], jnp.concatenate([columns[0], columns[1]], axis=1)).astype(BF16)
    for i in range(2):
        picked[i] = wide[:, i * lanes : (i + 1) * lanes].reshape(n, slots, lanes)

    z_order = sorted(range(ZN), key=lambda d: near(d, ZN))
    z_rank = [z_order.index(d) for d in range(ZN)]

    def block_of(o):
        return lax.rem(y + o * half, YN)

    def seat_of(b, k, j):
        return x.at[b, j // size, k, j % size]

    def dispatch(o, dz, dx):
        e = sp_at(z, xx, dz, dx)
        rz, rx = (-dz) % ZN, (-dx) % XN
        j = z_rank[rz] * per + rx // 2
        b = block_of(o)
        return remote(
            picked.at[b // half, e], seat_of(b, c, j), v["ds"].at[o, dz * XN + dx], v["dr"].at[o, c, j],
            {"sp": e, "tp": y * 2 + dx % 2},
        )

    homes = [
        pltpu.make_async_copy(picked.at[block_of(o) // half, sp], seat_of(block_of(o), 0, 0), v["dr"].at[o, 0, 0])
        for o in range(2)
    ]
    offsets = sorted(
        [(dz, dx) for dz in range(ZN) for dx in range(XN)], key=lambda o: near(o[0], ZN) + near(o[1], XN)
    )
    def send_wave(o):
        for dz, dx in offsets:
            if dz or dx:
                dispatch(o, dz, dx).start()
        pl.when(c == 0)(lambda: homes[o].start())
        pl.when(c == 1)(lambda: dispatch(o, 0, 0).start())

    send_wave(0)

    def arrive(o, j):
        for k in range(2):
            coming = remote(
                picked.at[0, 0], seat_of(block_of(o), k, j), v["ds"].at[0, 0], v["dr"].at[o, k, j], partner
            )
            if k == 0 and j == 0:
                pl.when(c == 0)(lambda: homes[o].wait())
                pl.when(c == 1)(lambda: coming.wait_recv())
            else:
                coming.wait_recv()

    def hop(way, h, g, behind=0):
        step = step_of(way)
        b = lax.rem(y + (h - 1 + behind) * (YN - step), YN)
        return remote(
            x.at[b, g], x.at[b, g], v["gs"].at[way, h - 1, g], v["gr"].at[way, h - 1, g],
            {"tp": lax.rem(y + step, YN) * 2 + c},
        )

    wg, wu, wd = v["wg"], v["wu"], v["wd"]

    def widen(b, first=False):
        at = pl.ds(pl.multiple_of(b * 2 * lanes, 2 * lanes), 2 * lanes)
        block = jnp.concatenate([x[b, :, k].reshape(group, lanes) for k in range(2)], axis=1)
        w = jnp.concatenate([ref[i, at, :] for ref in (wg, wu) for i in range(2)], axis=1)
        value = mm(block, w)
        acc[...] = value if first else acc[...] + value

    for g in range(groups):
        for j in range(g * size, (g + 1) * size):
            arrive(0, j)
        for way in range(2):
            if half > 1:
                hop(way, 1, g).start()
    send_wave(1)
    for load_w in loads:
        load_w.wait()
    for swap in swaps[2:]:
        swap.wait_recv()
    widen(y, first=True)
    for h in range(1, half):
        if h == half - 1:
            for j in range(count):
                arrive(1, j)
            widen(block_of(1))
        for g in range(groups):
            for way in range(2):
                hop(way, h, g, 1).wait_recv()
                if h < half - 1:
                    hop(way, h + 1, g).start()
        widen(lax.rem(y + YN - h, YN))
        widen(lax.rem(y + h, YN))
    if half == 1:
        for j in range(count):
            arrive(1, j)
        widen(block_of(1))

    hidden = 2 * lanes
    act[...] = (silu(acc[:, :hidden]) * acc[:, hidden:]).astype(BF16)

    def narrow(o):
        b = lax.rem(y + o, YN)
        at = pl.ds(pl.multiple_of(b * hidden, hidden), hidden)
        p[o] = mm(act[...], jnp.concatenate([wd[i, :, at] for i in range(2)], axis=0))

    def give(o, k, j):
        rz = z_order[j // per]
        rx = 2 * (j % per) + c
        back = ((-rz) % ZN) * XN + lax.rem(XN - rx, XN)
        return remote(
            q.at[o, k, j], pieces.at[o, sp], v["bs"].at[o, k, j], v["br"].at[o, back],
            {"sp": sp_at(z, xx, rz, rx), "tp": y * 2 + k},
        )

    returns = [pltpu.make_async_copy(q.at[o, 0, 0], pieces.at[o, sp], v["br"].at[o, 0]) for o in range(2)]

    def give_back(o, j):
        for k in range(2):
            if k == 0 and j == 0:
                pl.when(c == 0)(lambda: returns[o].start())
                pl.when(c == 1)(lambda: give(o, 0, 0).start())
            else:
                give(o, k, j).start()

    def opposite():
        narrow(half)
        for k in range(2):
            q[1, k] = p[half, :, k * lanes : (k + 1) * lanes].astype(BF16).reshape(count, slots, lanes)
        for j in reversed(range(count)):
            give_back(1, j)

    tall = group // groups

    def moe_done(g, total):
        total = total.astype(BF16)
        js = range(g * size, (g + 1) * size)
        for k in range(2):
            q[0, k, g * size : (g + 1) * size] = total[:, k * lanes : (k + 1) * lanes].reshape(size, slots, lanes)
        for j in reversed(js):
            give_back(0, j)

    sent += ring_sum(
        y, c, list(reversed(range(groups))), 0, lambda o, g: p[o, g * tall : (g + 1) * tall, :], narrow, opposite,
        v["s2"], v["r2"], v["s2s"], v["s2r"], moe_done,
    )
    for o in (1, 0):
        for dz in range(ZN):
            for dx in range(XN):
                i = dz * XN + dx
                coming = remote(
                    q.at[0, 0, 0], pieces.at[o, sp_at(z, xx, dz, dx)], v["bs"].at[0, 0, 0], v["br"].at[o, i], partner
                )
                if i == 0:
                    pl.when(c == 0)(lambda: returns[o].wait())
                    pl.when(c == 1)(lambda: coming.wait_recv())
                else:
                    coming.wait_recv()

    term, mixbox = v["term"], v["mixbox"]
    flat = jnp.concatenate([pieces[o].reshape(n * slots, lanes) for o in range(2)], axis=1)
    total = (mm(v["mixhi"][...], flat) + mm(v["mixlo"][...], flat)).astype(BF16)
    for o in range(2):
        term[o] = total[:, o * lanes : (o + 1) * lanes]

    def spread_rows(k):
        peer = lax.rem(tp + k, m)
        return remote(term.at[:, rows_of(peer), :], mixbox.at[tp], v["fs"].at[k], v["fr"].at[k], {"tp": peer})

    for k in far_tp:
        spread_rows(k).start()
    mixbox[tp] = term[:, rows_of(tp), :]
    for k in range(1, m):
        source = lax.rem(tp + m - k, m)
        remote(
            term.at[:, rows_of(0), :], mixbox.at[source], v["fs"].at[k], v["fr"].at[k], {"tp": source}
        ).wait_recv()
    mixture = jnp.concatenate(
        [mixbox[i, 0].astype(F32) + mixbox[(i + YN) % m, 1].astype(F32) for i in range(m)], axis=1
    )
    out[...] = layer_norm(settled[...] + mixture, v["gain_moe"][...]).astype(BF16)

    for j in range(1, XN):
        along_x(j).wait_send()
        back_x(j).wait_send()
    for j in range(1, ZN):
        along_z(j).wait_send()
    hand.wait_send()
    for swap in swaps:
        swap.wait_send()
    for copy in sent:
        copy.wait_send()
    for k in range(1, m):
        to_columns(k).wait_send()
        spread_rows(k).wait_send()
    for o in range(2):
        for dz, dx in offsets:
            if dz or dx:
                dispatch(o, dz, dx).wait_send()
        pl.when(c == 1)(lambda: dispatch(o, 0, 0).wait_send())
        for k in range(2):
            for j in range(count):
                if k == 0 and j == 0:
                    pl.when(c == 1)(lambda: give(o, 0, 0).wait_send())
                else:
                    give(o, k, j).wait_send()
    for way in range(2):
        for h in range(1, half):
            for g in range(groups):
                hop(way, h, g).wait_send()


def body(
    query_one, key_one, value_one, gate_one, decay_one, query_two, key_two, value_two, gate_two, decay_two,
    head_gain, proj_one, proj_two, stream, gain_mix, gain_moe, routes, affinity, expert_gate, expert_up,
    expert_down,
):
    rows, width = stream.shape
    dv = head_gain.shape[0]
    scratch = shapes_of(rows, dv, width)
    return pl.pallas_call(
        functools.partial(layer_kernel, tuple(scratch)),
        out_shape=jax.ShapeDtypeStruct((rows // (YN * 2), width), BF16),
        in_specs=[ANY] * len(INPUTS),
        out_specs=VMEM,
        scratch_shapes=list(scratch.values()),
        compiler_params=pltpu.CompilerParams(
            vmem_limit_bytes=56 * 2**20, collective_id=1, has_side_effects=True
        ),
    )(
        query_one.T, key_one.T, value_one, gate_one, jnp.swapaxes(decay_one, 1, 2), query_two, key_two, value_two,
        gate_two, decay_two, head_gain.reshape(1, -1), proj_one, proj_two, stream, gain_mix.reshape(1, -1),
        gain_moe.reshape(1, -1), routes.T, affinity.T, expert_gate, expert_up, expert_down,
    )


def solution(mesh):
    return jax.shard_map(
        body,
        mesh=mesh,
        in_specs=(
            P("sp", "tp"),
            P("sp", "tp"),
            P("sp", "tp"),
            P("sp", "tp"),
            P(None, "sp", "tp"),
            P("sp", "tp"),
            P("sp", "tp"),
            P("sp", "tp"),
            P("sp", "tp"),
            P(None, "sp", "tp"),
            P(),
            P("tp", None),
            P("tp", None),
            P("sp", None),
            P(),
            P(),
            P("sp", None),
            P("sp", None),
            P("sp", None, "tp"),
            P("sp", None, "tp"),
            P("sp", "tp", None),
        ),
        out_specs=P(("sp", "tp"), None),
        check_vma=False,
    )
```

```python
import functools

import jax
import jax.numpy as jnp
from jax import lax
from jax.experimental import pallas as pl
from jax.experimental.pallas import tpu as pltpu
from jax.sharding import PartitionSpec as P

DK_A = 64
DK_B = 128
BLK = 64
SHARPNESS = 16.0
ZN, XN, YN = 8, 4, 8
CUTS = 4
GROUPS = 8
LAG = 20
FADES = 8
F32 = jnp.float32
BF16 = jnp.bfloat16
MESH = pl.DeviceIdType.MESH
VMEM = pl.BlockSpec(memory_space=pltpu.VMEM)
ANY = pl.BlockSpec(memory_space=pl.ANY)
DMA = pltpu.SemaphoreType.DMA


def mm(a, b):
    return jnp.dot(a, b, preferred_element_type=F32)


def mm_nt(a, b):
    return lax.dot_general(a, b, (((1,), (1,)), ((), ())), preferred_element_type=F32)


def mm_tn(a, b):
    return lax.dot_general(a, b, (((0,), (0,)), ((), ())), preferred_element_type=F32)


def log_sigmoid(x):
    return jnp.minimum(x, 0.0) - jnp.log1p(jnp.exp(-jnp.abs(x)))


def silu(x):
    return x / (1.0 + jnp.exp(-x))


def layer_norm(values, gain):
    mean = jnp.mean(values, axis=-1, keepdims=True)
    spread = jnp.mean(jnp.square(values - mean), axis=-1, keepdims=True)
    return (values - mean) * lax.rsqrt(spread + 1e-05) * gain


def remote(src, dst, send, recv, peer):
    return pltpu.make_async_remote_copy(
        src_ref=src, dst_ref=dst, send_sem=send, recv_sem=recv, device_id=peer, device_id_type=MESH
    )


def sp_at(z, x, dz, dx):
    return lax.rem(z + dz, ZN) * XN + lax.rem(x + dx, XN)


def near(d, n):
    return min(d, n - d)


def step_of(way):
    return 1 if way == 0 else YN - 1


def fade_rows(total):
    wide = total.shape[1]
    row = lax.broadcasted_iota(jnp.int32, (FADES, wide), 0)
    high = total.astype(BF16).astype(F32)
    return jnp.where(row == 0, high, jnp.where(row == 1, total - high, 0.0)).astype(BF16)


def local_states(keys, values, decays, base, stack, cum):
    rows, wide = keys.shape
    count = rows // BLK
    dv = values.shape[1]
    piece = dv // XN
    ii = lax.broadcasted_iota(jnp.int32, (rows, rows), 0)
    jj = lax.broadcasted_iota(jnp.int32, (rows, rows), 1)
    same = (ii // BLK) == (jj // BLK)
    for way in range(2):
        tri = jnp.where(same & ((ii >= jj) if way == 0 else (ii <= jj)), 1.0, 0.0).astype(BF16)
        fade = log_sigmoid(decays[way]) / SHARPNESS
        high = fade.astype(BF16)
        low = (fade - high.astype(F32)).astype(BF16)
        total = mm(tri, high) + mm(tri, low)
        cum[way, :, base : base + wide] = total
        tail = jnp.zeros((1, wide), F32)
        weighted = [None] * count
        for b in reversed(range(count)) if way == 0 else range(count):
            part = total[b * BLK : (b + 1) * BLK]
            last = part[BLK - 1 : BLK] if way == 0 else part[0:1]
            weighted[b] = (keys[b * BLK : (b + 1) * BLK] * jnp.exp(last - part + tail)).astype(BF16)
            tail = tail + last
        state = mm_tn(values, jnp.concatenate(weighted, axis=0)).astype(BF16)
        fades = fade_rows(tail)
        for i in range(XN):
            stack[i, way, 0:piece, base : base + wide] = state[i * piece : (i + 1) * piece]
            stack[i, way, piece : piece + FADES, base : base + wide] = fades


def local_mix(query, keys, values, base, cum, reach, column, mixed):
    rows, dk = keys.shape
    count = rows // BLK
    dv = values.shape[1]
    ii = lax.broadcasted_iota(jnp.int32, (BLK, BLK), 0)
    jj = lax.broadcasted_iota(jnp.int32, (BLK, BLK), 1)
    lanes = slice(base, base + dk)
    query = query * dk ** (-0.5)
    inner = [None] * count
    readers = [None] * count
    state = None
    passed = jnp.zeros((1, dk), F32)
    for b in range(count):
        at = slice(b * BLK, (b + 1) * BLK)
        value = values[at]
        cf = cum[0, at, lanes]
        cb = cum[1, at, lanes]
        qf = (query[at] * jnp.exp(cf)).astype(BF16)
        kf = (keys[at] * jnp.exp(-cf)).astype(BF16)
        qr = (query[at] * jnp.exp(cb)).astype(BF16)
        kr = (keys[at] * jnp.exp(-cb)).astype(BF16)
        scores = jnp.where(ii >= jj, mm_nt(qf, kf), 0.0) + jnp.where(ii <= jj, mm_nt(qr, kr), 0.0)
        inner[b] = mm(scores.astype(BF16), value)
        if b > 0:
            inner[b] = inner[b] + mm_nt(qf, state.astype(BF16))
        reach[0, at, lanes] = (query[at] * jnp.exp(cf + passed)).astype(BF16)
        last = cf[BLK - 1 : BLK]
        if b < count - 1:
            gain = mm_tn(value, (keys[at] * jnp.exp(last - cf)).astype(BF16))
            state = gain if b == 0 else jnp.exp(last) * state + gain
        passed = passed + last
        readers[b] = qr
    state = None
    passed = jnp.zeros((1, dk), F32)
    for b in reversed(range(count)):
        at = slice(b * BLK, (b + 1) * BLK)
        cb = cum[1, at, lanes]
        if b < count - 1:
            inner[b] = inner[b] + mm_nt(readers[b], state.astype(BF16))
        reach[1, at, lanes] = (query[at] * jnp.exp(cb + passed)).astype(BF16)
        last = cb[0:1]
        if b > 0:
            gain = mm_tn(values[at], (keys[at] * jnp.exp(last - cb)).astype(BF16))
            state = gain if b == count - 1 else jnp.exp(last) * state + gain
        passed = passed + last
        mixed[at, column : column + dv] = inner[b]


def ring_sum(y, c, order, jump, part, prepare, extra, s, r, ss, sr, finish):
    half = YN // 2

    def mine(way, k):
        return k // (len(order) // 2) == way

    def pass_sum(way, d, k):
        step = jump if d == half else 1
        return remote(
            s.at[way, d - 1, k], r.at[way, d - 1, k], ss.at[int(d == half)], sr.at[d - 1, k],
            {"tp": lax.rem(y + (step if way == 0 else YN - step), YN) * 2 + c},
        )

    def landed(d, k):
        box = r.at[:, d - 1, k]
        remote(box, box, ss.at[0], sr.at[d - 1, k], {"tp": y * 2 + 1 - c}).wait_recv()

    def collect(total, way, d, k):
        if d + 1 < half:
            total = total + r[way, d, k].astype(F32)
        if jump and mine(way, k) and half - jump == d:
            total = total + r[way, half - 1, k].astype(F32)
        return total

    def await_for(d, k):
        if d + 1 < half:
            landed(d + 1, k)
        if jump and half - jump == d:
            way = int(mine(1, k))
            pass_sum(way, half, k).wait_recv()

    def send(way, d, k):
        s[way, d - 1, k] = collect(part(d if way == 0 else YN - d, k), way, d, k).astype(BF16)
        pass_sum(way, d, k).start()

    if jump:
        prepare(half)
        for k in order:
            for way in range(2):
                if mine(way, k):
                    send(way, half, k)
    for d in range(half - 1, 0, -1):
        prepare(d)
        prepare(YN - d)
        for k in order:
            await_for(d, k)
            for way in range(2):
                send(way, d, k)
        if d == half - 1:
            extra()
    if half == 1:
        extra()
    prepare(0)
    for k in order:
        total = part(0, k)
        await_for(0, k)
        for way in range(2):
            total = collect(total, way, 0, k)
        finish(k, total)
    if half > 1:
        whole = s.at[:, 0 : half - 1]
        remote(whole, whole, ss.at[0], sr.at[0, 0], {"tp": y * 2 + 1 - c}).wait_send()
    if jump:
        whole = s.at[:, half - 1, 0 : len(order) // 2]
        remote(whole, whole, ss.at[1], sr.at[0, 0], {"tp": y * 2 + 1 - c}).wait_send()


INPUTS = (
    "qa", "ka", "va", "ga", "da", "qb", "kb", "vb", "gb", "db", "head_gain", "pa", "pb", "stream",
    "gain_mix", "gain_moe", "routes", "affinity", "wg", "wu", "wd",
)


def shapes_of(rows, dv, width):
    n = ZN * XN
    m = YN * 2
    half = YN // 2
    own = rows // m
    lanes = width // m
    slots = 3 * rows * 2 // (2 * n)
    count = n // 2
    group = count * slots
    keys = DK_A + DK_B
    piece = dv // XN
    big = piece + FADES
    mine = rows // 2
    groups = min(GROUPS, count)
    hops = max(1, half - 1)
    cut = width // CUTS
    v = pltpu.VMEM
    return dict(
        qa=v((DK_A, rows), BF16), ka=v((DK_A, rows), BF16), va=v((rows, dv), BF16), ga=v((rows, dv), BF16),
        da=v((2, DK_A, rows), F32), qb=v((rows, DK_B), BF16), kb=v((rows, DK_B), BF16), vb=v((rows, dv), BF16),
        gb=v((rows, dv), BF16), db=v((2, rows, DK_B), F32), head_gain=v((1, dv), F32),
        stream=v((own, width), BF16), gain_mix=v((1, width), F32), gain_moe=v((1, width), F32),
        routes=v((2, rows), jnp.int32), affinity=v((2, rows), F32),
        pj=v((2, 2, dv, width), BF16), wg=v((2, width, lanes), BF16), wu=v((2, width, lanes), BF16),
        wd=v((2, lanes, width), BF16), early=DMA((16,)), loads=DMA((3,)), swap_s=DMA((5,)), swap_r=DMA((5,)),
        cum=v((2, rows, keys), F32), stack=v((XN, 2, big, keys), BF16), xbox=v((XN, 2, big, keys), BF16),
        agg=v((2, big, keys), BF16), zbox=v((ZN, big, keys), BF16), outx=v((XN, 2, piece, keys), BF16),
        states=v((XN, 2, piece, keys), BF16), xs=DMA, xr=DMA, zs=DMA, zr=DMA,
        es=DMA, er=DMA,
        mixed=v((rows, 2 * dv), F32), reach=v((2, rows, keys), BF16), heads=v((2, mine, 2 * dv), BF16),
        hbox=v((mine, 2 * dv), BF16), hs=DMA((2,)), pp=v((YN, own, width), F32),
        s1=v((2, half, CUTS, own, cut), BF16), r1=v((2, half, CUTS, own, cut), BF16),
        s1s=DMA((2,)), s1r=DMA((half, CUTS)), settled=v((own, width), F32),
        moe_in=v((2, YN, own, lanes), BF16), columns=v((2, rows, lanes), BF16), cs=DMA, cr=DMA,
        hot=v((n * slots, rows), BF16),
        mixhi=v((rows, n * slots), BF16), mixlo=v((rows, n * slots), BF16), picked=v((2, n, slots, lanes), BF16),
        x=v((YN, groups, 2, count // groups, slots, lanes), BF16), acc=v((group, 4 * lanes), F32),
        act=v((group, 2 * lanes), BF16), p=v((YN, group, 2 * lanes), F32),
        s2=v((2, hops, groups, group // groups, 2 * lanes), BF16),
        r2=v((2, hops, groups, group // groups, 2 * lanes), BF16), s2s=DMA((2,)),
        s2r=DMA((hops, groups)), q=v((2, 2, count, slots, lanes), BF16), pieces=v((2, n, slots, lanes), BF16),
        term=v((2, rows, lanes), BF16), mixbox=v((2, m, own, lanes), BF16), ds=DMA((2, 2)), dr=DMA((groups + 1,)),
        gs=DMA, gr=DMA((hops, groups)), bs=DMA((2, 2)), br=DMA((2,)),
        fs=DMA((2,)), fr=DMA((2,)),
    )


def layer_kernel(scratch_names, *refs):
    hbm = dict(zip(INPUTS, refs))
    out = refs[len(INPUTS)]
    v = dict(zip(scratch_names, refs[len(INPUTS) + 1 :]))
    sp = lax.axis_index("sp")
    tp = lax.axis_index("tp")
    z, xx, y, c = sp // XN, lax.rem(sp, XN), tp // 2, lax.rem(tp, 2)
    n = ZN * XN
    m = YN * 2
    half = YN // 2
    per = XN // 2
    picked, x, acc, act, p, q, pieces = (v[i] for i in ("picked", "x", "acc", "act", "p", "q", "pieces"))
    slots = picked.shape[2]
    count = ZN * per
    group = count * slots
    lanes = picked.shape[3]
    groups = x.shape[1]
    size = count // groups
    rows = v["columns"].shape[1]
    own = rows // m
    partner = {"tp": tp + 1 - 2 * c}

    def rows_of(i):
        return pl.ds(pl.multiple_of(i * own, own), own)

    fetch = {}
    order = (
        "ka", "kb", "da", "db", "va", "vb", "qa", "qb", "ga", "gb", "head_gain", "routes", "affinity", "stream",
        "gain_mix", "gain_moe",
    )
    for i, name in enumerate(order):
        src = hbm[name].at[rows_of(tp), :] if name == "stream" else hbm[name]
        fetch[name] = pltpu.make_async_copy(src, v[name], v["early"].at[max(0, i - 5)])
        if i < 6:
            fetch[name].start()
    barrier = pltpu.get_barrier_semaphore()
    def far(dz, dx, dy):
        return near(dz, ZN) + near(dx, XN) + near(dy, YN)

    friends = [
        (far(dz, dx, 0), {"sp": sp_at(z, xx, dz, dx), "tp": y * 2 + core})
        for dz in range(ZN) for dx in range(XN) for core in range(2) if dz or dx
    ] + [(far(0, 0, k // 2), {"tp": lax.rem(tp + k, m)}) for k in range(1, m)]
    for _, peer in sorted(friends, key=lambda f: -f[0]):
        pl.semaphore_signal(barrier, inc=1, device_id=peer, device_id_type=MESH)
    greeted = len(friends)

    for i, name in enumerate(order):
        if i >= 6:
            fetch[name].start()
    for i, name in enumerate(("pa", "pb")):
        fetch[name] = pltpu.make_async_copy(hbm[name], v["pj"].at[0, i], v["early"].at[len(order) - 5])
        fetch[name].start()
    pairs = [(hbm[name].at[0], v[name]) for name in ("wg", "wu", "wd")]
    loads = [pltpu.make_async_copy(src, dst.at[0], v["loads"].at[i]) for i, (src, dst) in enumerate(pairs)]
    for load in loads:
        load.start()
    swaps = [
        remote(src, dst, v["swap_s"].at[i], v["swap_r"].at[i], partner)
        for i, (src, dst) in enumerate(
            [(hbm["pa"], v["pj"].at[1, 0]), (hbm["pb"], v["pj"].at[1, 1])] + [(s, d.at[1]) for s, d in pairs]
        )
    ]

    first = acc.at[0 : rows * 19 * DK_B // (16 * lanes)]
    pltpu.make_async_copy(first, first, v["early"].at[0]).wait()
    cum, stack = v["cum"], v["stack"]
    keys_a = v["ka"][...].astype(F32).T
    keys_b = v["kb"][...].astype(F32)
    local_states(keys_a, v["va"][...], [v["da"][i].T for i in range(2)], 0, stack, cum)
    local_states(keys_b, v["vb"][...], [v["db"][i] for i in range(2)], DK_A, stack, cum)

    pl.semaphore_wait(barrier, greeted)

    xbox, agg, zbox, outx, states = (v[i] for i in ("xbox", "agg", "zbox", "outx", "states"))
    piece = outx.shape[2]

    def along_x(j):
        peer = lax.rem(xx + j, XN)
        return remote(stack.at[peer], xbox.at[xx], v["xs"], v["xr"], {"sp": z * XN + peer})

    def along_z(j):
        peer = lax.rem(z + j, ZN)
        way = jnp.where(peer > z, 0, 1)
        return remote(agg.at[way], zbox.at[z], v["zs"], v["zr"], {"sp": peer * XN + xx})

    def back_x(j):
        peer = lax.rem(xx + j, XN)
        return remote(outx.at[peer], states.at[xx], v["es"], v["er"], {"sp": z * XN + peer})

    far_x = sorted(range(1, XN), key=lambda j: -near(j, XN))
    far_z = sorted(range(1, ZN), key=lambda j: -near(j, ZN))
    for j in far_x:
        along_x(j).start()
    for swap in swaps:
        swap.start()
    xbox[xx] = stack[xx]
    zbox[z] = jnp.zeros_like(zbox[z])

    for name in ("qa", "qb"):
        fetch[name].wait()
    mixed, reach = v["mixed"], v["reach"]
    dv = v["va"].shape[1]
    local_mix(v["qa"][...].astype(F32).T, keys_a, v["va"][...], 0, cum, reach, 0, mixed)

    def load(block):
        block = block.astype(F32)
        return block[0:piece], block[piece : piece + 1] + block[piece + 1 : piece + 2]

    def all_of(box, size, send, recv):
        box = box.at[0 : size - 1]
        return remote(box, box, send, recv, partner)

    if XN > 1:
        all_of(xbox, XN, v["xs"], v["xr"]).wait_recv()
    for way in range(2):
        state, fade = None, None
        for i in range(XN) if way == 0 else reversed(range(XN)):
            own_state, own_fade = load(xbox[i, way])
            state = own_state if state is None else jnp.exp(own_fade) * state + own_state
            fade = own_fade if fade is None else fade + own_fade
        agg[way, 0:piece] = state.astype(BF16)
        agg[way, piece : piece + FADES] = fade_rows(fade)
    for j in far_z:
        along_z(j).start()

    local_mix(v["qb"][...].astype(F32), keys_b, v["vb"][...], DK_A, cum, reach, dv, mixed)
    for name in ("routes", "affinity"):
        fetch[name].wait()
    routes, affinity = v["routes"][...], v["affinity"][...]
    lane = lax.broadcasted_iota(jnp.int32, (n, rows), 0)
    hots = [routes[i : i + 1] == lane for i in range(2)]
    named = sum(jnp.where(h, 1.0, 0.0) for h in hots)
    ii = lax.broadcasted_iota(jnp.int32, (rows, rows), 0)
    jj = lax.broadcasted_iota(jnp.int32, (rows, rows), 1)
    before = mm(named.astype(BF16), jnp.where(ii < jj, 1.0, 0.0).astype(BF16))
    place = [
        routes[i : i + 1] * slots
        + jnp.sum(jnp.where(hots[i], before, 0.0), axis=0, keepdims=True).astype(jnp.int32)
        for i in range(2)
    ]
    seat = lax.broadcasted_iota(jnp.int32, (n * slots, rows), 0)
    v["hot"][...] = jnp.where((seat == place[0]) | (seat == place[1]), 1.0, 0.0).astype(BF16)
    weights = [affinity[i : i + 1] / (affinity[0:1] + affinity[1:2]) for i in range(2)]
    mix = jnp.where(seat == place[0], weights[0], jnp.where(seat == place[1], weights[1], 0.0)).T
    high = mix.astype(BF16)
    v["mixhi"][...] = high
    v["mixlo"][...] = (mix - high.astype(F32)).astype(BF16)

    if ZN > 1:
        all_of(zbox, ZN, v["zs"], v["zr"]).wait_recv()
    keys = zbox.shape[2]
    ahead = jnp.zeros((piece, keys), F32)
    behind = jnp.zeros((piece, keys), F32)
    for i in range(ZN):
        state, fade = load(zbox[i])
        ahead = jnp.where(i < z, jnp.exp(fade) * ahead + state, ahead)
    for i in reversed(range(ZN)):
        state, fade = load(zbox[i])
        behind = jnp.where(i > z, jnp.exp(fade) * behind + state, behind)
    for i in range(XN):
        outx[i, 0] = ahead.astype(BF16)
        if i < XN - 1:
            state, fade = load(xbox[i, 0])
            ahead = jnp.exp(fade) * ahead + state
    for i in reversed(range(XN)):
        outx[i, 1] = behind.astype(BF16)
        if i > 0:
            state, fade = load(xbox[i, 1])
            behind = jnp.exp(fade) * behind + state
    for j in far_x:
        back_x(j).start()
    states[xx] = outx[xx]
    for name in ("ga", "gb", "head_gain", "stream", "gain_mix", "gain_moe"):
        fetch[name].wait()
    pltpu.make_async_copy(v["pj"].at[0], v["pj"].at[0], v["early"].at[len(order) - 5]).wait()
    if XN > 1:
        all_of(states, XN, v["es"], v["er"]).wait_recv()

    heads, hbox = v["heads"], v["hbox"]
    for i, (base, dk, gate) in enumerate(((0, DK_A, v["ga"]), (DK_A, DK_B, v["gb"]))):
        at = slice(base, base + dk)
        whole = mixed[:, i * dv : (i + 1) * dv]
        for way in range(2):
            start = states[:, way].reshape(dv, keys)
            whole = whole + mm_nt(reach[way, :, at], start[:, at])
        scale = lax.rsqrt(jnp.mean(whole * whole, axis=-1, keepdims=True) + 1e-06)
        value = (whole * scale * v["head_gain"][...] * silu(gate[...].astype(F32))).astype(BF16)
        value = value.reshape(YN, 2, own, dv)
        for core in range(2):
            heads[core, :, i * dv : (i + 1) * dv] = value[:, core].reshape(YN * own, dv)
    hand = remote(heads.at[1 - c], hbox, v["hs"].at[0], v["hs"].at[1], partner)
    hand.start()
    pj, pp = v["pj"], v["pp"]
    pp[...] = (mm(heads[c], pj[0].reshape(2 * dv, pj.shape[3]))).reshape(pp.shape)
    swaps[0].wait_recv()
    swaps[1].wait_recv()
    hand.wait_recv()
    pp[...] = pp[...] + (mm(hbox[...], pj[1].reshape(2 * dv, pj.shape[3]))).reshape(pp.shape)

    settled, moe_in, columns = v["settled"], v["moe_in"], v["columns"]
    cut = v["s1"].shape[4]

    def attn_part(o, k):
        return pp[lax.rem(y + o, YN), :, k * cut : (k + 1) * cut]

    def attn_done(k, total):
        settled[:, k * cut : (k + 1) * cut] = total

    ring_sum(
        y, c, [k // 2 + CUTS // 2 * (k % 2) for k in range(CUTS)], min(2, half), attn_part, lambda o: None,
        lambda: None, v["s1"], v["r1"], v["s1s"], v["s1r"], attn_done,
    )
    value = layer_norm(v["stream"][...].astype(F32) + settled[...], v["gain_mix"][...])
    settled[...] = value
    value = value.astype(BF16)
    for i in range(m):
        moe_in[i // YN, i % YN] = value[:, i * lanes : (i + 1) * lanes]

    far_tp = sorted(range(1, m), key=lambda k: -near(k // 2, YN))

    def to_columns(k):
        peer = lax.rem(tp + k, m)
        return remote(
            moe_in.at[:, lax.rem(peer, YN)], columns.at[:, rows_of(tp), :], v["cs"], v["cr"], {"tp": peer}
        )

    for k in far_tp:
        to_columns(k).start()
    columns[:, rows_of(tp), :] = moe_in[:, lax.rem(tp, YN)]
    most = columns.at[:, 0 : rows - own, :]
    all_columns = remote(most, most, v["cs"], v["cr"], partner)
    all_columns.wait_recv()
    wide = mm(v["hot"][...], jnp.concatenate([columns[0], columns[1]], axis=1)).astype(BF16)
    for i in range(2):
        picked[i] = wide[:, i * lanes : (i + 1) * lanes].reshape(n, slots, lanes)

    z_order = sorted(range(ZN), key=lambda d: near(d, ZN))
    z_rank = [z_order.index(d) for d in range(ZN)]

    def block_of(o):
        return lax.rem(y + o * half, YN)

    def seat_of(b, k, j):
        return x.at[b, j // size, k, j % size]

    def dispatch(o, dz, dx):
        e = sp_at(z, xx, dz, dx)
        rz, rx = (-dz) % ZN, (-dx) % XN
        j = z_rank[rz] * per + rx // 2
        b = block_of(o)
        return remote(
            picked.at[b // half, e], seat_of(b, c, j), v["ds"].at[o, int(dz + dx == 0)], v["dr"].at[groups if o else j // size],
            {"sp": e, "tp": y * 2 + dx % 2},
        )

    homes = [
        pltpu.make_async_copy(picked.at[block_of(o) // half, sp], seat_of(block_of(o), 0, 0), v["dr"].at[groups if o else 0])
        for o in range(2)
    ]
    offsets = sorted(
        [(dz, dx) for dz in range(ZN) for dx in range(XN)], key=lambda o: near(o[0], ZN) + near(o[1], XN)
    )
    def send_wave(o):
        for dz, dx in offsets:
            if dz or dx:
                dispatch(o, dz, dx).start()
        pl.when(c == 0)(lambda: homes[o].start())
        pl.when(c == 1)(lambda: dispatch(o, 0, 0).start())

    send_wave(0)

    def arrive(g):
        block = x.at[block_of(0), g]
        remote(block, block, v["ds"].at[0, 0], v["dr"].at[g], partner).wait_recv()

    def arrive_opposite():
        block = x.at[block_of(1)]
        remote(block, block, v["ds"].at[1, 0], v["dr"].at[groups], partner).wait_recv()
        widen(block_of(1))

    def hop(way, h, g, behind=0):
        step = step_of(way)
        b = lax.rem(y + (h - 1 + behind) * (YN - step), YN)
        return remote(
            x.at[b, g], x.at[b, g], v["gs"], v["gr"].at[h - 1, g],
            {"tp": lax.rem(y + step, YN) * 2 + c},
        )

    wg, wu, wd = v["wg"], v["wu"], v["wd"]

    def widen(b, first=False):
        at = pl.ds(pl.multiple_of(b * 2 * lanes, 2 * lanes), 2 * lanes)
        block = jnp.concatenate([x[b, :, k].reshape(group, lanes) for k in range(2)], axis=1)
        w = jnp.concatenate([ref[i, at, :] for ref in (wg, wu) for i in range(2)], axis=1)
        value = mm(block, w)
        acc[...] = value if first else acc[...] + value

    def land(h, g):
        pair = x.at[0:2, g]
        remote(pair, pair, v["gs"], v["gr"].at[h - 1, g], partner).wait_recv()

    turns = sorted(
        [(h, g) for h in range(max(1, half)) for g in range(groups)], key=lambda t: (t[1] + LAG * t[0], t[0])
    )
    for h, g in turns:
        if h == half - 1 and h > 0 and g == 0:
            arrive_opposite()
        if h == 0:
            arrive(g)
        else:
            land(h, g)
        if h < half - 1:
            for way in range(2):
                hop(way, h + 1, g).start()
        if g < groups - 1:
            continue
        if h == 0:
            send_wave(1)
            for load_w in loads:
                load_w.wait()
            for swap in swaps[2:]:
                swap.wait_recv()
            widen(y, first=True)
        else:
            widen(lax.rem(y + YN - h, YN))
            widen(lax.rem(y + h, YN))
    if half == 1:
        arrive_opposite()

    hidden = 2 * lanes
    act[...] = (silu(acc[:, :hidden]) * acc[:, hidden:]).astype(BF16)

    def narrow(o):
        b = lax.rem(y + o, YN)
        at = pl.ds(pl.multiple_of(b * hidden, hidden), hidden)
        p[o] = mm(act[...], jnp.concatenate([wd[i, :, at] for i in range(2)], axis=0))

    def give(o, k, j):
        rz = z_order[j // per]
        rx = 2 * (j % per) + c
        return remote(
            q.at[o, k, j], pieces.at[o, sp], v["bs"].at[o, int(k + j == 0)], v["br"].at[o],
            {"sp": sp_at(z, xx, rz, rx), "tp": y * 2 + k},
        )

    returns = [pltpu.make_async_copy(q.at[o, 0, 0], pieces.at[o, sp], v["br"].at[o]) for o in range(2)]

    def give_back(o, j):
        for k in range(2):
            if k == 0 and j == 0:
                pl.when(c == 0)(lambda: returns[o].start())
                pl.when(c == 1)(lambda: give(o, 0, 0).start())
            else:
                give(o, k, j).start()

    def opposite():
        narrow(half)
        for k in range(2):
            q[1, k] = p[half, :, k * lanes : (k + 1) * lanes].astype(BF16).reshape(count, slots, lanes)
        for j in reversed(range(count)):
            give_back(1, j)

    tall = group // groups

    def moe_done(g, total):
        total = total.astype(BF16)
        js = range(g * size, (g + 1) * size)
        for k in range(2):
            q[0, k, g * size : (g + 1) * size] = total[:, k * lanes : (k + 1) * lanes].reshape(size, slots, lanes)
        for j in reversed(js):
            give_back(0, j)

    ring_sum(
        y, c, list(reversed(range(groups))), 0, lambda o, g: p[o, g * tall : (g + 1) * tall, :], narrow, opposite,
        v["s2"], v["r2"], v["s2s"], v["s2r"], moe_done,
    )
    term, mixbox = v["term"], v["mixbox"]

    def spread_rows(o, k):
        peer = lax.rem(tp + k, m)
        return remote(term.at[o, rows_of(peer), :], mixbox.at[o, tp], v["fs"].at[o], v["fr"].at[o], {"tp": peer})

    for o in (1, 0):
        whole = pieces.at[o]
        remote(whole, whole, v["bs"].at[o, 0], v["br"].at[o], partner).wait_recv()
        flat = pieces[o].reshape(n * slots, lanes)
        term[o] = (mm(v["mixhi"][...], flat) + mm(v["mixlo"][...], flat)).astype(BF16)
        for k in far_tp:
            spread_rows(o, k).start()
        mixbox[o, tp] = term[o, rows_of(tp), :]
    row_waits = []
    for o in (1, 0):
        whole = mixbox.at[o, 0 : m - 1]
        row_waits.append(remote(whole, whole, v["fs"].at[o], v["fr"].at[o], partner))
        row_waits[-1].wait_recv()
    mixture = jnp.concatenate(
        [mixbox[0, i].astype(F32) + mixbox[1, (i + YN) % m].astype(F32) for i in range(m)], axis=1
    )
    out[...] = layer_norm(settled[...] + mixture, v["gain_moe"][...]).astype(BF16)

    if XN > 1:
        all_of(xbox, XN, v["xs"], v["xr"]).wait_send()
        all_of(states, XN, v["es"], v["er"]).wait_send()
    if ZN > 1:
        all_of(zbox, ZN, v["zs"], v["zr"]).wait_send()
    hand.wait_send()
    for swap in swaps:
        swap.wait_send()
    all_columns.wait_send()
    for wait in row_waits:
        wait.wait_send()
    for o in range(2):
        most = picked.at[0, 0 : n - 1]
        remote(most, most, v["ds"].at[o, 0], v["dr"].at[o], partner).wait_send()
        pl.when(c == 1)(lambda: dispatch(o, 0, 0).wait_send())
        most = pieces.at[o, 0 : n - 1]
        remote(most, most, v["bs"].at[o, 0], v["br"].at[o], partner).wait_send()
        pl.when(c == 1)(lambda: give(o, 0, 0).wait_send())
    if half > 1:
        whole = x.at[0 : 2 * (half - 1)]
        remote(whole, whole, v["gs"], v["gr"].at[0, 0], partner).wait_send()


def body(
    query_one, key_one, value_one, gate_one, decay_one, query_two, key_two, value_two, gate_two, decay_two,
    head_gain, proj_one, proj_two, stream, gain_mix, gain_moe, routes, affinity, expert_gate, expert_up,
    expert_down,
):
    rows, width = stream.shape
    dv = head_gain.shape[0]
    scratch = shapes_of(rows, dv, width)
    return pl.pallas_call(
        functools.partial(layer_kernel, tuple(scratch)),
        out_shape=jax.ShapeDtypeStruct((rows // (YN * 2), width), BF16),
        in_specs=[ANY] * len(INPUTS),
        out_specs=VMEM,
        scratch_shapes=list(scratch.values()),
        compiler_params=pltpu.CompilerParams(
            vmem_limit_bytes=56 * 2**20, collective_id=1, has_side_effects=True
        ),
    )(
        query_one.T, key_one.T, value_one, gate_one, jnp.swapaxes(decay_one, 1, 2), query_two, key_two, value_two,
        gate_two, decay_two, head_gain.reshape(1, -1), proj_one, proj_two, stream, gain_mix.reshape(1, -1),
        gain_moe.reshape(1, -1), routes.T, affinity.T, expert_gate, expert_up, expert_down,
    )


def solution(mesh):
    return jax.shard_map(
        body,
        mesh=mesh,
        in_specs=(
            P("sp", "tp"),
            P("sp", "tp"),
            P("sp", "tp"),
            P("sp", "tp"),
            P(None, "sp", "tp"),
            P("sp", "tp"),
            P("sp", "tp"),
            P("sp", "tp"),
            P("sp", "tp"),
            P(None, "sp", "tp"),
            P(),
            P("tp", None),
            P("tp", None),
            P("sp", None),
            P(),
            P(),
            P("sp", None),
            P("sp", None),
            P("sp", None, "tp"),
            P("sp", None, "tp"),
            P("sp", "tp", None),
        ),
        out_specs=P(("sp", "tp"), None),
        check_vma=False,
    )
```

```python
import functools

import jax
import jax.numpy as jnp
from jax import lax
from jax.experimental import pallas as pl
from jax.experimental.pallas import tpu as pltpu
from jax.sharding import PartitionSpec as P

DK_A = 64
DK_B = 128
BLK = 64
SHARPNESS = 16.0
ZN, XN, YN = 8, 4, 8
CUTS = 4
GROUPS = 8
LAG = 20
FADES = 8
F32 = jnp.float32
BF16 = jnp.bfloat16
MESH = pl.DeviceIdType.MESH
VMEM = pl.BlockSpec(memory_space=pltpu.VMEM)
ANY = pl.BlockSpec(memory_space=pl.ANY)
DMA = pltpu.SemaphoreType.DMA


def mm(a, b):
    return jnp.dot(a, b, preferred_element_type=F32)


def mm_nt(a, b):
    return lax.dot_general(a, b, (((1,), (1,)), ((), ())), preferred_element_type=F32)


def mm_tn(a, b):
    return lax.dot_general(a, b, (((0,), (0,)), ((), ())), preferred_element_type=F32)


def log_sigmoid(x):
    return jnp.minimum(x, 0.0) - jnp.log1p(jnp.exp(-jnp.abs(x)))


def silu(x):
    return x / (1.0 + jnp.exp(-x))


def layer_norm(values, gain):
    mean = jnp.mean(values, axis=-1, keepdims=True)
    spread = jnp.mean(jnp.square(values - mean), axis=-1, keepdims=True)
    return (values - mean) * lax.rsqrt(spread + 1e-05) * gain


def remote(src, dst, send, recv, peer):
    return pltpu.make_async_remote_copy(
        src_ref=src, dst_ref=dst, send_sem=send, recv_sem=recv, device_id=peer, device_id_type=MESH
    )


def sp_at(z, x, dz, dx):
    return lax.rem(z + dz, ZN) * XN + lax.rem(x + dx, XN)


def near(d, n):
    return min(d, n - d)


def step_of(way):
    return 1 if way == 0 else YN - 1


def split_fade(total):
    high = total.astype(BF16).astype(F32)
    return high, total - high


def fade_rows(fade_a, fade_b):
    row = lax.broadcasted_iota(jnp.int32, (FADES, fade_b.shape[1]), 0)
    rows = 0.0
    for i, value in enumerate(split_fade(fade_b) + split_fade(fade_a)):
        rows = jnp.where(row == i, value, rows)
    return rows.astype(BF16)


def local_states(keys, values, decays, base, cum):
    rows, wide = keys.shape
    count = rows // BLK
    ii = lax.broadcasted_iota(jnp.int32, (rows, rows), 0)
    jj = lax.broadcasted_iota(jnp.int32, (rows, rows), 1)
    same = (ii // BLK) == (jj // BLK)
    found = []
    for way in range(2):
        tri = jnp.where(same & ((ii >= jj) if way == 0 else (ii <= jj)), 1.0, 0.0).astype(BF16)
        fade = log_sigmoid(decays[way]) / SHARPNESS
        high = fade.astype(BF16)
        low = (fade - high.astype(F32)).astype(BF16)
        total = mm(tri, high) + mm(tri, low)
        cum[way, :, base : base + wide] = total
        tail = jnp.zeros((1, wide), F32)
        weighted = [None] * count
        for b in reversed(range(count)) if way == 0 else range(count):
            part = total[b * BLK : (b + 1) * BLK]
            last = part[BLK - 1 : BLK] if way == 0 else part[0:1]
            weighted[b] = (keys[b * BLK : (b + 1) * BLK] * jnp.exp(last - part + tail)).astype(BF16)
            tail = tail + last
        found.append((mm_tn(values, jnp.concatenate(weighted, axis=0)).astype(BF16), tail))
    return found


def local_mix(query, keys, values, base, cum, reach, column, mixed):
    rows, dk = keys.shape
    count = rows // BLK
    dv = values.shape[1]
    ii = lax.broadcasted_iota(jnp.int32, (BLK, BLK), 0)
    jj = lax.broadcasted_iota(jnp.int32, (BLK, BLK), 1)
    lanes = slice(base, base + dk)
    query = query * dk ** (-0.5)
    inner = [None] * count
    readers = [None] * count
    state = None
    passed = jnp.zeros((1, dk), F32)
    for b in range(count):
        at = slice(b * BLK, (b + 1) * BLK)
        value = values[at]
        cf = cum[0, at, lanes]
        cb = cum[1, at, lanes]
        qf = (query[at] * jnp.exp(cf)).astype(BF16)
        kf = (keys[at] * jnp.exp(-cf)).astype(BF16)
        qr = (query[at] * jnp.exp(cb)).astype(BF16)
        kr = (keys[at] * jnp.exp(-cb)).astype(BF16)
        scores = jnp.where(ii >= jj, mm_nt(qf, kf), 0.0) + jnp.where(ii <= jj, mm_nt(qr, kr), 0.0)
        inner[b] = mm(scores.astype(BF16), value)
        if b > 0:
            inner[b] = inner[b] + mm_nt(qf, state.astype(BF16))
        reach[0, at, lanes] = (query[at] * jnp.exp(cf + passed)).astype(BF16)
        last = cf[BLK - 1 : BLK]
        if b < count - 1:
            gain = mm_tn(value, (keys[at] * jnp.exp(last - cf)).astype(BF16))
            state = gain if b == 0 else jnp.exp(last) * state + gain
        passed = passed + last
        readers[b] = qr
    state = None
    passed = jnp.zeros((1, dk), F32)
    for b in reversed(range(count)):
        at = slice(b * BLK, (b + 1) * BLK)
        cb = cum[1, at, lanes]
        if b < count - 1:
            inner[b] = inner[b] + mm_nt(readers[b], state.astype(BF16))
        reach[1, at, lanes] = (query[at] * jnp.exp(cb + passed)).astype(BF16)
        last = cb[0:1]
        if b > 0:
            gain = mm_tn(values[at], (keys[at] * jnp.exp(last - cb)).astype(BF16))
            state = gain if b == count - 1 else jnp.exp(last) * state + gain
        passed = passed + last
        mixed[at, column : column + dv] = inner[b]


def ring_sum(y, c, order, jump, part, prepare, extra, s, r, ss, sr, finish):
    half = YN // 2

    def mine(way, k):
        return k // (len(order) // 2) == way

    def pass_sum(way, d, k):
        step = jump if d == half else 1
        return remote(
            s.at[way, d - 1, k], r.at[way, d - 1, k], ss.at[int(d == half)], sr.at[d - 1, k],
            {"tp": lax.rem(y + (step if way == 0 else YN - step), YN) * 2 + c},
        )

    def landed(d, k):
        box = r.at[:, d - 1, k]
        remote(box, box, ss.at[0], sr.at[d - 1, k], {"tp": y * 2 + 1 - c}).wait_recv()

    def collect(total, way, d, k):
        if d + 1 < half:
            total = total + r[way, d, k].astype(F32)
        if jump and mine(way, k) and half - jump == d:
            total = total + r[way, half - 1, k].astype(F32)
        return total

    def await_for(d, k):
        if d + 1 < half:
            landed(d + 1, k)
        if jump and half - jump == d:
            way = int(mine(1, k))
            pass_sum(way, half, k).wait_recv()

    def send(way, d, k):
        s[way, d - 1, k] = collect(part(d if way == 0 else YN - d, k), way, d, k).astype(BF16)
        pass_sum(way, d, k).start()

    def send_far():
        if jump:
            prepare(half)
            for k in order:
                for way in range(2):
                    if mine(way, k):
                        send(way, half, k)

    for d in range(half - 1, 0, -1):
        prepare(d)
        prepare(YN - d)
        for k in order:
            await_for(d, k)
            for way in range(2):
                send(way, d, k)
        if d == half - 1:
            send_far()
            extra()
    if half == 1:
        send_far()
        extra()
    prepare(0)
    for k in order:
        total = part(0, k)
        await_for(0, k)
        for way in range(2):
            total = collect(total, way, 0, k)
        finish(k, total)
    if half > 1:
        whole = s.at[:, 0 : half - 1]
        remote(whole, whole, ss.at[0], sr.at[0, 0], {"tp": y * 2 + 1 - c}).wait_send()
    if jump:
        whole = s.at[:, half - 1, 0 : len(order) // 2]
        remote(whole, whole, ss.at[1], sr.at[0, 0], {"tp": y * 2 + 1 - c}).wait_send()


INPUTS = (
    "qa", "ka", "va", "ga", "da", "qb", "kb", "vb", "gb", "db", "head_gain", "pa", "pb", "stream",
    "gain_mix", "gain_moe", "routes", "affinity", "wg", "wu", "wd",
)


def shapes_of(rows, dv, width):
    n = ZN * XN
    m = YN * 2
    half = YN // 2
    own = rows // m
    lanes = width // m
    slots = 3 * rows * 2 // (2 * n)
    count = n // 2
    group = count * slots
    keys = DK_A + DK_B
    piece = dv // XN + dv // (2 * XN)
    big = piece + FADES
    mine = rows // 2
    groups = min(GROUPS, count)
    hops = max(1, half - 1)
    cut = width // CUTS
    v = pltpu.VMEM
    return dict(
        qa=v((DK_A, rows), BF16), ka=v((DK_A, rows), BF16), va=v((rows, dv), BF16), ga=v((rows, dv), BF16),
        da=v((2, DK_A, rows), F32), qb=v((rows, DK_B), BF16), kb=v((rows, DK_B), BF16), vb=v((rows, dv), BF16),
        gb=v((rows, dv), BF16), db=v((2, rows, DK_B), F32), head_gain=v((1, dv), F32),
        stream=v((own, width), BF16), gain_mix=v((1, width), F32), gain_moe=v((1, width), F32),
        routes=v((2, rows), jnp.int32), affinity=v((2, rows), F32),
        pj=v((2, 2, dv, width), BF16), wg=v((2, width, lanes), BF16), wu=v((2, width, lanes), BF16),
        wd=v((2, lanes, width), BF16), early=DMA((16,)), loads=DMA((3,)), swap_s=DMA((5,)), swap_r=DMA((5,)),
        cum=v((2, rows, keys), F32), stack=v((XN, 2, big, DK_B), BF16), xbox=v((XN, 2, big, DK_B), BF16),
        agg=v((2, big, DK_B), BF16), zbox=v((ZN, big, DK_B), BF16), outx=v((XN, 2, piece, DK_B), BF16),
        states=v((XN, 2, piece, DK_B), BF16), xs=DMA, xr=DMA, zs=DMA, zr=DMA,
        es=DMA, er=DMA,
        mixed=v((rows, 2 * dv), F32), reach=v((2, rows, keys), BF16), heads=v((2, mine, 2 * dv), BF16),
        hbox=v((mine, 2 * dv), BF16), hs=DMA((2,)), pp=v((YN, own, width), F32),
        s1=v((2, half, CUTS, own, cut), BF16), r1=v((2, half, CUTS, own, cut), BF16),
        s1s=DMA((2,)), s1r=DMA((half, CUTS)), settled=v((own, width), F32),
        moe_in=v((2, YN, own, lanes), BF16), columns=v((2, rows, lanes), BF16), cs=DMA, cr=DMA,
        hot=v((n * slots, rows), BF16),
        mixhi=v((rows, n * slots), BF16), mixlo=v((rows, n * slots), BF16), picked=v((2, n, slots, lanes), BF16),
        x=v((YN, groups, 2, count // groups, slots, lanes), BF16), acc=v((group, 4 * lanes), F32),
        act=v((group, 2 * lanes), BF16), p=v((YN, group, 2 * lanes), F32),
        s2=v((2, hops, groups, group // groups, 2 * lanes), BF16),
        r2=v((2, hops, groups, group // groups, 2 * lanes), BF16), s2s=DMA((2,)),
        s2r=DMA((hops, groups)), q=v((2, 2, count, slots, lanes), BF16), pieces=v((2, n, slots, lanes), BF16),
        term=v((2, rows, lanes), BF16), mixbox=v((2, m, own, lanes), BF16), ds=DMA((2, 2)), dr=DMA((groups + 1,)),
        gs=DMA, gr=DMA((hops, groups)), bs=DMA((2, 2)), br=DMA((2,)),
        fs=DMA((2,)), fr=DMA((2,)),
    )


def layer_kernel(scratch_names, *refs):
    hbm = dict(zip(INPUTS, refs))
    out = refs[len(INPUTS)]
    v = dict(zip(scratch_names, refs[len(INPUTS) + 1 :]))
    sp = lax.axis_index("sp")
    tp = lax.axis_index("tp")
    z, xx, y, c = sp // XN, lax.rem(sp, XN), tp // 2, lax.rem(tp, 2)
    n = ZN * XN
    m = YN * 2
    half = YN // 2
    per = XN // 2
    picked, x, acc, act, p, q, pieces = (v[i] for i in ("picked", "x", "acc", "act", "p", "q", "pieces"))
    slots = picked.shape[2]
    count = ZN * per
    group = count * slots
    lanes = picked.shape[3]
    groups = x.shape[1]
    size = count // groups
    rows = v["columns"].shape[1]
    own = rows // m
    partner = {"tp": tp + 1 - 2 * c}

    def rows_of(i):
        return pl.ds(pl.multiple_of(i * own, own), own)

    fetch = {}
    order = (
        "ka", "kb", "da", "db", "va", "vb", "qa", "qb", "ga", "gb", "head_gain", "routes", "affinity", "stream",
        "gain_mix", "gain_moe",
    )
    for i, name in enumerate(order):
        src = hbm[name].at[rows_of(tp), :] if name == "stream" else hbm[name]
        fetch[name] = pltpu.make_async_copy(src, v[name], v["early"].at[max(0, i - 5)])
        if i < 6:
            fetch[name].start()
    barrier = pltpu.get_barrier_semaphore()
    def far(dz, dx, dy):
        return near(dz, ZN) + near(dx, XN) + near(dy, YN)

    friends = [
        (far(dz, dx, 0), {"sp": sp_at(z, xx, dz, dx), "tp": y * 2 + core})
        for dz in range(ZN) for dx in range(XN) for core in range(2) if dz or dx
    ] + [(far(0, 0, k // 2), {"tp": lax.rem(tp + k, m)}) for k in range(1, m)]
    for _, peer in sorted(friends, key=lambda f: -f[0]):
        pl.semaphore_signal(barrier, inc=1, device_id=peer, device_id_type=MESH)
    greeted = len(friends)

    for i, name in enumerate(order):
        if i >= 6:
            fetch[name].start()
    for i, name in enumerate(("pa", "pb")):
        fetch[name] = pltpu.make_async_copy(hbm[name], v["pj"].at[0, i], v["early"].at[len(order) - 5])
        fetch[name].start()
    pairs = [(hbm[name].at[0], v[name]) for name in ("wg", "wu", "wd")]
    loads = [pltpu.make_async_copy(src, dst.at[0], v["loads"].at[i]) for i, (src, dst) in enumerate(pairs)]
    for load in loads:
        load.start()
    swaps = [
        remote(src, dst, v["swap_s"].at[i], v["swap_r"].at[i], partner)
        for i, (src, dst) in enumerate(
            [(hbm["pa"], v["pj"].at[1, 0]), (hbm["pb"], v["pj"].at[1, 1])] + [(s, d.at[1]) for s, d in pairs]
        )
    ]

    first = acc.at[0 : rows * 19 * DK_B // (16 * lanes)]
    pltpu.make_async_copy(first, first, v["early"].at[0]).wait()
    cum, stack = v["cum"], v["stack"]
    keys_a = v["ka"][...].astype(F32).T
    keys_b = v["kb"][...].astype(F32)
    found_b = local_states(keys_b, v["vb"][...], [v["db"][i] for i in range(2)], 0, cum)
    found_a = local_states(keys_a, v["va"][...], [v["da"][i].T for i in range(2)], DK_B, cum)
    dv = v["va"].shape[1]
    tall_b, tall_a = dv // XN, dv // (2 * XN)
    piece = tall_b + tall_a
    for way in range(2):
        (state_a, fade_a), (state_b, fade_b) = found_a[way], found_b[way]
        state_a = jnp.concatenate([state_a[0 : dv // 2], state_a[dv // 2 : dv]], axis=1)
        fades = fade_rows(jnp.concatenate([fade_a, fade_a], axis=1), fade_b)
        for i in range(XN):
            stack[i, way, 0:tall_b] = state_b[i * tall_b : (i + 1) * tall_b]
            stack[i, way, tall_b:piece] = state_a[i * tall_a : (i + 1) * tall_a]
            stack[i, way, piece : piece + FADES] = fades

    pl.semaphore_wait(barrier, greeted)

    xbox, agg, zbox, outx, states = (v[i] for i in ("xbox", "agg", "zbox", "outx", "states"))

    def along_x(j):
        peer = lax.rem(xx + j, XN)
        return remote(stack.at[peer], xbox.at[xx], v["xs"], v["xr"], {"sp": z * XN + peer})

    def along_z(j):
        peer = lax.rem(z + j, ZN)
        way = jnp.where(peer > z, 0, 1)
        return remote(agg.at[way], zbox.at[z], v["zs"], v["zr"], {"sp": peer * XN + xx})

    def back_x(j):
        peer = lax.rem(xx + j, XN)
        return remote(outx.at[peer], states.at[xx], v["es"], v["er"], {"sp": z * XN + peer})

    far_x = sorted(range(1, XN), key=lambda j: -near(j, XN))
    far_z = sorted(range(1, ZN), key=lambda j: -near(j, ZN))
    for j in far_x:
        along_x(j).start()
    for swap in swaps:
        swap.start()
    xbox[xx] = stack[xx]
    zbox[z] = jnp.zeros_like(zbox[z])

    for name in ("qa", "qb"):
        fetch[name].wait()
    mixed, reach = v["mixed"], v["reach"]
    local_mix(v["qa"][...].astype(F32).T, keys_a, v["va"][...], DK_B, cum, reach, 0, mixed)

    def load(block):
        block = block.astype(F32)
        fades = block[piece : piece + FADES]
        return (block[0:tall_b], block[tall_b:piece]), (fades[0:1] + fades[1:2], fades[2:3] + fades[3:4])

    def advance(state, block):
        own, fade = load(block)
        return tuple(jnp.exp(f) * s + o for f, s, o in zip(fade, state, own))

    def keep(ref, at, state):
        ref[at + (slice(0, tall_b),)] = state[0].astype(BF16)
        ref[at + (slice(tall_b, piece),)] = state[1].astype(BF16)

    def all_of(box, size, send, recv):
        box = box.at[0 : size - 1]
        return remote(box, box, send, recv, partner)

    if XN > 1:
        all_of(xbox, XN, v["xs"], v["xr"]).wait_recv()
    for way in range(2):
        state, fades = None, None
        for i in range(XN) if way == 0 else reversed(range(XN)):
            own_state, own_fade = load(xbox[i, way])
            state = own_state if state is None else advance(state, xbox[i, way])
            fades = own_fade if fades is None else tuple(a + b for a, b in zip(fades, own_fade))
        keep(agg, (way,), state)
        agg[way, piece : piece + FADES] = fade_rows(fades[1], fades[0])
    for j in far_z:
        along_z(j).start()

    local_mix(v["qb"][...].astype(F32), keys_b, v["vb"][...], 0, cum, reach, dv, mixed)
    for name in ("routes", "affinity"):
        fetch[name].wait()
    routes, affinity = v["routes"][...], v["affinity"][...]
    lane = lax.broadcasted_iota(jnp.int32, (n, rows), 0)
    hots = [routes[i : i + 1] == lane for i in range(2)]
    named = sum(jnp.where(h, 1.0, 0.0) for h in hots)
    ii = lax.broadcasted_iota(jnp.int32, (rows, rows), 0)
    jj = lax.broadcasted_iota(jnp.int32, (rows, rows), 1)
    before = mm(named.astype(BF16), jnp.where(ii < jj, 1.0, 0.0).astype(BF16))
    place = [
        routes[i : i + 1] * slots
        + jnp.sum(jnp.where(hots[i], before, 0.0), axis=0, keepdims=True).astype(jnp.int32)
        for i in range(2)
    ]
    seat = lax.broadcasted_iota(jnp.int32, (n * slots, rows), 0)
    v["hot"][...] = jnp.where((seat == place[0]) | (seat == place[1]), 1.0, 0.0).astype(BF16)
    weights = [affinity[i : i + 1] / (affinity[0:1] + affinity[1:2]) for i in range(2)]
    mix = jnp.where(seat == place[0], weights[0], jnp.where(seat == place[1], weights[1], 0.0)).T
    high = mix.astype(BF16)
    v["mixhi"][...] = high
    v["mixlo"][...] = (mix - high.astype(F32)).astype(BF16)

    if ZN > 1:
        all_of(zbox, ZN, v["zs"], v["zr"]).wait_recv()
    start = tuple(jnp.zeros((tall, zbox.shape[2]), F32) for tall in (tall_b, tall_a))
    ahead, behind = start, start
    for i in range(ZN):
        ahead = tuple(jnp.where(i < z, a, b) for a, b in zip(advance(ahead, zbox[i]), ahead))
    for i in reversed(range(ZN)):
        behind = tuple(jnp.where(i > z, a, b) for a, b in zip(advance(behind, zbox[i]), behind))
    for i in range(XN):
        keep(outx, (i, 0), ahead)
        if i < XN - 1:
            ahead = advance(ahead, xbox[i, 0])
    for i in reversed(range(XN)):
        keep(outx, (i, 1), behind)
        if i > 0:
            behind = advance(behind, xbox[i, 1])
    for j in far_x:
        back_x(j).start()
    states[xx] = outx[xx]
    for name in ("ga", "gb", "head_gain", "stream", "gain_mix", "gain_moe"):
        fetch[name].wait()
    pltpu.make_async_copy(v["pj"].at[0], v["pj"].at[0], v["early"].at[len(order) - 5]).wait()
    if XN > 1:
        all_of(states, XN, v["es"], v["er"]).wait_recv()

    heads, hbox = v["heads"], v["hbox"]
    for i, (base, dk, gate) in enumerate(((DK_B, DK_A, v["ga"]), (0, DK_B, v["gb"]))):
        whole = mixed[:, i * dv : (i + 1) * dv]
        for way in range(2):
            if i == 0:
                start = states[:, way, tall_b:piece].reshape(dv // 2, 2 * DK_A)
                start = jnp.concatenate([start[:, 0:DK_A], start[:, DK_A:]], axis=0)
            else:
                start = states[:, way, 0:tall_b].reshape(dv, DK_B)
            whole = whole + mm_nt(reach[way, :, base : base + dk], start)
        scale = lax.rsqrt(jnp.mean(whole * whole, axis=-1, keepdims=True) + 1e-06)
        value = (whole * scale * v["head_gain"][...] * silu(gate[...].astype(F32))).astype(BF16)
        value = value.reshape(YN, 2, own, dv)
        for core in range(2):
            heads[core, :, i * dv : (i + 1) * dv] = value[:, core].reshape(YN * own, dv)
    hand = remote(heads.at[1 - c], hbox, v["hs"].at[0], v["hs"].at[1], partner)
    hand.start()
    pj, pp = v["pj"], v["pp"]
    pp[...] = (mm(heads[c], pj[0].reshape(2 * dv, pj.shape[3]))).reshape(pp.shape)
    swaps[0].wait_recv()
    swaps[1].wait_recv()
    hand.wait_recv()
    pp[...] = pp[...] + (mm(hbox[...], pj[1].reshape(2 * dv, pj.shape[3]))).reshape(pp.shape)

    settled, moe_in, columns = v["settled"], v["moe_in"], v["columns"]
    cut = v["s1"].shape[4]

    def attn_part(o, k):
        return pp[lax.rem(y + o, YN), :, k * cut : (k + 1) * cut]

    def attn_done(k, total):
        settled[:, k * cut : (k + 1) * cut] = total

    ring_sum(
        y, c, [k // 2 + CUTS // 2 * (k % 2) for k in range(CUTS)], min(3, half), attn_part, lambda o: None,
        lambda: None, v["s1"], v["r1"], v["s1s"], v["s1r"], attn_done,
    )
    value = layer_norm(v["stream"][...].astype(F32) + settled[...], v["gain_mix"][...])
    settled[...] = value
    value = value.astype(BF16)
    for i in range(m):
        moe_in[i // YN, i % YN] = value[:, i * lanes : (i + 1) * lanes]

    far_tp = sorted(range(1, m), key=lambda k: -near(k // 2, YN))

    def to_columns(k):
        peer = lax.rem(tp + k, m)
        return remote(
            moe_in.at[:, lax.rem(peer, YN)], columns.at[:, rows_of(tp), :], v["cs"], v["cr"], {"tp": peer}
        )

    for k in far_tp:
        to_columns(k).start()
    columns[:, rows_of(tp), :] = moe_in[:, lax.rem(tp, YN)]
    most = columns.at[:, 0 : rows - own, :]
    all_columns = remote(most, most, v["cs"], v["cr"], partner)
    all_columns.wait_recv()
    wide = mm(v["hot"][...], jnp.concatenate([columns[0], columns[1]], axis=1)).astype(BF16)
    for i in range(2):
        picked[i] = wide[:, i * lanes : (i + 1) * lanes].reshape(n, slots, lanes)

    z_order = sorted(range(ZN), key=lambda d: near(d, ZN))
    z_rank = [z_order.index(d) for d in range(ZN)]

    def block_of(o):
        return lax.rem(y + o * half, YN)

    def seat_of(b, k, j):
        return x.at[b, j // size, k, j % size]

    def dispatch(o, dz, dx):
        e = sp_at(z, xx, dz, dx)
        rz, rx = (-dz) % ZN, (-dx) % XN
        j = z_rank[rz] * per + rx // 2
        b = block_of(o)
        return remote(
            picked.at[b // half, e], seat_of(b, c, j), v["ds"].at[o, int(dz + dx == 0)], v["dr"].at[groups if o else j // size],
            {"sp": e, "tp": y * 2 + dx % 2},
        )

    homes = [
        pltpu.make_async_copy(picked.at[block_of(o) // half, sp], seat_of(block_of(o), 0, 0), v["dr"].at[groups if o else 0])
        for o in range(2)
    ]
    offsets = sorted(
        [(dz, dx) for dz in range(ZN) for dx in range(XN)], key=lambda o: (z_rank[-o[0] % ZN], -near(o[1], XN))
    )
    def send_wave(o):
        for dz, dx in offsets:
            if dz or dx:
                dispatch(o, dz, dx).start()
        pl.when(c == 0)(lambda: homes[o].start())
        pl.when(c == 1)(lambda: dispatch(o, 0, 0).start())

    send_wave(0)

    def arrive(g):
        block = x.at[block_of(0), g]
        remote(block, block, v["ds"].at[0, 0], v["dr"].at[g], partner).wait_recv()

    def arrive_opposite():
        block = x.at[block_of(1)]
        remote(block, block, v["ds"].at[1, 0], v["dr"].at[groups], partner).wait_recv()
        widen(block_of(1))

    def hop(way, h, g, behind=0):
        step = step_of(way)
        b = lax.rem(y + (h - 1 + behind) * (YN - step), YN)
        return remote(
            x.at[b, g], x.at[b, g], v["gs"], v["gr"].at[h - 1, g],
            {"tp": lax.rem(y + step, YN) * 2 + c},
        )

    wg, wu, wd = v["wg"], v["wu"], v["wd"]

    def widen(b, first=False):
        at = pl.ds(pl.multiple_of(b * 2 * lanes, 2 * lanes), 2 * lanes)
        block = jnp.concatenate([x[b, :, k].reshape(group, lanes) for k in range(2)], axis=1)
        w = jnp.concatenate([ref[i, at, :] for ref in (wg, wu) for i in range(2)], axis=1)
        value = mm(block, w)
        acc[...] = value if first else acc[...] + value

    def land(h, g):
        pair = x.at[0:2, g]
        remote(pair, pair, v["gs"], v["gr"].at[h - 1, g], partner).wait_recv()

    turns = sorted(
        [(h, g) for h in range(max(1, half)) for g in range(groups)], key=lambda t: (t[1] + LAG * t[0], t[0])
    )
    for h, g in turns:
        if h == half - 1 and h > 0 and g == 0:
            arrive_opposite()
        if h == 0:
            arrive(g)
        else:
            land(h, g)
        if h < half - 1:
            for way in range(2):
                hop(way, h + 1, g).start()
        if g < groups - 1:
            continue
        if h == 0:
            send_wave(1)
            for load_w in loads:
                load_w.wait()
            for swap in swaps[2:]:
                swap.wait_recv()
            widen(y, first=True)
        else:
            widen(lax.rem(y + YN - h, YN))
            widen(lax.rem(y + h, YN))
    if half == 1:
        arrive_opposite()

    hidden = 2 * lanes
    act[...] = (silu(acc[:, :hidden]) * acc[:, hidden:]).astype(BF16)

    def narrow(o):
        b = lax.rem(y + o, YN)
        at = pl.ds(pl.multiple_of(b * hidden, hidden), hidden)
        p[o] = mm(act[...], jnp.concatenate([wd[i, :, at] for i in range(2)], axis=0))

    def give(o, k, j):
        rz = z_order[j // per]
        rx = 2 * (j % per) + c
        return remote(
            q.at[o, k, j], pieces.at[o, sp], v["bs"].at[o, int(k + j == 0)], v["br"].at[o],
            {"sp": sp_at(z, xx, rz, rx), "tp": y * 2 + k},
        )

    returns = [pltpu.make_async_copy(q.at[o, 0, 0], pieces.at[o, sp], v["br"].at[o]) for o in range(2)]

    def give_back(o, j):
        for k in range(2):
            if k == 0 and j == 0:
                pl.when(c == 0)(lambda: returns[o].start())
                pl.when(c == 1)(lambda: give(o, 0, 0).start())
            else:
                give(o, k, j).start()

    def opposite():
        narrow(half)
        for k in range(2):
            q[1, k] = p[half, :, k * lanes : (k + 1) * lanes].astype(BF16).reshape(count, slots, lanes)
        for j in reversed(range(count)):
            give_back(1, j)

    tall = group // groups

    def moe_done(g, total):
        total = total.astype(BF16)
        js = range(g * size, (g + 1) * size)
        for k in range(2):
            q[0, k, g * size : (g + 1) * size] = total[:, k * lanes : (k + 1) * lanes].reshape(size, slots, lanes)
        for j in reversed(js):
            give_back(0, j)

    ring_sum(
        y, c, list(reversed(range(groups))), 0, lambda o, g: p[o, g * tall : (g + 1) * tall, :], narrow, opposite,
        v["s2"], v["r2"], v["s2s"], v["s2r"], moe_done,
    )
    term, mixbox = v["term"], v["mixbox"]

    def spread_rows(o, k):
        peer = lax.rem(tp + k, m)
        return remote(term.at[o, rows_of(peer), :], mixbox.at[o, tp], v["fs"].at[o], v["fr"].at[o], {"tp": peer})

    for o in (1, 0):
        whole = pieces.at[o]
        remote(whole, whole, v["bs"].at[o, 0], v["br"].at[o], partner).wait_recv()
        flat = pieces[o].reshape(n * slots, lanes)
        term[o] = (mm(v["mixhi"][...], flat) + mm(v["mixlo"][...], flat)).astype(BF16)
        for k in far_tp:
            spread_rows(o, k).start()
        mixbox[o, tp] = term[o, rows_of(tp), :]
    row_waits = []
    for o in (1, 0):
        whole = mixbox.at[o, 0 : m - 1]
        row_waits.append(remote(whole, whole, v["fs"].at[o], v["fr"].at[o], partner))
        row_waits[-1].wait_recv()
    mixture = jnp.concatenate(
        [mixbox[0, i].astype(F32) + mixbox[1, (i + YN) % m].astype(F32) for i in range(m)], axis=1
    )
    out[...] = layer_norm(settled[...] + mixture, v["gain_moe"][...]).astype(BF16)

    if XN > 1:
        all_of(xbox, XN, v["xs"], v["xr"]).wait_send()
        all_of(states, XN, v["es"], v["er"]).wait_send()
    if ZN > 1:
        all_of(zbox, ZN, v["zs"], v["zr"]).wait_send()
    hand.wait_send()
    for swap in swaps:
        swap.wait_send()
    all_columns.wait_send()
    for wait in row_waits:
        wait.wait_send()
    for o in range(2):
        most = picked.at[0, 0 : n - 1]
        remote(most, most, v["ds"].at[o, 0], v["dr"].at[o], partner).wait_send()
        pl.when(c == 1)(lambda: dispatch(o, 0, 0).wait_send())
        most = pieces.at[o, 0 : n - 1]
        remote(most, most, v["bs"].at[o, 0], v["br"].at[o], partner).wait_send()
        pl.when(c == 1)(lambda: give(o, 0, 0).wait_send())
    if half > 1:
        whole = x.at[0 : 2 * (half - 1)]
        remote(whole, whole, v["gs"], v["gr"].at[0, 0], partner).wait_send()


def body(
    query_one, key_one, value_one, gate_one, decay_one, query_two, key_two, value_two, gate_two, decay_two,
    head_gain, proj_one, proj_two, stream, gain_mix, gain_moe, routes, affinity, expert_gate, expert_up,
    expert_down,
):
    rows, width = stream.shape
    dv = head_gain.shape[0]
    scratch = shapes_of(rows, dv, width)
    return pl.pallas_call(
        functools.partial(layer_kernel, tuple(scratch)),
        out_shape=jax.ShapeDtypeStruct((rows // (YN * 2), width), BF16),
        in_specs=[ANY] * len(INPUTS),
        out_specs=VMEM,
        scratch_shapes=list(scratch.values()),
        compiler_params=pltpu.CompilerParams(
            vmem_limit_bytes=56 * 2**20, collective_id=1, has_side_effects=True
        ),
    )(
        query_one.T, key_one.T, value_one, gate_one, jnp.swapaxes(decay_one, 1, 2), query_two, key_two, value_two,
        gate_two, decay_two, head_gain.reshape(1, -1), proj_one, proj_two, stream, gain_mix.reshape(1, -1),
        gain_moe.reshape(1, -1), routes.T, affinity.T, expert_gate, expert_up, expert_down,
    )


def solution(mesh):
    return jax.shard_map(
        body,
        mesh=mesh,
        in_specs=(
            P("sp", "tp"),
            P("sp", "tp"),
            P("sp", "tp"),
            P("sp", "tp"),
            P(None, "sp", "tp"),
            P("sp", "tp"),
            P("sp", "tp"),
            P("sp", "tp"),
            P("sp", "tp"),
            P(None, "sp", "tp"),
            P(),
            P("tp", None),
            P("tp", None),
            P("sp", None),
            P(),
            P(),
            P("sp", None),
            P("sp", None),
            P("sp", None, "tp"),
            P("sp", None, "tp"),
            P("sp", "tp", None),
        ),
        out_specs=P(("sp", "tp"), None),
        check_vma=False,
    )
```

```python
import functools

import jax
import jax.numpy as jnp
from jax import lax
from jax.experimental import pallas as pl
from jax.experimental.pallas import tpu as pltpu
from jax.sharding import PartitionSpec as P

DK_A = 64
DK_B = 128
BLK = 64
SHARPNESS = 16.0
ZN, XN, YN = 8, 4, 8
CUTS = 4
GROUPS = 8
LAG = 20
FADES = 8
F32 = jnp.float32
BF16 = jnp.bfloat16
MESH = pl.DeviceIdType.MESH
VMEM = pl.BlockSpec(memory_space=pltpu.VMEM)
ANY = pl.BlockSpec(memory_space=pl.ANY)
DMA = pltpu.SemaphoreType.DMA


def mm(a, b):
    return jnp.dot(a, b, preferred_element_type=F32)


def mm_nt(a, b):
    return lax.dot_general(a, b, (((1,), (1,)), ((), ())), preferred_element_type=F32)


def mm_tn(a, b):
    return lax.dot_general(a, b, (((0,), (0,)), ((), ())), preferred_element_type=F32)


def log_sigmoid(x):
    return jnp.minimum(x, 0.0) - jnp.log1p(jnp.exp(-jnp.abs(x)))


def silu(x):
    return x / (1.0 + jnp.exp(-x))


def layer_norm(values, gain):
    mean = jnp.mean(values, axis=-1, keepdims=True)
    spread = jnp.mean(jnp.square(values - mean), axis=-1, keepdims=True)
    return (values - mean) * lax.rsqrt(spread + 1e-05) * gain


def remote(src, dst, send, recv, peer):
    return pltpu.make_async_remote_copy(
        src_ref=src, dst_ref=dst, send_sem=send, recv_sem=recv, device_id=peer, device_id_type=MESH
    )


def sp_at(z, x, dz, dx):
    return lax.rem(z + dz, ZN) * XN + lax.rem(x + dx, XN)


def near(d, n):
    return min(d, n - d)


def step_of(way):
    return 1 if way == 0 else YN - 1


def split_fade(total):
    high = total.astype(BF16).astype(F32)
    return high, total - high


def fade_rows(fade_a, fade_b):
    row = lax.broadcasted_iota(jnp.int32, (FADES, fade_b.shape[1]), 0)
    rows = 0.0
    for i, value in enumerate(split_fade(fade_b) + split_fade(fade_a)):
        rows = jnp.where(row == i, value, rows)
    return rows.astype(BF16)


def local_states(keys, values, decays, base, cum):
    rows, wide = keys.shape
    count = rows // BLK
    ii = lax.broadcasted_iota(jnp.int32, (rows, rows), 0)
    jj = lax.broadcasted_iota(jnp.int32, (rows, rows), 1)
    same = (ii // BLK) == (jj // BLK)
    found = []
    for way in range(2):
        tri = jnp.where(same & ((ii >= jj) if way == 0 else (ii <= jj)), 1.0, 0.0).astype(BF16)
        fade = log_sigmoid(decays[way]) / SHARPNESS
        high = fade.astype(BF16)
        low = (fade - high.astype(F32)).astype(BF16)
        total = mm(tri, high) + mm(tri, low)
        cum[way, :, base : base + wide] = total
        tail = jnp.zeros((1, wide), F32)
        weighted = [None] * count
        for b in reversed(range(count)) if way == 0 else range(count):
            part = total[b * BLK : (b + 1) * BLK]
            last = part[BLK - 1 : BLK] if way == 0 else part[0:1]
            weighted[b] = (keys[b * BLK : (b + 1) * BLK] * jnp.exp(last - part + tail)).astype(BF16)
            tail = tail + last
        found.append((mm_tn(values, jnp.concatenate(weighted, axis=0)).astype(BF16), tail))
    return found


def local_mix(query, keys, values, base, cum, reach, column, mixed):
    rows, dk = keys.shape
    count = rows // BLK
    dv = values.shape[1]
    ii = lax.broadcasted_iota(jnp.int32, (BLK, BLK), 0)
    jj = lax.broadcasted_iota(jnp.int32, (BLK, BLK), 1)
    lanes = slice(base, base + dk)
    query = query * dk ** (-0.5)
    inner = [None] * count
    readers = [None] * count
    state = None
    passed = jnp.zeros((1, dk), F32)
    for b in range(count):
        at = slice(b * BLK, (b + 1) * BLK)
        value = values[at]
        cf = cum[0, at, lanes]
        cb = cum[1, at, lanes]
        qf = (query[at] * jnp.exp(cf)).astype(BF16)
        kf = (keys[at] * jnp.exp(-cf)).astype(BF16)
        qr = (query[at] * jnp.exp(cb)).astype(BF16)
        kr = (keys[at] * jnp.exp(-cb)).astype(BF16)
        scores = jnp.where(ii >= jj, mm_nt(qf, kf), 0.0) + jnp.where(ii <= jj, mm_nt(qr, kr), 0.0)
        inner[b] = mm(scores.astype(BF16), value)
        if b > 0:
            inner[b] = inner[b] + mm_nt(qf, state.astype(BF16))
        reach[0, at, lanes] = (query[at] * jnp.exp(cf + passed)).astype(BF16)
        last = cf[BLK - 1 : BLK]
        if b < count - 1:
            gain = mm_tn(value, (keys[at] * jnp.exp(last - cf)).astype(BF16))
            state = gain if b == 0 else jnp.exp(last) * state + gain
        passed = passed + last
        readers[b] = qr
    state = None
    passed = jnp.zeros((1, dk), F32)
    for b in reversed(range(count)):
        at = slice(b * BLK, (b + 1) * BLK)
        cb = cum[1, at, lanes]
        if b < count - 1:
            inner[b] = inner[b] + mm_nt(readers[b], state.astype(BF16))
        reach[1, at, lanes] = (query[at] * jnp.exp(cb + passed)).astype(BF16)
        last = cb[0:1]
        if b > 0:
            gain = mm_tn(values[at], (keys[at] * jnp.exp(last - cb)).astype(BF16))
            state = gain if b == count - 1 else jnp.exp(last) * state + gain
        passed = passed + last
        mixed[at, column : column + dv] = inner[b]


def ring_sum(y, c, order, jump, part, prepare, extra, s, r, ss, sr, finish):
    half = YN // 2

    def mine(way, k):
        return k // (len(order) // 2) == way

    def pass_sum(way, d, k):
        step = jump if d == half else 1
        return remote(
            s.at[way, d - 1, k], r.at[way, d - 1, k], ss.at[int(d == half)], sr.at[d - 1, k],
            {"tp": lax.rem(y + (step if way == 0 else YN - step), YN) * 2 + c},
        )

    def landed(d, k):
        box = r.at[:, d - 1, k]
        remote(box, box, ss.at[0], sr.at[d - 1, k], {"tp": y * 2 + 1 - c}).wait_recv()

    def collect(total, way, d, k):
        if d + 1 < half:
            total = total + r[way, d, k].astype(F32)
        if jump and mine(way, k) and half - jump == d:
            total = total + r[way, half - 1, k].astype(F32)
        return total

    def await_for(d, k):
        if d + 1 < half:
            landed(d + 1, k)
        if jump and half - jump == d:
            way = int(mine(1, k))
            pass_sum(way, half, k).wait_recv()

    def send(way, d, k):
        s[way, d - 1, k] = collect(part(d if way == 0 else YN - d, k), way, d, k).astype(BF16)
        pass_sum(way, d, k).start()

    def send_far():
        if jump:
            prepare(half)
            for k in order:
                for way in range(2):
                    if mine(way, k):
                        send(way, half, k)

    for d in range(half - 1, 0, -1):
        prepare(d)
        prepare(YN - d)
        for k in order:
            await_for(d, k)
            for way in range(2):
                send(way, d, k)
        if d == half - 1:
            send_far()
            extra()
    if half == 1:
        send_far()
        extra()
    prepare(0)
    for k in order:
        total = part(0, k)
        await_for(0, k)
        for way in range(2):
            total = collect(total, way, 0, k)
        finish(k, total)
    if half > 1:
        whole = s.at[:, 0 : half - 1]
        remote(whole, whole, ss.at[0], sr.at[0, 0], {"tp": y * 2 + 1 - c}).wait_send()
    if jump:
        whole = s.at[:, half - 1, 0 : len(order) // 2]
        remote(whole, whole, ss.at[1], sr.at[0, 0], {"tp": y * 2 + 1 - c}).wait_send()


INPUTS = (
    "qa", "ka", "va", "ga", "da", "qb", "kb", "vb", "gb", "db", "head_gain", "pa", "pb", "stream",
    "gain_mix", "gain_moe", "routes", "affinity", "wg", "wu", "wd",
)


def shapes_of(rows, dv, width):
    n = ZN * XN
    m = YN * 2
    half = YN // 2
    own = rows // m
    lanes = width // m
    slots = 3 * rows * 2 // (2 * n)
    count = n // 2
    group = count * slots
    keys = DK_A + DK_B
    piece = dv // XN + dv // (2 * XN)
    big = piece + FADES
    mine = rows // 2
    groups = min(GROUPS, count)
    hops = max(1, half - 1)
    cut = width // CUTS
    v = pltpu.VMEM
    return dict(
        qa=v((DK_A, rows), BF16), ka=v((DK_A, rows), BF16), va=v((rows, dv), BF16), ga=v((rows, dv), BF16),
        da=v((2, DK_A, rows), F32), qb=v((rows, DK_B), BF16), kb=v((rows, DK_B), BF16), vb=v((rows, dv), BF16),
        gb=v((rows, dv), BF16), db=v((2, rows, DK_B), F32), head_gain=v((1, dv), F32),
        stream=v((own, width), BF16), gain_mix=v((1, width), F32), gain_moe=v((1, width), F32),
        routes=v((2, rows), jnp.int32), affinity=v((2, rows), F32),
        pj=v((2, 2, dv, width), BF16), wg=v((2, width, lanes), BF16), wu=v((2, width, lanes), BF16),
        wd=v((2, lanes, width), BF16), early=DMA((16,)), loads=DMA((3,)), swap_s=DMA((5,)), swap_r=DMA((5,)),
        cum=v((2, rows, keys), F32), stack=v((XN, 2, big, DK_B), BF16), xbox=v((XN, 2, big, DK_B), BF16),
        agg=v((2, big, DK_B), BF16), zbox=v((ZN, big, DK_B), BF16), outx=v((XN, 2, piece, DK_B), BF16),
        states=v((XN, 2, piece, DK_B), BF16), xs=DMA, xr=DMA, zs=DMA, zr=DMA,
        es=DMA, er=DMA,
        mixed=v((rows, 2 * dv), F32), shine=v((rows, 2 * dv), F32), reach=v((2, rows, keys), BF16), heads=v((2, mine, 2 * dv), BF16),
        hbox=v((mine, 2 * dv), BF16), hs=DMA((2,)), pp=v((YN, own, width), F32),
        s1=v((2, half, CUTS, own, cut), BF16), r1=v((2, half, CUTS, own, cut), BF16),
        s1s=DMA((2,)), s1r=DMA((half, CUTS)), settled=v((own, width), F32),
        moe_in=v((2, YN, own, lanes), BF16), columns=v((2, rows, lanes), BF16), cs=DMA, cr=DMA,
        hot=v((n * slots, rows), BF16),
        mixhi=v((rows, n * slots), BF16), mixlo=v((rows, n * slots), BF16), picked=v((2, n, slots, lanes), BF16),
        x=v((YN, groups, 2, count // groups, slots, lanes), BF16), acc=v((group, 4 * lanes), F32),
        act=v((group, 2 * lanes), BF16), p=v((YN, group, 2 * lanes), F32),
        s2=v((2, hops, groups, group // groups, 2 * lanes), BF16),
        r2=v((2, hops, groups, group // groups, 2 * lanes), BF16), s2s=DMA((2,)),
        s2r=DMA((hops, groups)), q=v((2, 2, count, slots, lanes), BF16), pieces=v((2, n, slots, lanes), BF16),
        term=v((2, rows, lanes), BF16), mixbox=v((2, m, own, lanes), BF16), ds=DMA((2, 2)), dr=DMA((groups + 1,)),
        gs=DMA, gr=DMA((hops, groups)), bs=DMA((2, 2)), br=DMA((2,)),
        fs=DMA((2,)), fr=DMA((2,)),
    )


def layer_kernel(scratch_names, *refs):
    hbm = dict(zip(INPUTS, refs))
    out = refs[len(INPUTS)]
    v = dict(zip(scratch_names, refs[len(INPUTS) + 1 :]))
    sp = lax.axis_index("sp")
    tp = lax.axis_index("tp")
    z, xx, y, c = sp // XN, lax.rem(sp, XN), tp // 2, lax.rem(tp, 2)
    n = ZN * XN
    m = YN * 2
    half = YN // 2
    per = XN // 2
    picked, x, acc, act, p, q, pieces = (v[i] for i in ("picked", "x", "acc", "act", "p", "q", "pieces"))
    slots = picked.shape[2]
    count = ZN * per
    group = count * slots
    lanes = picked.shape[3]
    groups = x.shape[1]
    size = count // groups
    rows = v["columns"].shape[1]
    own = rows // m
    partner = {"tp": tp + 1 - 2 * c}

    def rows_of(i):
        return pl.ds(pl.multiple_of(i * own, own), own)

    fetch = {}
    order = (
        "ka", "kb", "da", "db", "va", "vb", "qa", "qb", "ga", "gb", "head_gain", "routes", "affinity", "stream",
        "gain_mix", "gain_moe",
    )
    for i, name in enumerate(order):
        src = hbm[name].at[rows_of(tp), :] if name == "stream" else hbm[name]
        fetch[name] = pltpu.make_async_copy(src, v[name], v["early"].at[max(0, i - 5)])
        if i < 6:
            fetch[name].start()
    barrier = pltpu.get_barrier_semaphore()
    def far(dz, dx, dy):
        return near(dz, ZN) + near(dx, XN) + near(dy, YN)

    friends = [
        (far(dz, dx, 0), {"sp": sp_at(z, xx, dz, dx)})
        for dz in range(ZN) for dx in range(XN) if (dz == 0) != (dx == 0)
    ] + [(far(0, 0, k // 2), {"tp": lax.rem(tp + k, m)}) for k in range(1, m)]
    for _, peer in sorted(friends, key=lambda f: -f[0]):
        pl.semaphore_signal(barrier, inc=1, device_id=peer, device_id_type=MESH)
    greeted = len(friends)

    for i, name in enumerate(order):
        if i >= 6:
            fetch[name].start()
    for i, name in enumerate(("pa", "pb")):
        fetch[name] = pltpu.make_async_copy(hbm[name], v["pj"].at[0, i], v["early"].at[len(order) - 5])
        fetch[name].start()
    pairs = [(hbm[name].at[0], v[name]) for name in ("wg", "wu", "wd")]
    loads = [pltpu.make_async_copy(src, dst.at[0], v["loads"].at[i]) for i, (src, dst) in enumerate(pairs)]
    for load in loads:
        load.start()
    swaps = [
        remote(src, dst, v["swap_s"].at[i], v["swap_r"].at[i], partner)
        for i, (src, dst) in enumerate(
            [(hbm["pa"], v["pj"].at[1, 0]), (hbm["pb"], v["pj"].at[1, 1])] + [(s, d.at[1]) for s, d in pairs]
        )
    ]

    first = acc.at[0 : rows * 19 * DK_B // (16 * lanes)]
    pltpu.make_async_copy(first, first, v["early"].at[0]).wait()
    cum, stack = v["cum"], v["stack"]
    keys_a = v["ka"][...].astype(F32).T
    keys_b = v["kb"][...].astype(F32)
    found_b = local_states(keys_b, v["vb"][...], [v["db"][i] for i in range(2)], 0, cum)
    found_a = local_states(keys_a, v["va"][...], [v["da"][i].T for i in range(2)], DK_B, cum)
    dv = v["va"].shape[1]
    tall_b, tall_a = dv // XN, dv // (2 * XN)
    piece = tall_b + tall_a
    for way in range(2):
        (state_a, fade_a), (state_b, fade_b) = found_a[way], found_b[way]
        state_a = jnp.concatenate([state_a[0 : dv // 2], state_a[dv // 2 : dv]], axis=1)
        fades = fade_rows(jnp.concatenate([fade_a, fade_a], axis=1), fade_b)
        for i in range(XN):
            stack[i, way, 0:tall_b] = state_b[i * tall_b : (i + 1) * tall_b]
            stack[i, way, tall_b:piece] = state_a[i * tall_a : (i + 1) * tall_a]
            stack[i, way, piece : piece + FADES] = fades

    pl.semaphore_wait(barrier, greeted)

    xbox, agg, zbox, outx, states = (v[i] for i in ("xbox", "agg", "zbox", "outx", "states"))

    def along_x(j):
        peer = lax.rem(xx + j, XN)
        return remote(stack.at[peer], xbox.at[xx], v["xs"], v["xr"], {"sp": z * XN + peer})

    def along_z(j):
        peer = lax.rem(z + j, ZN)
        way = jnp.where(peer > z, 0, 1)
        return remote(agg.at[way], zbox.at[z], v["zs"], v["zr"], {"sp": peer * XN + xx})

    def back_x(j):
        peer = lax.rem(xx + j, XN)
        return remote(outx.at[peer], states.at[xx], v["es"], v["er"], {"sp": z * XN + peer})

    far_x = sorted(range(1, XN), key=lambda j: -near(j, XN))
    far_z = sorted(range(1, ZN), key=lambda j: -near(j, ZN))
    for j in far_x:
        along_x(j).start()
    for swap in swaps:
        swap.start()
    xbox[xx] = stack[xx]
    zbox[z] = jnp.zeros_like(zbox[z])

    for name in ("qa", "qb"):
        fetch[name].wait()
    mixed, reach = v["mixed"], v["reach"]
    local_mix(v["qa"][...].astype(F32).T, keys_a, v["va"][...], DK_B, cum, reach, 0, mixed)

    def load(block):
        block = block.astype(F32)
        fades = block[piece : piece + FADES]
        return (block[0:tall_b], block[tall_b:piece]), (fades[0:1] + fades[1:2], fades[2:3] + fades[3:4])

    def advance(state, block):
        own, fade = load(block)
        return tuple(jnp.exp(f) * s + o for f, s, o in zip(fade, state, own))

    def keep(ref, at, state):
        ref[at + (slice(0, tall_b),)] = state[0].astype(BF16)
        ref[at + (slice(tall_b, piece),)] = state[1].astype(BF16)

    def all_of(box, size, send, recv):
        box = box.at[0 : size - 1]
        return remote(box, box, send, recv, partner)

    if XN > 1:
        all_of(xbox, XN, v["xs"], v["xr"]).wait_recv()
    for way in range(2):
        state, fades = None, None
        for i in range(XN) if way == 0 else reversed(range(XN)):
            own_state, own_fade = load(xbox[i, way])
            state = own_state if state is None else advance(state, xbox[i, way])
            fades = own_fade if fades is None else tuple(a + b for a, b in zip(fades, own_fade))
        keep(agg, (way,), state)
        agg[way, piece : piece + FADES] = fade_rows(fades[1], fades[0])
    for j in far_z:
        along_z(j).start()

    local_mix(v["qb"][...].astype(F32), keys_b, v["vb"][...], 0, cum, reach, dv, mixed)
    for name in ("routes", "affinity", "ga", "gb", "head_gain"):
        fetch[name].wait()
    for i, gate in enumerate((v["ga"], v["gb"])):
        v["shine"][:, i * dv : (i + 1) * dv] = v["head_gain"][...] * silu(gate[...].astype(F32))
    routes, affinity = v["routes"][...], v["affinity"][...]
    lane = lax.broadcasted_iota(jnp.int32, (n, rows), 0)
    hots = [routes[i : i + 1] == lane for i in range(2)]
    named = sum(jnp.where(h, 1.0, 0.0) for h in hots)
    ii = lax.broadcasted_iota(jnp.int32, (rows, rows), 0)
    jj = lax.broadcasted_iota(jnp.int32, (rows, rows), 1)
    before = mm(named.astype(BF16), jnp.where(ii < jj, 1.0, 0.0).astype(BF16))
    place = [
        routes[i : i + 1] * slots
        + jnp.sum(jnp.where(hots[i], before, 0.0), axis=0, keepdims=True).astype(jnp.int32)
        for i in range(2)
    ]
    seat = lax.broadcasted_iota(jnp.int32, (n * slots, rows), 0)
    v["hot"][...] = jnp.where((seat == place[0]) | (seat == place[1]), 1.0, 0.0).astype(BF16)
    weights = [affinity[i : i + 1] / (affinity[0:1] + affinity[1:2]) for i in range(2)]
    mix = jnp.where(seat == place[0], weights[0], jnp.where(seat == place[1], weights[1], 0.0)).T
    high = mix.astype(BF16)
    v["mixhi"][...] = high
    v["mixlo"][...] = (mix - high.astype(F32)).astype(BF16)

    if ZN > 1:
        all_of(zbox, ZN, v["zs"], v["zr"]).wait_recv()
    start = tuple(jnp.zeros((tall, zbox.shape[2]), F32) for tall in (tall_b, tall_a))
    ahead, behind = start, start
    for i in range(ZN):
        ahead = tuple(jnp.where(i < z, a, b) for a, b in zip(advance(ahead, zbox[i]), ahead))
    for i in reversed(range(ZN)):
        behind = tuple(jnp.where(i > z, a, b) for a, b in zip(advance(behind, zbox[i]), behind))
    for i in range(XN):
        keep(outx, (i, 0), ahead)
        if i < XN - 1:
            ahead = advance(ahead, xbox[i, 0])
    for i in reversed(range(XN)):
        keep(outx, (i, 1), behind)
        if i > 0:
            behind = advance(behind, xbox[i, 1])
    for j in far_x:
        back_x(j).start()
    states[xx] = outx[xx]
    for name in ("stream", "gain_mix", "gain_moe"):
        fetch[name].wait()
    pltpu.make_async_copy(v["pj"].at[0], v["pj"].at[0], v["early"].at[len(order) - 5]).wait()
    if XN > 1:
        all_of(states, XN, v["es"], v["er"]).wait_recv()

    heads, hbox = v["heads"], v["hbox"]
    for i, (base, dk) in enumerate(((DK_B, DK_A), (0, DK_B))):
        whole = mixed[:, i * dv : (i + 1) * dv]
        for way in range(2):
            if i == 0:
                start = states[:, way, tall_b:piece].reshape(dv // 2, 2 * DK_A)
                start = jnp.concatenate([start[:, 0:DK_A], start[:, DK_A:]], axis=0)
            else:
                start = states[:, way, 0:tall_b].reshape(dv, DK_B)
            whole = whole + mm_nt(reach[way, :, base : base + dk], start)
        scale = lax.rsqrt(jnp.mean(whole * whole, axis=-1, keepdims=True) + 1e-06)
        value = (whole * scale * v["shine"][:, i * dv : (i + 1) * dv]).astype(BF16)
        value = value.reshape(YN, 2, own, dv)
        for core in range(2):
            heads[core, :, i * dv : (i + 1) * dv] = value[:, core].reshape(YN * own, dv)
    hand = remote(heads.at[1 - c], hbox, v["hs"].at[0], v["hs"].at[1], partner)
    hand.start()
    pj, pp = v["pj"], v["pp"]
    pp[...] = (mm(heads[c], pj[0].reshape(2 * dv, pj.shape[3]))).reshape(pp.shape)
    swaps[0].wait_recv()
    swaps[1].wait_recv()
    hand.wait_recv()
    pp[...] = pp[...] + (mm(hbox[...], pj[1].reshape(2 * dv, pj.shape[3]))).reshape(pp.shape)

    settled, moe_in, columns = v["settled"], v["moe_in"], v["columns"]
    cut = v["s1"].shape[4]

    def attn_part(o, k):
        return pp[lax.rem(y + o, YN), :, k * cut : (k + 1) * cut]

    def attn_done(k, total):
        settled[:, k * cut : (k + 1) * cut] = total

    ring_sum(
        y, c, [k // 2 + CUTS // 2 * (k % 2) for k in range(CUTS)], min(3, half), attn_part, lambda o: None,
        lambda: None, v["s1"], v["r1"], v["s1s"], v["s1r"], attn_done,
    )
    value = layer_norm(v["stream"][...].astype(F32) + settled[...], v["gain_mix"][...])
    settled[...] = value
    value = value.astype(BF16)
    for i in range(m):
        moe_in[i // YN, i % YN] = value[:, i * lanes : (i + 1) * lanes]

    far_tp = sorted(range(1, m), key=lambda k: -near(k // 2, YN))

    def to_columns(k):
        peer = lax.rem(tp + k, m)
        return remote(
            moe_in.at[:, lax.rem(peer, YN)], columns.at[:, rows_of(tp), :], v["cs"], v["cr"], {"tp": peer}
        )

    for k in far_tp:
        to_columns(k).start()
    columns[:, rows_of(tp), :] = moe_in[:, lax.rem(tp, YN)]
    most = columns.at[:, 0 : rows - own, :]
    all_columns = remote(most, most, v["cs"], v["cr"], partner)
    all_columns.wait_recv()

    def pick(o):
        i = lax.rem(y + o * half, YN) // half
        picked[i] = mm(v["hot"][...], columns[i]).astype(BF16).reshape(n, slots, lanes)

    pick(0)

    z_order = sorted(range(ZN), key=lambda d: near(d, ZN))
    z_rank = [z_order.index(d) for d in range(ZN)]

    def block_of(o):
        return lax.rem(y + o * half, YN)

    def seat_of(b, k, j):
        return x.at[b, j // size, k, j % size]

    def dispatch(o, dz, dx):
        e = sp_at(z, xx, dz, dx)
        rz, rx = (-dz) % ZN, (-dx) % XN
        j = z_rank[rz] * per + rx // 2
        b = block_of(o)
        return remote(
            picked.at[b // half, e], seat_of(b, c, j), v["ds"].at[o, int(dz + dx == 0)], v["dr"].at[groups if o else j // size],
            {"sp": e, "tp": y * 2 + dx % 2},
        )

    homes = [
        pltpu.make_async_copy(picked.at[block_of(o) // half, sp], seat_of(block_of(o), 0, 0), v["dr"].at[groups if o else 0])
        for o in range(2)
    ]
    offsets = sorted(
        [(dz, dx) for dz in range(ZN) for dx in range(XN)], key=lambda o: (z_rank[-o[0] % ZN], -near(o[1], XN))
    )
    def send_wave(o):
        for dz, dx in offsets:
            if dz or dx:
                dispatch(o, dz, dx).start()
        pl.when(c == 0)(lambda: homes[o].start())
        pl.when(c == 1)(lambda: dispatch(o, 0, 0).start())

    send_wave(0)
    pick(1)

    def arrive(g):
        block = x.at[block_of(0), g]
        remote(block, block, v["ds"].at[0, 0], v["dr"].at[g], partner).wait_recv()

    def arrive_opposite():
        block = x.at[block_of(1)]
        remote(block, block, v["ds"].at[1, 0], v["dr"].at[groups], partner).wait_recv()
        widen(block_of(1))

    def hop(way, h, g, behind=0):
        step = step_of(way)
        b = lax.rem(y + (h - 1 + behind) * (YN - step), YN)
        return remote(
            x.at[b, g], x.at[b, g], v["gs"], v["gr"].at[h - 1, g],
            {"tp": lax.rem(y + step, YN) * 2 + c},
        )

    wg, wu, wd = v["wg"], v["wu"], v["wd"]

    def widen(b, first=False, low=0, high=groups):
        tall = group // groups
        span = slice(low * tall, high * tall)
        at = pl.ds(pl.multiple_of(b * 2 * lanes, 2 * lanes), 2 * lanes)
        block = jnp.concatenate(
            [x[b, low:high, k].reshape((high - low) * tall, lanes) for k in range(2)], axis=1
        )
        w = jnp.concatenate([ref[i, at, :] for ref in (wg, wu) for i in range(2)], axis=1)
        value = mm(block, w)
        acc[span] = value if first else acc[span] + value

    def land(h, g):
        pair = x.at[0:2, g]
        remote(pair, pair, v["gs"], v["gr"].at[h - 1, g], partner).wait_recv()

    turns = sorted(
        [(h, g) for h in range(max(1, half)) for g in range(groups)], key=lambda t: (t[1] + LAG * t[0], t[0])
    )
    for h, g in turns:
        if h == half - 1 and h > 0 and g == 0:
            arrive_opposite()
        if h == 0:
            arrive(g)
        else:
            land(h, g)
        if h < half - 1:
            for way in range(2):
                hop(way, h + 1, g).start()
        cut_at = groups // 2 if h == half - 1 and h > 0 else 0
        if g < groups - 1 and g + 1 != cut_at:
            continue
        if h == 0:
            send_wave(1)
            for load_w in loads:
                load_w.wait()
            for swap in swaps[2:]:
                swap.wait_recv()
            widen(y, first=True)
        else:
            edges = (0, cut_at) if g + 1 == cut_at else (cut_at, groups)
            widen(lax.rem(y + YN - h, YN), False, *edges)
            widen(lax.rem(y + h, YN), False, *edges)
    if half == 1:
        arrive_opposite()

    hidden = 2 * lanes
    act[...] = (silu(acc[:, :hidden]) * acc[:, hidden:]).astype(BF16)

    def narrow(o):
        b = lax.rem(y + o, YN)
        at = pl.ds(pl.multiple_of(b * hidden, hidden), hidden)
        p[o] = mm(act[...], jnp.concatenate([wd[i, :, at] for i in range(2)], axis=0))

    def give(o, k, j):
        rz = z_order[j // per]
        rx = 2 * (j % per) + c
        return remote(
            q.at[o, k, j], pieces.at[o, sp], v["bs"].at[o, int(k + j == 0)], v["br"].at[o],
            {"sp": sp_at(z, xx, rz, rx), "tp": y * 2 + k},
        )

    returns = [pltpu.make_async_copy(q.at[o, 0, 0], pieces.at[o, sp], v["br"].at[o]) for o in range(2)]

    def give_back(o, j):
        for k in range(2):
            if k == 0 and j == 0:
                pl.when(c == 0)(lambda: returns[o].start())
                pl.when(c == 1)(lambda: give(o, 0, 0).start())
            else:
                give(o, k, j).start()

    def opposite():
        narrow(half)
        for k in range(2):
            q[1, k] = p[half, :, k * lanes : (k + 1) * lanes].astype(BF16).reshape(count, slots, lanes)
        for j in reversed(range(count)):
            give_back(1, j)

    tall = group // groups

    def moe_done(g, total):
        total = total.astype(BF16)
        js = range(g * size, (g + 1) * size)
        for k in range(2):
            q[0, k, g * size : (g + 1) * size] = total[:, k * lanes : (k + 1) * lanes].reshape(size, slots, lanes)
        for j in reversed(js):
            give_back(0, j)

    ring_sum(
        y, c, list(reversed(range(groups))), 0, lambda o, g: p[o, g * tall : (g + 1) * tall, :], narrow, opposite,
        v["s2"], v["r2"], v["s2s"], v["s2r"], moe_done,
    )
    term, mixbox = v["term"], v["mixbox"]

    def spread_rows(o, k):
        peer = lax.rem(tp + k, m)
        return remote(term.at[o, rows_of(peer), :], mixbox.at[o, tp], v["fs"].at[o], v["fr"].at[o], {"tp": peer})

    for o in (1, 0):
        whole = pieces.at[o]
        remote(whole, whole, v["bs"].at[o, 0], v["br"].at[o], partner).wait_recv()
        flat = pieces[o].reshape(n * slots, lanes)
        term[o] = (mm(v["mixhi"][...], flat) + mm(v["mixlo"][...], flat)).astype(BF16)
        for k in far_tp:
            spread_rows(o, k).start()
        mixbox[o, tp] = term[o, rows_of(tp), :]
    row_waits = []
    for o in (1, 0):
        whole = mixbox.at[o, 0 : m - 1]
        row_waits.append(remote(whole, whole, v["fs"].at[o], v["fr"].at[o], partner))
        row_waits[-1].wait_recv()
    mixture = jnp.concatenate(
        [mixbox[0, i].astype(F32) + mixbox[1, (i + YN) % m].astype(F32) for i in range(m)], axis=1
    )
    out[...] = layer_norm(settled[...] + mixture, v["gain_moe"][...]).astype(BF16)

    if XN > 1:
        all_of(xbox, XN, v["xs"], v["xr"]).wait_send()
        all_of(states, XN, v["es"], v["er"]).wait_send()
    if ZN > 1:
        all_of(zbox, ZN, v["zs"], v["zr"]).wait_send()
    hand.wait_send()
    for swap in swaps:
        swap.wait_send()
    all_columns.wait_send()
    for wait in row_waits:
        wait.wait_send()
    for o in range(2):
        most = picked.at[0, 0 : n - 1]
        remote(most, most, v["ds"].at[o, 0], v["dr"].at[o], partner).wait_send()
        pl.when(c == 1)(lambda: dispatch(o, 0, 0).wait_send())
        most = pieces.at[o, 0 : n - 1]
        remote(most, most, v["bs"].at[o, 0], v["br"].at[o], partner).wait_send()
        pl.when(c == 1)(lambda: give(o, 0, 0).wait_send())
    if half > 1:
        whole = x.at[0 : 2 * (half - 1)]
        remote(whole, whole, v["gs"], v["gr"].at[0, 0], partner).wait_send()


def body(
    query_one, key_one, value_one, gate_one, decay_one, query_two, key_two, value_two, gate_two, decay_two,
    head_gain, proj_one, proj_two, stream, gain_mix, gain_moe, routes, affinity, expert_gate, expert_up,
    expert_down,
):
    rows, width = stream.shape
    dv = head_gain.shape[0]
    scratch = shapes_of(rows, dv, width)
    return pl.pallas_call(
        functools.partial(layer_kernel, tuple(scratch)),
        out_shape=jax.ShapeDtypeStruct((rows // (YN * 2), width), BF16),
        in_specs=[ANY] * len(INPUTS),
        out_specs=VMEM,
        scratch_shapes=list(scratch.values()),
        compiler_params=pltpu.CompilerParams(
            vmem_limit_bytes=56 * 2**20, collective_id=1, has_side_effects=True
        ),
    )(
        query_one.T, key_one.T, value_one, gate_one, jnp.swapaxes(decay_one, 1, 2), query_two, key_two, value_two,
        gate_two, decay_two, head_gain.reshape(1, -1), proj_one, proj_two, stream, gain_mix.reshape(1, -1),
        gain_moe.reshape(1, -1), routes.T, affinity.T, expert_gate, expert_up, expert_down,
    )


def solution(mesh):
    return jax.shard_map(
        body,
        mesh=mesh,
        in_specs=(
            P("sp", "tp"),
            P("sp", "tp"),
            P("sp", "tp"),
            P("sp", "tp"),
            P(None, "sp", "tp"),
            P("sp", "tp"),
            P("sp", "tp"),
            P("sp", "tp"),
            P("sp", "tp"),
            P(None, "sp", "tp"),
            P(),
            P("tp", None),
            P("tp", None),
            P("sp", None),
            P(),
            P(),
            P("sp", None),
            P("sp", None),
            P("sp", None, "tp"),
            P("sp", None, "tp"),
            P("sp", "tp", None),
        ),
        out_specs=P(("sp", "tp"), None),
        check_vma=False,
    )
```
